128 devices in a mesh: sp: 32 (over z, y, core), tp: 4 (over x).
Axes of the slice: x: 4, y: 4, z: 4, core: 2. Of those that a mesh axis runs over, the one named last changes fastest.
Arguments:
- residual: bfloat16 [32768, 2048], P('sp', 'tp'), may hold values from -64 to 64
- rotated_query_rows: bfloat16 [32768, 1536], P('sp', 'tp'), may hold values from -256 to 256
- rotated_key_rows: bfloat16 [32768, 512], P('sp', 'tp'), may hold values from -6 to 6
- value_matrix_rows: bfloat16 [32768, 512], P('sp', 'tp'), may hold values from -16 to 16
- head_sink_logit: float32 [24], P('tp'), may hold values from 2 to 7
- out_proj: bfloat16 [1536, 2048], P('tp'), may hold values from -1.2247449 to 1.2247449
- gain_mix: float32 [2048], replicated, may hold values from 0.1 to 1.9
- gain_pre: float32 [2048], replicated, may hold values from 0.1 to 1.9
- gain_post: float32 [2048], replicated, may hold values from 0.1 to 1.9
- gate_proj: bfloat16 [2048, 5632], P('sp', 'tp'), may hold values from -0.125 to 0.125
- up_proj: bfloat16 [2048, 5632], P('sp', 'tp'), may hold values from -0.125 to 0.125
- down_proj: bfloat16 [5632, 2048], P('tp', 'sp'), may hold values from -0.21320072 to 0.21320072
Outputs:
- layer_out: bfloat16 [32768, 2048], P('sp', 'tp')
The draws below stay inside these ranges and needn't reach their ends.
All inputs are finite; a program needn't handle non-finite values.
Results may differ from the reference program's by a relative error of at most 0.0095.
Values may be sent and summed in bfloat16 or wider, within the bound.
A program may use at most 128 MiB of HBM per device.

```python
import math
import jax
import jax.numpy as jnp
from jax import lax

D = 2048
FF = 5632
QUERY_HEAD_COUNT = 24
KEY_VALUE_HEADS = 8
HEAD_WIDTH = 64
WINDOW = 128
TOKEN_COUNT = 32768
N_TP = 4


def rising(count, top_scale):
    return jnp.exp(jnp.linspace(0.0, math.log(top_scale), count, dtype=jnp.float32))


def drawn_pair(key):
    key_sample, query_draw = jax.random.split(jax.random.fold_in(key, 7), 2)
    key_entries = jnp.clip(jax.random.normal(key_sample, (TOKEN_COUNT, KEY_VALUE_HEADS * HEAD_WIDTH), jnp.float32), -6.0, 6.0)
    query_vals = jnp.clip(jax.random.normal(query_draw, (TOKEN_COUNT, QUERY_HEAD_COUNT * HEAD_WIDTH), jnp.float32), -6.0, 6.0)
    return (query_vals, key_entries)


def draw_rotated_query_rows(key, part):
    return drawn_pair(key)[0].astype(jnp.bfloat16)


def draw_rotated_key_rows(key, part):
    return drawn_pair(key)[1].astype(jnp.bfloat16)


def draw_value_matrix_rows(key, part):
    base_key, scale_key = jax.random.split(jax.random.fold_in(key, 19))
    regions = TOKEN_COUNT // WINDOW
    head_scale = jnp.exp(jax.random.uniform(scale_key, (regions, KEY_VALUE_HEADS), jnp.float32, math.log(0.3), math.log(3.0)))
    spread_scale = jnp.repeat(jnp.repeat(head_scale, WINDOW, axis=0), HEAD_WIDTH, axis=1)
    base_draw = jnp.clip(jax.random.normal(base_key, (TOKEN_COUNT, KEY_VALUE_HEADS * HEAD_WIDTH), jnp.float32), -5.0, 5.0)
    return (base_draw * spread_scale).astype(jnp.bfloat16)


def draw_residual(key, part):
    base_key, scale_key = jax.random.split(jax.random.fold_in(key, 11))
    base_draw = jnp.clip(jax.random.normal(base_key, (TOKEN_COUNT, D), jnp.float32), -5.0, 5.0)
    block_scale = jnp.exp(jax.random.uniform(scale_key, (TOKEN_COUNT, N_TP), jnp.float32, math.log(0.2), math.log(2.0)))
    column_scale = jnp.repeat(block_scale, D // N_TP, axis=1)
    return (base_draw * column_scale * rising(D, 3.0)).astype(jnp.bfloat16)


def scaled_weight(key, salt, fan_in):
    base_key = jax.random.fold_in(key, salt)
    base_draw = jnp.clip(jax.random.normal(base_key, (fan_in, D), jnp.float32), -4.0, 4.0)
    return base_draw * fan_in ** (-0.5) * rising(D, 3.0)


def draw_out_proj(key, part):
    fan_in = QUERY_HEAD_COUNT * HEAD_WIDTH
    pairing = jax.random.permutation(jax.random.fold_in(key, 23), N_TP)
    row_group = jnp.arange(fan_in, dtype=jnp.int32) // (fan_in // N_TP)
    column_group = jnp.arange(D, dtype=jnp.int32) // (D // N_TP)
    boosted = jnp.where(pairing[row_group][:, None] == column_group[None, :], 3.0, 1.0)
    return (scaled_weight(key, 13, fan_in) * boosted).astype(jnp.bfloat16)


def draw_down_proj(key, part):
    return scaled_weight(key, 17, FF).astype(jnp.bfloat16)


def level_of(stream_key, dims, shards, least, largest):
    def one(position, shards_of):
        steps = jax.random.uniform(jax.random.fold_in(jax.random.fold_in(stream_key, 6), position), (shards_of,), jnp.float32, least / len(shards), largest / len(shards))
        return jnp.repeat(jnp.exp(steps), dims[position] // shards_of).reshape((-1,) + (1,) * (len(dims) - position - 1))

    level = one(*shards[0])
    for cut in shards[1:]:
        level = level * one(*cut)
    return level


def scatter_about(key, dims, deviation, limit, pieces=(), held_as=jnp.bfloat16):
    level = level_of(key, dims, pieces, -0.22, 0.18) if pieces else 1.0
    result = jax.random.normal(key, dims, jnp.float32) * deviation * level
    return jnp.minimum(jnp.maximum(result, -limit), limit).astype(held_as)


def setup_inputs(seed: int = 0) -> dict:
    keys = jax.random.split(jax.random.key(seed), 13)
    residual = draw_residual(jax.random.fold_in(keys[12], 71), 0)
    rotated_query_rows = draw_rotated_query_rows(jax.random.fold_in(keys[12], 71), 0)
    rotated_key_rows = draw_rotated_key_rows(jax.random.fold_in(keys[12], 71), 0)
    value_matrix_rows = draw_value_matrix_rows(jax.random.fold_in(keys[12], 71), 0)
    head_sink_logit = jnp.clip(2.0 + 5.0 * jax.random.uniform(keys[4], (QUERY_HEAD_COUNT,), jnp.float32) ** level_of(keys[4], (QUERY_HEAD_COUNT,), ((0, 4),), -0.2, 0.2), 2.0, 7.0)
    out_proj = draw_out_proj(jax.random.fold_in(keys[12], 71), 0)
    gain_mix = jnp.clip(1.0 + 0.18 * jax.random.normal(keys[6], (D,), jnp.float32), 0.1, 1.9)
    gain_pre = jnp.clip(1.0 + 0.18 * jax.random.normal(keys[7], (D,), jnp.float32), 0.1, 1.9)
    gain_post = jnp.clip(1.0 + 0.18 * jax.random.normal(keys[8], (D,), jnp.float32), 0.1, 1.9)
    gate_proj = scatter_about(keys[9], (D, FF), D ** -0.5, 0.125, ((0, 32), (1, 4)))
    up_proj = scatter_about(keys[10], (D, FF), D ** -0.5, 0.125, ((0, 32), (1, 4)))
    down_proj = draw_down_proj(jax.random.fold_in(keys[12], 71), 0)
    return dict(residual=residual, rotated_query_rows=rotated_query_rows, rotated_key_rows=rotated_key_rows, value_matrix_rows=value_matrix_rows, head_sink_logit=head_sink_logit, out_proj=out_proj, gain_mix=gain_mix, gain_pre=gain_pre, gain_post=gain_post, gate_proj=gate_proj, up_proj=up_proj, down_proj=down_proj)


norm_eps = 1e-06

def scale_rows(values, gain):
    return values * lax.rsqrt(lax.optimization_barrier(jnp.mean(values * values, axis=1, keepdims=True)) + norm_eps) * gain

def band_attention(query_part, padded, sink_part, first_pos, seq_total):
    row_count = query_part.shape[0]
    blocks = row_count // WINDOW
    kv_heads = padded.shape[1] // (2 * HEAD_WIDTH)
    heads_per_group = query_part.shape[1] // (kv_heads * HEAD_WIDTH)
    query_tiles = query_part.reshape(blocks, WINDOW, kv_heads, heads_per_group, HEAD_WIDTH).astype(jnp.float32)
    kv_tiles = padded.reshape(blocks + 2, WINDOW, padded.shape[1])
    kv_band = jnp.concatenate([kv_tiles[:-2], kv_tiles[1:-1], kv_tiles[2:]], axis=1)
    key_band = kv_band[:, :, :kv_heads * HEAD_WIDTH].reshape(blocks, 3 * WINDOW, kv_heads, HEAD_WIDTH).astype(jnp.float32)
    value_band = kv_band[:, :, kv_heads * HEAD_WIDTH:].reshape(blocks, 3 * WINDOW, kv_heads, HEAD_WIDTH).astype(jnp.float32)
    scores = jnp.einsum('nqhgd,nkhd->nhgqk', query_tiles, key_band) * HEAD_WIDTH ** (-0.5)
    block_start = first_pos + jnp.arange(blocks, dtype=jnp.int32)[:, None, None] * WINDOW
    query_pos = block_start + jnp.arange(WINDOW, dtype=jnp.int32)[None, :, None]
    key_pos = block_start - WINDOW + jnp.arange(3 * WINDOW, dtype=jnp.int32)[None, None, :]
    inside = (jnp.abs(query_pos - key_pos) <= WINDOW) & (key_pos >= 0) & (key_pos < seq_total)
    scores = jnp.where(inside[:, None, None], scores, -jnp.inf)
    sink_tiles = sink_part.reshape(kv_heads, heads_per_group)[None, :, :, None, None]
    row_max = jnp.maximum(lax.optimization_barrier(jnp.max(scores, axis=-1, keepdims=True)), sink_tiles)
    exp_scores = jnp.exp(scores - row_max)
    denominator = lax.optimization_barrier(jnp.sum(exp_scores, axis=-1, keepdims=True)) + jnp.exp(sink_tiles - row_max)
    weights = (exp_scores / denominator).astype(jnp.bfloat16).astype(jnp.float32)
    attn_out = jnp.einsum('nhgqk,nkhd->nqhgd', weights, value_band)
    return attn_out.reshape(row_count, query_part.shape[1]).astype(jnp.bfloat16)

def grouped_sum(left, right):
    width = left.shape[1] // N_TP
    total = jnp.zeros((left.shape[0], right.shape[1]), jnp.float32)
    for head_group in range(N_TP):
        partial_value = jnp.dot(left[:, head_group * width:(head_group + 1) * width], right[head_group * width:(head_group + 1) * width, :], preferred_element_type=jnp.float32)
        total = total + lax.optimization_barrier(partial_value.astype(jnp.bfloat16)).astype(jnp.float32)
    return total

def reference(residual, rotated_query_rows, rotated_key_rows, value_matrix_rows, head_sink_logit, out_proj, gain_mix, gain_pre, gain_post, gate_proj, up_proj, down_proj):
    heads_per_group = QUERY_HEAD_COUNT // KEY_VALUE_HEADS
    query_head_total = jnp.transpose(rotated_query_rows.reshape(TOKEN_COUNT, KEY_VALUE_HEADS, heads_per_group * HEAD_WIDTH), (1, 0, 2))
    key_head_count = jnp.transpose(rotated_key_rows.reshape(TOKEN_COUNT, KEY_VALUE_HEADS, HEAD_WIDTH), (1, 0, 2))
    value_head_count = jnp.transpose(value_matrix_rows.reshape(TOKEN_COUNT, KEY_VALUE_HEADS, HEAD_WIDTH), (1, 0, 2))
    sink_head_count = head_sink_logit.reshape(KEY_VALUE_HEADS, heads_per_group)

    def one_head(inputs):
        query_part, key_part, value_part, sink_part = inputs
        padded = jnp.pad(jnp.concatenate([key_part, value_part], axis=1), ((WINDOW, WINDOW), (0, 0)))
        return band_attention(query_part, padded, sink_part, 0, TOKEN_COUNT)
    attended = lax.map(one_head, (query_head_total, key_head_count, value_head_count, sink_head_count))
    attended = jnp.transpose(attended, (1, 0, 2)).reshape(TOKEN_COUNT, QUERY_HEAD_COUNT * HEAD_WIDTH)
    mixed_sum = grouped_sum(attended, out_proj)
    first_rows = (residual.astype(jnp.float32) + scale_rows(mixed_sum, gain_mix)).astype(jnp.bfloat16)
    first_wide = first_rows.astype(jnp.float32)
    normed = scale_rows(first_wide, gain_pre).astype(jnp.bfloat16)
    gate_pre = jnp.dot(normed, gate_proj, preferred_element_type=jnp.float32)
    up_pre = jnp.dot(normed, up_proj, preferred_element_type=jnp.float32)
    hidden = (jax.nn.silu(gate_pre) * up_pre).astype(jnp.bfloat16)
    ffn_sum = grouped_sum(hidden, down_proj)
    return (first_wide + 0.5 * scale_rows(ffn_sum, gain_post)).astype(jnp.bfloat16)
```

```python
import functools

import jax
import jax.numpy as jnp
from jax import lax
from jax.experimental import pallas as pl
from jax.experimental.pallas import tpu as pltpu
from jax.sharding import PartitionSpec as P

WINDOW = 128
EPS = 1e-06
MESH = pl.DeviceIdType.MESH
F32 = jnp.float32
BF16 = jnp.bfloat16
NT = (((1,), (1,)), ((), ()))


def ring():
    me = lax.axis_index("tp")
    right, left, far = (lax.rem(me + k, 4) for k in (1, 3, 2))
    return me, right, left, far


def tp_copy(src, dst, send, recv, to):
    return pltpu.make_async_remote_copy(
        src_ref=src, dst_ref=dst, send_sem=send, recv_sem=recv,
        device_id={"tp": to}, device_id_type=MESH,
    )


def greet(barrier, others):
    for other in others:
        pl.semaphore_signal(barrier, inc=1, device_id=other, device_id_type=MESH)
    pl.semaphore_wait(barrier, len(others))


class Scatter:
    def __init__(self, sent, got, own, send, recv):
        self.sent, self.got, self.own, self.send, self.recv = sent, got, own, send, recv
        self.me, self.right, self.left, self.far = ring()

    def copy(self, slot, m):
        to = self.right if m % 2 == 0 else self.left
        return tp_copy(
            self.sent.at[slot, m], self.got.at[slot, m],
            self.send.at[slot, m], self.recv.at[slot, m], to,
        )

    def first(self, slot, part):
        self.sent[slot, 0] = part(self.far, 0)
        self.copy(slot, 0).start()
        self.sent[slot, 1] = part(self.far, 1)
        self.copy(slot, 1).start()
        self.sent[slot, 2] = part(self.right, 1)
        self.copy(slot, 2).start()
        self.sent[slot, 3] = part(self.left, 0)
        self.copy(slot, 3).start()
        self.sent[slot, 4] = part(self.right, 0)
        self.sent[slot, 5] = part(self.left, 1)
        self.own[slot, :, :256] = part(self.me, 0)
        self.own[slot, :, 256:] = part(self.me, 1)

    def second(self, slot):
        for k in (0, 1):
            self.copy(slot, k).wait_recv()
            total = self.sent[slot, 4 + k].astype(F32) + self.got[slot, k].astype(F32)
            self.sent[slot, 4 + k] = total.astype(BF16)
            self.copy(slot, 4 + k).start()

    def last(self, slot):
        for m in (2, 3, 4, 5):
            self.copy(slot, m).wait_recv()
        half0 = (
            self.own[slot, :, :256].astype(F32)
            + self.got[slot, 4].astype(F32)
            + self.got[slot, 3].astype(F32)
        )
        half1 = (
            self.own[slot, :, 256:].astype(F32)
            + self.got[slot, 2].astype(F32)
            + self.got[slot, 5].astype(F32)
        )
        return half0, half1

    def drain(self, slot):
        for m in range(6):
            self.copy(slot, m).wait_send()


class Squares:
    def __init__(self, mine, got, send, recv):
        self.mine, self.got, self.send, self.recv = mine, got, send, recv
        self.me, self.right, self.left, self.far = ring()

    def copies(self, slot):
        for m, to in enumerate((self.right, self.left, self.far)):
            yield tp_copy(
                self.mine.at[slot], self.got.at[slot, m],
                self.send.at[slot, m], self.recv.at[slot, m], to,
            )

    def give(self, slot, half0, half1):
        total = jnp.sum(half0 * half0, axis=1, keepdims=True) + jnp.sum(
            half1 * half1, axis=1, keepdims=True
        )
        for g in range(total.shape[0] // 128):
            wide = jnp.broadcast_to(total[128 * g : 128 * g + 128], (128, 128))
            self.mine[slot, 8 * g : 8 * g + 8] = wide.T[:8]
        for copy in self.copies(slot):
            copy.start()

    def take(self, slot):
        for copy in self.copies(slot):
            copy.wait_recv()
        total = self.mine[slot] + self.got[slot, 0] + self.got[slot, 1] + self.got[slot, 2]
        columns = [
            jnp.broadcast_to(total[8 * g : 8 * g + 1], (128, 128)).T[:, :1]
            for g in range(total.shape[0] // 8)
        ]
        return columns[0] if len(columns) == 1 else jnp.concatenate(columns, axis=0)

    def drain(self, slot):
        for copy in self.copies(slot):
            copy.wait_send()


def attend(row, first_key, q_ref, kv, sink_ref, lowest, highest):
    keys, keys_turned, values, values_turned = (
        a[pl.ds(first_key, 3 * WINDOW), :] for a in kv
    )
    lane = lax.broadcasted_iota(jnp.int32, (WINDOW, 128), 1)
    query = lax.broadcasted_iota(jnp.int32, (WINDOW, 3 * WINDOW), 0)
    key = lax.broadcasted_iota(jnp.int32, (WINDOW, 3 * WINDOW), 1)
    inside = (key >= query) & (key <= query + 2 * WINDOW) & (key >= lowest) & (key < highest)
    tiles = []
    for t in range(3):
        pair = q_ref[pl.ds(row, WINDOW), 128 * t : 128 * t + 128].astype(F32) * 0.125
        outs = []
        for half in range(2):
            h = 2 * t + half
            turned = (h // 3) != half
            q = jnp.where((lane >= 64) == (half == 1), pair, 0.0).astype(BF16)
            scores = lax.dot_general(
                q, keys_turned if turned else keys, NT, preferred_element_type=F32
            )
            scores = jnp.where(inside, scores, -1e30)
            sink = sink_ref[h]
            top = jnp.maximum(jnp.max(scores, axis=1, keepdims=True), sink)
            e = jnp.exp(scores - top)
            below = jnp.sum(e, axis=1, keepdims=True) + jnp.exp(sink - top)
            out = jnp.dot(
                e.astype(BF16), values_turned if turned else values,
                preferred_element_type=F32,
            )
            outs.append(out * (1.0 / below))
        tiles.append(jnp.where(lane < 64, outs[0], outs[1]).astype(BF16))
    return jnp.concatenate(tiles, axis=1)


def turn(x):
    return pltpu.roll(x.astype(F32), 64, 1).astype(BF16)


def mix_kernel(
    chunks, sp_count,
    res_ref, q_ref, k_ref, v_ref, sink_ref, proj_ref, gain_ref,
    out_ref,
    keys, keys_turned, values, values_turned, att,
    sent, got, own, mixed, mine, squares, rows,
    halo_send, halo_recv, rs_send, rs_recv, sq_send, sq_recv, ag_send, ag_recv,
):
    me, right, left, far = ring()
    sp = lax.axis_index("sp")
    after = lax.rem(sp + 1, sp_count)
    before = lax.rem(sp + sp_count - 1, sp_count)
    length = chunks * WINDOW
    greet(
        pltpu.get_barrier_semaphore(),
        [{"tp": right}, {"tp": left}, {"tp": far}, {"sp": after}, {"sp": before}],
    )

    def halo(n):
        mine_ref, whole = ((k_ref, keys), (v_ref, values))[n // 2]
        if n % 2 == 0:
            src, dst, to = mine_ref.at[pl.ds(length - WINDOW, WINDOW)], whole.at[pl.ds(0, WINDOW)], after
        else:
            src, dst, to = mine_ref.at[pl.ds(0, WINDOW)], whole.at[pl.ds(length + WINDOW, WINDOW)], before
        return pltpu.make_async_remote_copy(
            src_ref=src, dst_ref=dst, send_sem=halo_send.at[n], recv_sem=halo_recv.at[n],
            device_id={"sp": to}, device_id_type=MESH,
        )

    for n in range(4):
        halo(n).start()
    middle = pl.ds(WINDOW, length)
    keys[middle, :] = k_ref[...]
    values[middle, :] = v_ref[...]
    keys_turned[middle, :] = turn(k_ref[...])
    values_turned[middle, :] = turn(v_ref[...])

    scatter = Scatter(sent, got, own, rs_send, rs_recv)
    sums = Squares(mine, squares, sq_send, sq_recv)
    gain = gain_ref[:, pl.ds(pl.multiple_of(me * 512, 512), 512)]

    def place(slot):
        return lax.rem(slot + 1, chunks) * WINDOW

    def gather(slot, m):
        owner, to, part = (
            (me, right, pl.ds(0, 512)), (me, left, pl.ds(0, 512)),
            (left, right, pl.ds(0, 256)), (right, left, pl.ds(256, 256)),
        )[m]
        ref = rows.at[owner, slot, :, part]
        return tp_copy(ref, ref, ag_send.at[slot, m], ag_recv.at[slot, m], to)

    def arrived(slot, m):
        owner, part = (
            (left, pl.ds(0, 512)), (right, pl.ds(0, 512)),
            (far, pl.ds(0, 256)), (far, pl.ds(256, 256)),
        )[m]
        ref = rows.at[owner, slot, :, part]
        tp_copy(ref, ref, ag_send.at[slot, m], ag_recv.at[slot, m], right).wait_recv()

    def step(t, carry):
        @pl.when(t == chunks - 2)
        def _():
            for n in range(4):
                halo(n).wait_recv()
            for at in (0, length + WINDOW):
                keys_turned[pl.ds(at, WINDOW), :] = turn(keys[pl.ds(at, WINDOW), :])
                values_turned[pl.ds(at, WINDOW), :] = turn(values[pl.ds(at, WINDOW), :])

        @pl.when(t < chunks)
        def _():
            row = pl.multiple_of(place(t), WINDOW)
            lowest = jnp.where((sp == 0) & (t == chunks - 1), WINDOW, 0)
            highest = jnp.where((sp == sp_count - 1) & (t == chunks - 2), 2 * WINDOW, 3 * WINDOW)
            att[...] = attend(
                row, row, q_ref, (keys, keys_turned, values, values_turned),
                sink_ref, lowest, highest,
            )

            def part(block, half):
                columns = pl.ds(pl.multiple_of(block * 512 + 256 * half, 256), 256)
                return jnp.dot(
                    att[...], proj_ref[:, columns], preferred_element_type=F32
                ).astype(BF16)

            scatter.first(t, part)

        @pl.when((t >= 1) & (t < chunks + 1))
        def _():
            scatter.second(t - 1)

        @pl.when((t >= 2) & (t < chunks + 2))
        def _():
            half0, half1 = scatter.last(t - 2)
            mixed[t - 2, :, :256] = half0
            mixed[t - 2, :, 256:] = half1
            sums.give(t - 2, half0, half1)

        @pl.when((t >= 3) & (t < chunks + 3))
        def _():
            s = t - 3
            scale = lax.rsqrt(sums.take(s) / 2048.0 + EPS)
            res = res_ref[pl.ds(pl.multiple_of(place(s), WINDOW), WINDOW), :].astype(F32)
            rows[me, s] = (res + mixed[s] * scale * gain).astype(BF16)
            gather(s, 0).start()
            gather(s, 1).start()

        @pl.when((t >= 4) & (t < chunks + 4))
        def _():
            arrived(t - 4, 0)
            gather(t - 4, 2).start()
            arrived(t - 4, 1)
            gather(t - 4, 3).start()

        @pl.when(t >= 5)
        def _():
            arrived(t - 5, 2)
            arrived(t - 5, 3)

        return carry

    lax.fori_loop(0, chunks + 5, step, 0)

    for n in range(4):
        halo(n).wait_send()

    def drain(slot, carry):
        scatter.drain(slot)
        sums.drain(slot)
        for m in range(4):
            gather(slot, m).wait_send()
        return carry

    lax.fori_loop(0, chunks, drain, 0)
    out_ref[...] = rows[...]


def feed_kernel(
    chunks,
    rows_ref, gain_pre_ref, gain_post_ref, w_ref,
    out_ref,
    w_in, w_out, normed, hidden,
    sent, got, own, total, mine, squares,
    w_sem, rs_send, rs_recv, sq_send, sq_recv,
):
    me, right, left, far = ring()
    tiles = w_in.shape[1] // 256
    inner = w_in.shape[1]
    big = 2 * WINDOW

    def load(j):
        columns = pl.ds(pl.multiple_of(j * 256, 256), 256)
        return pltpu.make_async_copy(w_ref.at[:, columns], w_in.at[:, columns], w_sem.at[j])

    def load_out():
        return pltpu.make_async_copy(
            w_ref.at[:, pl.ds(inner, w_out.shape[1])], w_out, w_sem.at[tiles]
        )

    for j in range(tiles):
        load(j).start()
    load_out().start()
    greet(pltpu.get_barrier_semaphore(), [{"tp": right}, {"tp": left}, {"tp": far}])
    scatter = Scatter(sent, got, own, rs_send, rs_recv)
    sums = Squares(mine, squares, sq_send, sq_recv)
    gain = gain_post_ref[:, pl.ds(pl.multiple_of(me * 512, 512), 512)]

    def step(t, carry):
        @pl.when(t < chunks)
        def _():
            for k in range(2):
                squared = jnp.zeros((WINDOW, 1), F32)
                for b in range(4):
                    x = rows_ref[b, 2 * t + k].astype(F32)
                    squared += jnp.sum(x * x, axis=1, keepdims=True)
                scale = lax.rsqrt(squared / 2048.0 + EPS)
                for b in range(4):
                    x = rows_ref[b, 2 * t + k].astype(F32)
                    normed[WINDOW * k : WINDOW * k + WINDOW, 512 * b : 512 * b + 512] = (
                        x * scale * gain_pre_ref[:, 512 * b : 512 * b + 512]
                    ).astype(BF16)

            def tile(j, carry):
                @pl.when(t == 0)
                def _():
                    load(j).wait()

                both = jnp.dot(
                    normed[...], w_in[:, pl.ds(pl.multiple_of(j * 256, 256), 256)],
                    preferred_element_type=F32,
                )
                gate, up = both[:, :128], both[:, 128:]
                hidden[:, pl.ds(pl.multiple_of(j * 128, 128), 128)] = (
                    gate / (1.0 + jnp.exp(-gate)) * up
                ).astype(BF16)
                return carry

            lax.fori_loop(0, tiles, tile, 0)

            @pl.when(t == 0)
            def _():
                load_out().wait()

            def part(block, half):
                at = pl.ds(pl.multiple_of(block * 512 + 256 * half, 256), 256)
                return lax.dot_general(
                    hidden[...], w_out[at, :], NT, preferred_element_type=F32
                ).astype(BF16)

            scatter.first(t, part)

        @pl.when((t >= 1) & (t < chunks + 1))
        def _():
            scatter.second(t - 1)

        @pl.when((t >= 2) & (t < chunks + 2))
        def _():
            half0, half1 = scatter.last(t - 2)
            total[t - 2, :, :256] = half0
            total[t - 2, :, 256:] = half1
            sums.give(t - 2, half0, half1)

        @pl.when(t >= 3)
        def _():
            s = t - 3
            scale = lax.rsqrt(sums.take(s) / 2048.0 + EPS)
            for k in range(2):
                part = pl.ds(WINDOW * k, WINDOW)
                row = pl.multiple_of(lax.rem(2 * s + k + 1, 2 * chunks) * WINDOW, WINDOW)
                out_ref[pl.ds(row, WINDOW), :] = (
                    rows_ref[me, 2 * s + k].astype(F32)
                    + 0.5 * (total[s, part, :] * scale[WINDOW * k : WINDOW * k + WINDOW] * gain)
                ).astype(BF16)

        return carry

    lax.fori_loop(0, chunks + 3, step, 0)

    def drain(slot, carry):
        scatter.drain(slot)
        sums.drain(slot)
        return carry

    lax.fori_loop(0, chunks, drain, 0)


def sems(*shapes):
    return [pltpu.SemaphoreType.DMA(s) for s in shapes]


def body(
    residual, rotated_query_rows, rotated_key_rows, value_matrix_rows, head_sink_logit,
    out_proj, gain_mix, gain_pre, gain_post, gate_proj, up_proj, down_proj,
):
    length = residual.shape[0]
    chunks = length // WINDOW
    depth, units = gate_proj.shape
    both = jnp.stack(
        [gate_proj.reshape(depth, units // 128, 128), up_proj.reshape(depth, units // 128, 128)],
        axis=2,
    ).reshape(depth, 2 * units)
    weights = lax.all_gather(
        jnp.concatenate([both, down_proj.T], axis=1), "sp", axis=0, tiled=True
    )
    vmem = pl.BlockSpec(memory_space=pltpu.VMEM)
    rows = pl.pallas_call(
        functools.partial(mix_kernel, chunks, lax.axis_size("sp")),
        out_shape=jax.ShapeDtypeStruct((4, chunks, WINDOW, 512), BF16),
        in_specs=[vmem] * 4 + [pl.BlockSpec(memory_space=pltpu.SMEM)] + [vmem] * 2,
        out_specs=vmem,
        scratch_shapes=[pltpu.VMEM((length + 2 * WINDOW, 128), BF16)] * 4
        + [
            pltpu.VMEM((WINDOW, 384), BF16),
            pltpu.VMEM((chunks, 6, WINDOW, 256), BF16),
            pltpu.VMEM((chunks, 6, WINDOW, 256), BF16),
            pltpu.VMEM((chunks, WINDOW, 512), BF16),
            pltpu.VMEM((chunks, WINDOW, 512), F32),
            pltpu.VMEM((chunks, 8, 128), F32),
            pltpu.VMEM((chunks, 3, 8, 128), F32),
            pltpu.VMEM((4, chunks, WINDOW, 512), BF16),
        ]
        + sems((4,), (4,), (chunks, 6), (chunks, 6), (chunks, 3), (chunks, 3), (chunks, 4), (chunks, 4)),
        compiler_params=pltpu.CompilerParams(
            collective_id=0, has_side_effects=True, vmem_limit_bytes=40 * 2**20
        ),
        cost_estimate=pl.CostEstimate(
            flops=50 * 10**9, bytes_accessed=8 * 2**20, transcendentals=0
        ),
    )(
        residual, rotated_query_rows, rotated_key_rows, value_matrix_rows, head_sink_logit,
        out_proj, gain_mix[None],
    )
    half = chunks // 2
    big = 2 * WINDOW
    full = weights.shape[0]
    return pl.pallas_call(
        functools.partial(feed_kernel, half),
        out_shape=jax.ShapeDtypeStruct(residual.shape, BF16),
        in_specs=[vmem] * 3 + [pl.BlockSpec(memory_space=pl.ANY)],
        out_specs=vmem,
        scratch_shapes=[
            pltpu.VMEM((full, 2 * units), BF16),
            pltpu.VMEM((full, units), BF16),
            pltpu.VMEM((big, full), BF16),
            pltpu.VMEM((big, units), BF16),
            pltpu.VMEM((half, 6, big, 256), BF16),
            pltpu.VMEM((half, 6, big, 256), BF16),
            pltpu.VMEM((half, big, 512), BF16),
            pltpu.VMEM((half, big, 512), F32),
            pltpu.VMEM((half, 16, 128), F32),
            pltpu.VMEM((half, 3, 16, 128), F32),
        ]
        + sems((2 * units // 256 + 1,), (half, 6), (half, 6), (half, 3), (half, 3)),
        compiler_params=pltpu.CompilerParams(
            collective_id=1, has_side_effects=True, vmem_limit_bytes=60 * 2**20
        ),
    )(rows, gain_pre[None], gain_post[None], weights)


def solution(mesh):
    placed = (
        P("sp", "tp"), P("sp", "tp"), P("sp", "tp"), P("sp", "tp"), P("tp"), P("tp", None),
        P(), P(), P(), P("sp", "tp"), P("sp", "tp"), P("tp", "sp"),
    )
    return jax.shard_map(body, mesh=mesh, in_specs=placed, out_specs=P("sp", "tp"), check_vma=False)
```

```python
import functools

import jax
import jax.numpy as jnp
from jax import lax
from jax.experimental import pallas as pl
from jax.experimental.pallas import tpu as pltpu
from jax.sharding import PartitionSpec as P

WINDOW = 128
EPS = 1e-06
FEED_AT = 8
MESH = pl.DeviceIdType.MESH
F32 = jnp.float32
BF16 = jnp.bfloat16
NT = (((1,), (1,)), ((), ()))


def ring():
    me = lax.axis_index("tp")
    right, left, far = (lax.rem(me + k, 4) for k in (1, 3, 2))
    return me, right, left, far


def tp_copy(src, dst, send, recv, to):
    return pltpu.make_async_remote_copy(
        src_ref=src, dst_ref=dst, send_sem=send, recv_sem=recv,
        device_id={"tp": to}, device_id_type=MESH,
    )


class Scatter:
    def __init__(self, sent, got, own, send, recv):
        self.sent, self.got, self.own, self.send, self.recv = sent, got, own, send, recv
        self.me, self.right, self.left, self.far = ring()

    def copy(self, slot, m):
        to = self.right if m % 2 == 0 else self.left
        return tp_copy(
            self.sent.at[slot, m], self.got.at[slot, m],
            self.send.at[slot, m], self.recv.at[slot, m], to,
        )

    def first(self, slot, part):
        self.sent[slot, 0] = part(self.far, 0)
        self.copy(slot, 0).start()
        self.sent[slot, 1] = part(self.far, 1)
        self.copy(slot, 1).start()
        self.sent[slot, 2] = part(self.right, 1)
        self.copy(slot, 2).start()
        self.sent[slot, 3] = part(self.left, 0)
        self.copy(slot, 3).start()
        self.sent[slot, 4] = part(self.right, 0)
        self.sent[slot, 5] = part(self.left, 1)
        self.own[slot, :, :256] = part(self.me, 0)
        self.own[slot, :, 256:] = part(self.me, 1)

    def second(self, slot):
        for k in (0, 1):
            self.copy(slot, k).wait_recv()
            total = self.sent[slot, 4 + k].astype(F32) + self.got[slot, k].astype(F32)
            self.sent[slot, 4 + k] = total.astype(BF16)
            self.copy(slot, 4 + k).start()

    def last(self, slot):
        for m in (2, 3, 4, 5):
            self.copy(slot, m).wait_recv()
        half0 = (
            self.own[slot, :, :256].astype(F32)
            + self.got[slot, 4].astype(F32)
            + self.got[slot, 3].astype(F32)
        )
        half1 = (
            self.own[slot, :, 256:].astype(F32)
            + self.got[slot, 2].astype(F32)
            + self.got[slot, 5].astype(F32)
        )
        return half0, half1

    def drain(self, slot):
        for m in range(6):
            self.copy(slot, m).wait_send()


class Squares:
    def __init__(self, mine, got, send, recv):
        self.mine, self.got, self.send, self.recv = mine, got, send, recv
        self.me, self.right, self.left, self.far = ring()

    def copies(self, slot):
        for m, to in enumerate((self.right, self.left, self.far)):
            yield tp_copy(
                self.mine.at[slot], self.got.at[slot, m],
                self.send.at[slot, m], self.recv.at[slot, m], to,
            )

    def give(self, slot, half0, half1):
        total = jnp.sum(half0 * half0, axis=1, keepdims=True) + jnp.sum(
            half1 * half1, axis=1, keepdims=True
        )
        for g in range(total.shape[0] // 128):
            wide = jnp.broadcast_to(total[128 * g : 128 * g + 128], (128, 128))
            self.mine[slot, 8 * g : 8 * g + 8] = wide.T[:8]
        for copy in self.copies(slot):
            copy.start()

    def take(self, slot):
        for copy in self.copies(slot):
            copy.wait_recv()
        total = self.mine[slot] + self.got[slot, 0] + self.got[slot, 1] + self.got[slot, 2]
        columns = [
            jnp.broadcast_to(total[8 * g : 8 * g + 1], (128, 128)).T[:, :1]
            for g in range(total.shape[0] // 8)
        ]
        return columns[0] if len(columns) == 1 else jnp.concatenate(columns, axis=0)

    def drain(self, slot):
        for copy in self.copies(slot):
            copy.wait_send()


def attend(row, first_key, q_ref, kv, sink_ref, lowest, highest):
    keys, keys_turned, values, values_turned = (
        a[pl.ds(first_key, 3 * WINDOW), :] for a in kv
    )
    lane = lax.broadcasted_iota(jnp.int32, (WINDOW, 128), 1)
    query = lax.broadcasted_iota(jnp.int32, (WINDOW, 3 * WINDOW), 0)
    key = lax.broadcasted_iota(jnp.int32, (WINDOW, 3 * WINDOW), 1)
    inside = (key >= query) & (key <= query + 2 * WINDOW) & (key >= lowest) & (key < highest)
    tiles = []
    for t in range(3):
        pair = q_ref[pl.ds(row, WINDOW), 128 * t : 128 * t + 128].astype(F32) * 0.125
        outs = []
        for half in range(2):
            h = 2 * t + half
            turned = (h // 3) != half
            q = jnp.where((lane >= 64) == (half == 1), pair, 0.0).astype(BF16)
            scores = lax.dot_general(
                q, keys_turned if turned else keys, NT, preferred_element_type=F32
            )
            scores = jnp.where(inside, scores, -1e30)
            sink = sink_ref[h]
            top = jnp.maximum(jnp.max(scores, axis=1, keepdims=True), sink)
            e = jnp.exp(scores - top)
            below = jnp.sum(e, axis=1, keepdims=True) + jnp.exp(sink - top)
            out = jnp.dot(
                e.astype(BF16), values_turned if turned else values,
                preferred_element_type=F32,
            )
            outs.append(out * (1.0 / below))
        tiles.append(jnp.where(lane < 64, outs[0], outs[1]).astype(BF16))
    return jnp.concatenate(tiles, axis=1)


def turn(x):
    return pltpu.roll(x.astype(F32), 64, 1).astype(BF16)


class Weights:
    across = (0, 1, 3, 2)

    def __init__(self, whole, send, recv, core_send, core_recv):
        self.whole, self.send, self.recv = whole, send, recv
        self.core_send, self.core_recv = core_send, core_recv
        sp = lax.axis_index("sp")
        self.core, self.y, self.z = lax.rem(sp, 2), lax.rem(lax.div(sp, 2), 4), lax.div(sp, 8)

    def device(self, way, a, b, core):
        dy, dz = (a, b) if way == 0 else (b, a)
        return (lax.rem(self.z + dz, 4) * 4 + lax.rem(self.y + dy, 4)) * 2 + core

    def neighbours(self):
        ring = [self.device(0, a, b, self.core) for a, b in ((1, 0), (3, 0), (0, 1), (0, 3))]
        return ring + [self.device(0, 0, 0, 1 - self.core)]

    def rows(self, way, a, b, core, part=None):
        start = self.device(way, a, b, core) * 64 + 32 * way
        if part is None:
            return self.whole.at[pl.ds(pl.multiple_of(start, 32), 32), :]
        return self.whole.at[pl.ds(pl.multiple_of(start + 16 * part, 16), 16), :]

    def at(self, stage, k):
        return (k, 0) if stage == 0 else (self.across[stage - 1], k)

    def copy(self, way, stage, m, incoming=False):
        offset = ((3, 1, 2, 2) if incoming else (0, 0, 3, 1))[m]
        ref = self.rows(way, *self.at(stage, offset), self.core, None if m < 2 else m - 2)
        to = self.device(way, *((1 if m % 2 == 0 else 3, 0) if stage == 0 else (0, 1 if m % 2 == 0 else 3)), self.core)
        return pltpu.make_async_remote_copy(
            src_ref=ref, dst_ref=ref,
            send_sem=self.send.at[way, stage, m], recv_sem=self.recv.at[way, stage, m],
            device_id={"sp": to}, device_id_type=MESH,
        )

    def over(self, way, a, b, incoming=False):
        ref = self.rows(way, a, b, 1 - self.core if incoming else self.core)
        return pltpu.make_async_remote_copy(
            src_ref=ref, dst_ref=ref,
            send_sem=self.core_send.at[way, 4 * a + b], recv_sem=self.core_recv.at[way, 4 * a + b],
            device_id={"sp": self.device(way, 0, 0, 1 - self.core)}, device_id_type=MESH,
        )

    def open(self, way, stage):
        self.copy(way, stage, 0).start()
        self.copy(way, stage, 1).start()

    def relay(self, way, stage):
        for m in (0, 1):
            self.copy(way, stage, m, True).wait_recv()
            self.copy(way, stage, m + 2).start()

    def share(self, way, stage, ks):
        for k in ks:
            self.over(way, *self.at(stage, k)).start()

    def close(self, way, stage):
        for m in (2, 3):
            self.copy(way, stage, m, True).wait_recv()
        self.share(way, stage, (2,))

    def step(self, n):
        for way in (0, 1):
            if n == 0:
                self.open(way, 0)
            elif n == 1:
                self.relay(way, 0)
        for way in (0, 1):
            if n == 0:
                self.open(way, 1)
                self.over(way, 0, 0).start()
            elif n == 1:
                self.open(way, 2)
                self.open(way, 3)
                self.share(way, 0, (1, 3))
            elif n == 2:
                self.relay(way, 1)
                self.share(way, 1, (1, 3))
            elif n == 3:
                self.close(way, 0)
                self.open(way, 4)
            elif n == 4:
                for stage in (2, 3):
                    self.relay(way, stage)
                    self.share(way, stage, (1, 3))
            elif n == 5:
                self.close(way, 1)
                self.relay(way, 4)
                self.share(way, 4, (1, 3))
            elif n == 6:
                for stage in (2, 3, 4):
                    self.close(way, stage)
            elif n == 7:
                for a in range(4):
                    for b in range(4):
                        self.over(way, a, b, True).wait_recv()

    def drain(self):
        for way in (0, 1):
            for stage in range(5):
                for m in range(4):
                    self.copy(way, stage, m).wait_send()
            for a in range(4):
                for b in range(4):
                    self.over(way, a, b).wait_send()


def layer_kernel(
    chunks, sp_count,
    res_hbm, q_hbm, k_hbm, v_hbm, sink_ref, proj_hbm, gain_mix_ref, gain_pre_ref, gain_post_ref,
    gate_hbm, up_hbm, down_hbm,
    out_ref,
    res_ref, q_ref, k_ref, v_ref, proj_ref, gate_ref, up_ref, down_ref,
    whole, keys, keys_turned, values, values_turned, att,
    sent, got, own, mixed, mine, squares, rows,
    normed, hidden, f_sent, f_got, f_own, f_total, f_mine, f_squares,
    load_sem, w_send, w_recv, core_send, core_recv,
    halo_send, halo_recv, rs_send, rs_recv, sq_send, sq_recv, ag_send, ag_recv,
    f_rs_send, f_rs_recv, f_sq_send, f_sq_recv,
):
    me, right, left, far = ring()
    sp = lax.axis_index("sp")
    after = lax.rem(sp + 1, sp_count)
    before = lax.rem(sp + sp_count - 1, sp_count)
    length = chunks * WINDOW
    half_chunks = chunks // 2
    units = gate_ref.shape[1]
    tiles = units // 128
    inner = 2 * units
    loads = [
        pltpu.make_async_copy(a, b, load_sem.at[n])
        for n, (a, b) in enumerate((
            (gate_hbm, gate_ref), (up_hbm, up_ref), (down_hbm, down_ref), (k_hbm, k_ref),
            (v_hbm, v_ref), (q_hbm, q_ref), (proj_hbm, proj_ref), (res_hbm, res_ref),
        ))
    ]
    for load in loads:
        load.start()
    weights = Weights(whole, w_send, w_recv, core_send, core_recv)
    barrier = pltpu.get_barrier_semaphore()
    others = [{"tp": right}, {"tp": left}, {"tp": far}, {"sp": after}, {"sp": before}]
    others += [{"sp": n} for n in weights.neighbours()]
    for other in others:
        pl.semaphore_signal(barrier, inc=1, device_id=other, device_id_type=MESH)
    for load in loads[:3]:
        load.wait()
    shard = pl.ds(pl.multiple_of(sp * 64, 64), 64)
    for j in range(tiles):
        whole[shard, 256 * j : 256 * j + 128] = gate_ref[:, 128 * j : 128 * j + 128]
        whole[shard, 256 * j + 128 : 256 * j + 256] = up_ref[:, 128 * j : 128 * j + 128]
        whole[shard, inner + 128 * j : inner + 128 * j + 128] = (
            down_ref[128 * j : 128 * j + 128, :].astype(F32).T.astype(BF16)
        )
    for load in loads[3:5]:
        load.wait()
    pl.semaphore_wait(barrier, len(others))

    def halo(n):
        mine_ref, both = ((k_ref, keys), (v_ref, values))[n // 2]
        if n % 2 == 0:
            src, dst, to = mine_ref.at[pl.ds(length - WINDOW, WINDOW)], both.at[pl.ds(0, WINDOW)], after
        else:
            src, dst, to = mine_ref.at[pl.ds(0, WINDOW)], both.at[pl.ds(length + WINDOW, WINDOW)], before
        return pltpu.make_async_remote_copy(
            src_ref=src, dst_ref=dst, send_sem=halo_send.at[n], recv_sem=halo_recv.at[n],
            device_id={"sp": to}, device_id_type=MESH,
        )

    for n in range(4):
        halo(n).start()
    weights.step(0)
    middle = pl.ds(WINDOW, length)
    keys[middle, :] = k_ref[...]
    values[middle, :] = v_ref[...]
    keys_turned[middle, :] = turn(k_ref[...])
    values_turned[middle, :] = turn(v_ref[...])
    for load in loads[5:]:
        load.wait()

    scatter = Scatter(sent, got, own, rs_send, rs_recv)
    sums = Squares(mine, squares, sq_send, sq_recv)
    f_scatter = Scatter(f_sent, f_got, f_own, f_rs_send, f_rs_recv)
    f_sums = Squares(f_mine, f_squares, f_sq_send, f_sq_recv)
    columns = pl.ds(pl.multiple_of(me * 512, 512), 512)
    gain_mix = gain_mix_ref[:, columns]
    gain_post = gain_post_ref[:, columns]

    def place(slot):
        return pl.multiple_of(lax.rem(slot + 1, chunks) * WINDOW, WINDOW)

    def gather(slot, m):
        owner, to, part = (
            (me, right, pl.ds(0, 512)), (me, left, pl.ds(0, 512)),
            (left, right, pl.ds(0, 256)), (right, left, pl.ds(256, 256)),
        )[m]
        ref = rows.at[owner, slot, :, part]
        return tp_copy(ref, ref, ag_send.at[slot, m], ag_recv.at[slot, m], to)

    def arrived(slot, m):
        owner, part = (
            (left, pl.ds(0, 512)), (right, pl.ds(0, 512)),
            (far, pl.ds(0, 256)), (far, pl.ds(256, 256)),
        )[m]
        ref = rows.at[owner, slot, :, part]
        tp_copy(ref, ref, ag_send.at[slot, m], ag_recv.at[slot, m], right).wait_recv()

    def attention(t):
        @pl.when(t == chunks - 2)
        def _():
            for n in range(4):
                halo(n).wait_recv()
            for at in (0, length + WINDOW):
                keys_turned[pl.ds(at, WINDOW), :] = turn(keys[pl.ds(at, WINDOW), :])
                values_turned[pl.ds(at, WINDOW), :] = turn(values[pl.ds(at, WINDOW), :])

        row = place(t)
        lowest = jnp.where((sp == 0) & (t == chunks - 1), WINDOW, 0)
        highest = jnp.where((sp == sp_count - 1) & (t == chunks - 2), 2 * WINDOW, 3 * WINDOW)
        att[...] = attend(
            row, row, q_ref, (keys, keys_turned, values, values_turned), sink_ref, lowest, highest
        )

        def part(block, half):
            at = pl.ds(pl.multiple_of(block * 512 + 256 * half, 256), 256)
            return jnp.dot(att[...], proj_ref[:, at], preferred_element_type=F32).astype(BF16)

        scatter.first(t, part)

    def mix(s):
        half0, half1 = scatter.last(s)
        mixed[s, :, :256] = half0
        mixed[s, :, 256:] = half1
        sums.give(s, half0, half1)

    def first_rows(s):
        scale = lax.rsqrt(sums.take(s) / 2048.0 + EPS)
        res = res_ref[pl.ds(place(s), WINDOW), :].astype(F32)
        rows[me, s] = (res + mixed[s] * scale * gain_mix).astype(BF16)
        gather(s, 0).start()
        gather(s, 1).start()

    def relay(s):
        for m in (0, 1):
            arrived(s, m)
            gather(s, m + 2).start()

    def feed(u):
        for k in range(2):
            squared = jnp.zeros((WINDOW, 1), F32)
            for b in range(4):
                x = rows[b, 2 * u + k].astype(F32)
                squared += jnp.sum(x * x, axis=1, keepdims=True)
            scale = lax.rsqrt(squared / 2048.0 + EPS)
            for b in range(4):
                x = rows[b, 2 * u + k].astype(F32)
                normed[WINDOW * k : WINDOW * k + WINDOW, 512 * b : 512 * b + 512] = (
                    x * scale * gain_pre_ref[:, 512 * b : 512 * b + 512]
                ).astype(BF16)

        def tile(j, carry):
            both = jnp.dot(
                normed[...], whole[:, pl.ds(pl.multiple_of(j * 256, 256), 256)],
                preferred_element_type=F32,
            )
            gate, up = both[:, :128], both[:, 128:]
            hidden[:, pl.ds(pl.multiple_of(j * 128, 128), 128)] = (
                gate / (1.0 + jnp.exp(-gate)) * up
            ).astype(BF16)
            return carry

        lax.fori_loop(0, tiles, tile, 0)

        def part(block, half):
            at = pl.ds(pl.multiple_of(block * 512 + 256 * half, 256), 256)
            return lax.dot_general(
                hidden[...], whole[at, inner : inner + units], NT, preferred_element_type=F32
            ).astype(BF16)

        f_scatter.first(u, part)

    def feed_sum(u):
        half0, half1 = f_scatter.last(u)
        f_total[u, :, :256] = half0
        f_total[u, :, 256:] = half1
        f_sums.give(u, half0, half1)

    def finish(u):
        scale = lax.rsqrt(f_sums.take(u) / 2048.0 + EPS)
        for k in range(2):
            part = pl.ds(WINDOW * k, WINDOW)
            out_ref[pl.ds(place(2 * u + k), WINDOW), :] = (
                rows[me, 2 * u + k].astype(F32)
                + 0.5 * (f_total[u, part, :] * scale[WINDOW * k : WINDOW * k + WINDOW] * gain_post)
            ).astype(BF16)

    def step(t, carry):
        def when(lag, fn):
            @pl.when((t >= lag) & (t < chunks + lag))
            def _():
                fn(t - lag)

        def when_fed(lag, fn):
            begin = FEED_AT + lag

            @pl.when((t >= begin) & (t < begin + chunks) & (lax.rem(t - begin + chunks, 2) == 0))
            def _():
                fn(lax.div(t - begin, 2))

        when(0, attention)
        when(1, scatter.second)
        when_fed(1, f_scatter.second)
        when(2, mix)
        when_fed(2, feed_sum)
        when(3, first_rows)
        when(4, relay)
        when_fed(3, finish)

        @pl.when((t >= 5) & (t < chunks + 5))
        def _():
            arrived(t - 5, 2)
            arrived(t - 5, 3)

        for n in range(1, 8):
            @pl.when(t == n)
            def _():
                weights.step(n)

        when_fed(0, feed)
        return carry

    lax.fori_loop(0, FEED_AT + chunks + 2, step, 0)

    for n in range(4):
        halo(n).wait_send()
    weights.drain()

    def drain(slot, carry):
        scatter.drain(slot)
        sums.drain(slot)
        for m in range(4):
            gather(slot, m).wait_send()
        return carry

    lax.fori_loop(0, chunks, drain, 0)

    def f_drain(slot, carry):
        f_scatter.drain(slot)
        f_sums.drain(slot)
        return carry

    lax.fori_loop(0, half_chunks, f_drain, 0)


def sems(*shapes):
    return [pltpu.SemaphoreType.DMA(s) for s in shapes]


def body(
    residual, rotated_query_rows, rotated_key_rows, value_matrix_rows, head_sink_logit,
    out_proj, gain_mix, gain_pre, gain_post, gate_proj, up_proj, down_proj,
):
    length = residual.shape[0]
    chunks = length // WINDOW
    half = chunks // 2
    units = gate_proj.shape[1]
    sp_count = lax.axis_size("sp")
    full = sp_count * gate_proj.shape[0]
    big = 2 * WINDOW
    vmem = pl.BlockSpec(memory_space=pltpu.VMEM)
    smem = pl.BlockSpec(memory_space=pltpu.SMEM)
    hbm = pl.BlockSpec(memory_space=pl.ANY)
    loaded = (
        residual, rotated_query_rows, rotated_key_rows, value_matrix_rows, out_proj,
        gate_proj, up_proj, down_proj,
    )
    return pl.pallas_call(
        functools.partial(layer_kernel, chunks, sp_count),
        out_shape=jax.ShapeDtypeStruct(residual.shape, BF16),
        in_specs=[hbm] * 4 + [smem, hbm] + [vmem] * 3 + [hbm] * 3,
        out_specs=vmem,
        scratch_shapes=[pltpu.VMEM(a.shape, BF16) for a in loaded]
        + [pltpu.VMEM((full, 3 * units), BF16)]
        + [pltpu.VMEM((length + big, 128), BF16)] * 4
        + [
            pltpu.VMEM((WINDOW, 384), BF16),
            pltpu.VMEM((chunks, 6, WINDOW, 256), BF16),
            pltpu.VMEM((chunks, 6, WINDOW, 256), BF16),
            pltpu.VMEM((chunks, WINDOW, 512), BF16),
            pltpu.VMEM((chunks, WINDOW, 512), F32),
            pltpu.VMEM((chunks, 8, 128), F32),
            pltpu.VMEM((chunks, 3, 8, 128), F32),
            pltpu.VMEM((4, chunks, WINDOW, 512), BF16),
            pltpu.VMEM((big, full), BF16),
            pltpu.VMEM((big, units), BF16),
            pltpu.VMEM((half, 6, big, 256), BF16),
            pltpu.VMEM((half, 6, big, 256), BF16),
            pltpu.VMEM((half, big, 512), BF16),
            pltpu.VMEM((half, big, 512), F32),
            pltpu.VMEM((half, 16, 128), F32),
            pltpu.VMEM((half, 3, 16, 128), F32),
        ]
        + sems((8,), (2, 5, 4), (2, 5, 4), (2, 16), (2, 16))
        + sems((4,), (4,), (chunks, 6), (chunks, 6), (chunks, 3), (chunks, 3), (chunks, 4), (chunks, 4))
        + sems((half, 6), (half, 6), (half, 3), (half, 3)),
        compiler_params=pltpu.CompilerParams(
            collective_id=0, has_side_effects=True, vmem_limit_bytes=63 * 2**20
        ),
    )(
        residual, rotated_query_rows, rotated_key_rows, value_matrix_rows, head_sink_logit,
        out_proj, gain_mix[None], gain_pre[None], gain_post[None], gate_proj, up_proj, down_proj,
    )


def solution(mesh):
    placed = (
        P("sp", "tp"), P("sp", "tp"), P("sp", "tp"), P("sp", "tp"), P("tp"), P("tp", None),
        P(), P(), P(), P("sp", "tp"), P("sp", "tp"), P("tp", "sp"),
    )
    return jax.shard_map(body, mesh=mesh, in_specs=placed, out_specs=P("sp", "tp"), check_vma=False)
```

```python
import functools

import jax
import jax.numpy as jnp
from jax import lax
from jax.experimental import pallas as pl
from jax.experimental.pallas import tpu as pltpu
from jax.sharding import PartitionSpec as P

WINDOW = 128
EPS = 1e-06
FEED, SECOND, SUM, FINISH = (8, 9, 10, 12), (9, 10, 11, 13), (10, 11, 12, 14), (11, 12, 13, 15)
MESH = pl.DeviceIdType.MESH
F32 = jnp.float32
BF16 = jnp.bfloat16
NT = (((1,), (1,)), ((), ()))


def ring():
    me = lax.axis_index("tp")
    right, left, far = (lax.rem(me + k, 4) for k in (1, 3, 2))
    return me, right, left, far


def tp_copy(src, dst, send, recv, to):
    return pltpu.make_async_remote_copy(
        src_ref=src, dst_ref=dst, send_sem=send, recv_sem=recv,
        device_id={"tp": to}, device_id_type=MESH,
    )


class Scatter:
    def __init__(self, sent, got, own, send, recv):
        self.sent, self.got, self.own, self.send, self.recv = sent, got, own, send, recv
        self.me, self.right, self.left, self.far = ring()

    def copy(self, slot, m):
        to = self.right if m % 2 == 0 else self.left
        return tp_copy(
            self.sent.at[slot, m], self.got.at[slot, m],
            self.send.at[slot, m], self.recv.at[slot, m], to,
        )

    def first(self, slot, part):
        self.sent[slot, 0] = part(self.far, 0)
        self.sent[slot, 1] = part(self.far, 1)
        self.copy(slot, 0).start()
        self.copy(slot, 1).start()
        self.sent[slot, 2] = part(self.right, 1)
        self.sent[slot, 3] = part(self.left, 0)
        self.copy(slot, 2).start()
        self.copy(slot, 3).start()
        self.sent[slot, 4] = part(self.right, 0)
        self.sent[slot, 5] = part(self.left, 1)
        self.own[slot, :, :256] = part(self.me, 0)
        self.own[slot, :, 256:] = part(self.me, 1)

    def second(self, slot):
        for k in (0, 1):
            self.copy(slot, k).wait_recv()
            total = self.sent[slot, 4 + k].astype(F32) + self.got[slot, k].astype(F32)
            self.sent[slot, 4 + k] = total.astype(BF16)
            self.copy(slot, 4 + k).start()

    def last(self, slot):
        for m in (2, 3, 4, 5):
            self.copy(slot, m).wait_recv()
        half0 = (
            self.own[slot, :, :256].astype(F32)
            + self.got[slot, 4].astype(F32)
            + self.got[slot, 3].astype(F32)
        )
        half1 = (
            self.own[slot, :, 256:].astype(F32)
            + self.got[slot, 2].astype(F32)
            + self.got[slot, 5].astype(F32)
        )
        return half0, half1

    def drain(self, slot):
        for m in range(6):
            self.copy(slot, m).wait_send()


class Squares:
    def __init__(self, mine, got, send, recv):
        self.mine, self.got, self.send, self.recv = mine, got, send, recv
        self.me, self.right, self.left, self.far = ring()

    def copies(self, slot):
        for m, to in enumerate((self.right, self.left, self.far)):
            yield tp_copy(
                self.mine.at[slot], self.got.at[slot, m],
                self.send.at[slot, m], self.recv.at[slot, m], to,
            )

    def give(self, slot, half0, half1):
        total = jnp.sum(half0 * half0, axis=1, keepdims=True) + jnp.sum(
            half1 * half1, axis=1, keepdims=True
        )
        for g in range(total.shape[0] // 128):
            wide = jnp.broadcast_to(total[128 * g : 128 * g + 128], (128, 128))
            self.mine[slot, 8 * g : 8 * g + 8] = wide.T[:8]
        for copy in self.copies(slot):
            copy.start()

    def take(self, slot):
        for copy in self.copies(slot):
            copy.wait_recv()
        total = self.mine[slot] + self.got[slot, 0] + self.got[slot, 1] + self.got[slot, 2]
        columns = [
            jnp.broadcast_to(total[8 * g : 8 * g + 1], (128, 128)).T[:, :1]
            for g in range(total.shape[0] // 8)
        ]
        return columns[0] if len(columns) == 1 else jnp.concatenate(columns, axis=0)

    def drain(self, slot):
        for copy in self.copies(slot):
            copy.wait_send()


def attend(row, first_key, q_ref, kv, sink_ref, lowest, highest):
    keys, keys_turned, values, values_turned = (
        a[pl.ds(first_key, 3 * WINDOW), :] for a in kv
    )
    lane = lax.broadcasted_iota(jnp.int32, (WINDOW, 128), 1)
    query = lax.broadcasted_iota(jnp.int32, (WINDOW, 3 * WINDOW), 0)
    key = lax.broadcasted_iota(jnp.int32, (WINDOW, 3 * WINDOW), 1)
    inside = (key >= query) & (key <= query + 2 * WINDOW) & (key >= lowest) & (key < highest)
    tiles = []
    for t in range(3):
        pair = q_ref[pl.ds(row, WINDOW), 128 * t : 128 * t + 128].astype(F32) * 0.125
        outs = []
        for half in range(2):
            h = 2 * t + half
            turned = (h // 3) != half
            q = jnp.where((lane >= 64) == (half == 1), pair, 0.0).astype(BF16)
            scores = lax.dot_general(
                q, keys_turned if turned else keys, NT, preferred_element_type=F32
            )
            scores = jnp.where(inside, scores, -1e30)
            sink = sink_ref[h]
            top = jnp.maximum(jnp.max(scores, axis=1, keepdims=True), sink)
            e = jnp.exp(scores - top)
            below = jnp.sum(e, axis=1, keepdims=True) + jnp.exp(sink - top)
            out = jnp.dot(
                e.astype(BF16), values_turned if turned else values,
                preferred_element_type=F32,
            )
            outs.append(out * (1.0 / below))
        tiles.append(jnp.where(lane < 64, outs[0], outs[1]).astype(BF16))
    return jnp.concatenate(tiles, axis=1)


def turn(x):
    return pltpu.roll(x.astype(F32), 64, 1).astype(BF16)


class Weights:
    across = (0, 1, 3, 2)

    def __init__(self, whole, send, recv, core_send, core_recv):
        self.whole, self.send, self.recv = whole, send, recv
        self.core_send, self.core_recv = core_send, core_recv
        sp = lax.axis_index("sp")
        self.core, self.y, self.z = lax.rem(sp, 2), lax.rem(lax.div(sp, 2), 4), lax.div(sp, 8)

    def device(self, way, a, b, core):
        dy, dz = (a, b) if way == 0 else (b, a)
        return (lax.rem(self.z + dz, 4) * 4 + lax.rem(self.y + dy, 4)) * 2 + core

    def neighbours(self):
        ring = [self.device(0, a, b, self.core) for a, b in ((1, 0), (3, 0), (0, 1), (0, 3))]
        return ring + [self.device(0, 0, 0, 1 - self.core)]

    def rows(self, way, a, b, core, part=None):
        start = self.device(way, a, b, core) * 64 + 32 * way
        if part is None:
            return self.whole.at[pl.ds(pl.multiple_of(start, 32), 32), :]
        return self.whole.at[pl.ds(pl.multiple_of(start + 16 * part, 16), 16), :]

    def at(self, stage, k):
        return (k, 0) if stage == 0 else (self.across[stage - 1], k)

    def copy(self, way, stage, m, incoming=False):
        offset = ((3, 1, 2, 2) if incoming else (0, 0, 3, 1))[m]
        ref = self.rows(way, *self.at(stage, offset), self.core, None if m < 2 else m - 2)
        to = self.device(way, *((1 if m % 2 == 0 else 3, 0) if stage == 0 else (0, 1 if m % 2 == 0 else 3)), self.core)
        return pltpu.make_async_remote_copy(
            src_ref=ref, dst_ref=ref,
            send_sem=self.send.at[way, stage, m], recv_sem=self.recv.at[way, stage, m],
            device_id={"sp": to}, device_id_type=MESH,
        )

    def over(self, way, a, b, incoming=False):
        ref = self.rows(way, a, b, 1 - self.core if incoming else self.core)
        return pltpu.make_async_remote_copy(
            src_ref=ref, dst_ref=ref,
            send_sem=self.core_send.at[way, 4 * a + b], recv_sem=self.core_recv.at[way, 4 * a + b],
            device_id={"sp": self.device(way, 0, 0, 1 - self.core)}, device_id_type=MESH,
        )

    def open(self, way, stage):
        self.copy(way, stage, 0).start()
        self.copy(way, stage, 1).start()

    def relay(self, way, stage):
        for m in (0, 1):
            self.copy(way, stage, m, True).wait_recv()
            self.copy(way, stage, m + 2).start()

    def share(self, way, stage, ks):
        for k in ks:
            self.over(way, *self.at(stage, k)).start()

    def close(self, way, stage):
        for m in (2, 3):
            self.copy(way, stage, m, True).wait_recv()
        self.share(way, stage, (2,))

    def step(self, n):
        for way in (0, 1):
            if n == 0:
                self.open(way, 0)
            elif n == 1:
                self.relay(way, 0)
        for way in (0, 1):
            if n == 0:
                self.open(way, 1)
                self.over(way, 0, 0).start()
            elif n == 1:
                self.open(way, 2)
                self.open(way, 3)
                self.share(way, 0, (1, 3))
            elif n == 2:
                self.relay(way, 1)
                self.share(way, 1, (1, 3))
            elif n == 3:
                self.close(way, 0)
                self.open(way, 4)
            elif n == 4:
                for stage in (2, 3):
                    self.relay(way, stage)
                    self.share(way, stage, (1, 3))
            elif n == 5:
                self.close(way, 1)
                self.relay(way, 4)
                self.share(way, 4, (1, 3))
            elif n == 6:
                for stage in (2, 3, 4):
                    self.close(way, stage)
            elif n == 7:
                for a in range(4):
                    for b in range(4):
                        self.over(way, a, b, True).wait_recv()

    def drain(self):
        for way in (0, 1):
            for stage in range(5):
                for m in range(4):
                    self.copy(way, stage, m).wait_send()
            for a in range(4):
                for b in range(4):
                    self.over(way, a, b).wait_send()


def layer_kernel(
    chunks, sp_count,
    res_hbm, q_hbm, k_hbm, v_hbm, sink_ref, proj_hbm, gain_mix_ref, gain_pre_ref, gain_post_ref,
    gate_hbm, up_hbm, down_hbm,
    out_ref,
    res_ref, q_ref, k_ref, v_ref, proj_ref, gate_ref, up_ref, down_ref,
    whole, keys, keys_turned, values, values_turned, att,
    sent, got, own, mixed, mine, squares, rows,
    normed, hidden, f_sent, f_got, f_own, f_total, f_mine, f_squares,
    load_sem, w_send, w_recv, core_send, core_recv,
    halo_send, halo_recv, rs_send, rs_recv, sq_send, sq_recv, ag_send, ag_recv,
    f_rs_send, f_rs_recv, f_sq_send, f_sq_recv,
):
    me, right, left, far = ring()
    sp = lax.axis_index("sp")
    after = lax.rem(sp + 1, sp_count)
    before = lax.rem(sp + sp_count - 1, sp_count)
    length = chunks * WINDOW
    half_chunks = chunks // 2
    units = gate_ref.shape[1]
    tiles = units // 128
    inner = 2 * units
    loads = [
        pltpu.make_async_copy(a, b, load_sem.at[n])
        for n, (a, b) in enumerate((
            (gate_hbm, gate_ref), (up_hbm, up_ref), (down_hbm, down_ref), (k_hbm, k_ref),
            (v_hbm, v_ref), (q_hbm, q_ref), (proj_hbm, proj_ref), (res_hbm, res_ref),
        ))
    ]
    for load in loads:
        load.start()
    weights = Weights(whole, w_send, w_recv, core_send, core_recv)
    barrier = pltpu.get_barrier_semaphore()
    others = [{"tp": right}, {"tp": left}, {"tp": far}, {"sp": after}, {"sp": before}]
    others += [{"sp": n} for n in weights.neighbours()]
    for other in others:
        pl.semaphore_signal(barrier, inc=1, device_id=other, device_id_type=MESH)
    for load in loads[:3]:
        load.wait()
    shard = pl.ds(pl.multiple_of(sp * 64, 64), 64)
    for j in range(tiles):
        whole[shard, 256 * j : 256 * j + 128] = gate_ref[:, 128 * j : 128 * j + 128]
        whole[shard, 256 * j + 128 : 256 * j + 256] = up_ref[:, 128 * j : 128 * j + 128]
        whole[shard, inner + 128 * j : inner + 128 * j + 128] = (
            down_ref[:, 128 * j : 128 * j + 128]
        )
    for load in loads[3:5]:
        load.wait()
    pl.semaphore_wait(barrier, len(others))

    def halo(n):
        mine_ref, both = ((k_ref, keys), (v_ref, values))[n // 2]
        if n % 2 == 0:
            src, dst, to = mine_ref.at[pl.ds(length - WINDOW, WINDOW)], both.at[pl.ds(0, WINDOW)], after
        else:
            src, dst, to = mine_ref.at[pl.ds(0, WINDOW)], both.at[pl.ds(length + WINDOW, WINDOW)], before
        return pltpu.make_async_remote_copy(
            src_ref=src, dst_ref=dst, send_sem=halo_send.at[n], recv_sem=halo_recv.at[n],
            device_id={"sp": to}, device_id_type=MESH,
        )

    for n in range(4):
        halo(n).start()
    weights.step(0)
    middle = pl.ds(WINDOW, length)
    keys[middle, :] = k_ref[...]
    values[middle, :] = v_ref[...]
    keys_turned[middle, :] = turn(k_ref[...])
    values_turned[middle, :] = turn(v_ref[...])
    for load in loads[5:]:
        load.wait()

    scatter = Scatter(sent, got, own, rs_send, rs_recv)
    sums = Squares(mine, squares, sq_send, sq_recv)
    f_scatter = Scatter(f_sent, f_got, f_own, f_rs_send, f_rs_recv)
    f_sums = Squares(f_mine, f_squares, f_sq_send, f_sq_recv)
    columns = pl.ds(pl.multiple_of(me * 512, 512), 512)
    gain_mix = gain_mix_ref[:, columns]
    gain_post = gain_post_ref[:, columns]

    def place(slot):
        return pl.multiple_of(lax.rem(slot + 1, chunks) * WINDOW, WINDOW)

    def gather(slot, m):
        owner, to, part = (
            (me, right, pl.ds(0, 512)), (me, left, pl.ds(0, 512)),
            (left, right, pl.ds(0, 256)), (right, left, pl.ds(256, 256)),
        )[m]
        ref = rows.at[owner, slot, :, part]
        return tp_copy(ref, ref, ag_send.at[slot, m], ag_recv.at[slot, m], to)

    def arrived(slot, m):
        owner, part = (
            (left, pl.ds(0, 512)), (right, pl.ds(0, 512)),
            (far, pl.ds(0, 256)), (far, pl.ds(256, 256)),
        )[m]
        ref = rows.at[owner, slot, :, part]
        tp_copy(ref, ref, ag_send.at[slot, m], ag_recv.at[slot, m], right).wait_recv()

    def attention(t):
        @pl.when(t == chunks - 2)
        def _():
            for n in range(4):
                halo(n).wait_recv()
            for at in (0, length + WINDOW):
                keys_turned[pl.ds(at, WINDOW), :] = turn(keys[pl.ds(at, WINDOW), :])
                values_turned[pl.ds(at, WINDOW), :] = turn(values[pl.ds(at, WINDOW), :])

        row = place(t)
        lowest = jnp.where((sp == 0) & (t == chunks - 1), WINDOW, 0)
        highest = jnp.where((sp == sp_count - 1) & (t == chunks - 2), 2 * WINDOW, 3 * WINDOW)
        att[...] = attend(
            row, row, q_ref, (keys, keys_turned, values, values_turned), sink_ref, lowest, highest
        )

        def part(block, half):
            at = pl.ds(pl.multiple_of(block * 512 + 256 * half, 256), 256)
            return jnp.dot(att[...], proj_ref[:, at], preferred_element_type=F32).astype(BF16)

        scatter.first(t, part)

    def mix(s):
        half0, half1 = scatter.last(s)
        mixed[s, :, :256] = half0
        mixed[s, :, 256:] = half1
        sums.give(s, half0, half1)

    def first_rows(s):
        scale = lax.rsqrt(sums.take(s) / 2048.0 + EPS)
        res = res_ref[pl.ds(place(s), WINDOW), :].astype(F32)
        rows[me, s] = (res + mixed[s] * scale * gain_mix).astype(BF16)
        gather(s, 0).start()
        gather(s, 1).start()

    def relay(s):
        for m in (0, 1):
            arrived(s, m)
            gather(s, m + 2).start()

    def feed(u):
        for k in range(2):
            squared = jnp.zeros((WINDOW, 1), F32)
            for b in range(4):
                x = rows[b, 2 * u + k].astype(F32)
                squared += jnp.sum(x * x, axis=1, keepdims=True)
            scale = lax.rsqrt(squared / 2048.0 + EPS)
            for b in range(4):
                x = rows[b, 2 * u + k].astype(F32)
                normed[WINDOW * k : WINDOW * k + WINDOW, 512 * b : 512 * b + 512] = (
                    x * scale * gain_pre_ref[:, 512 * b : 512 * b + 512]
                ).astype(BF16)

        for j in range(tiles):
            both = jnp.dot(
                normed[...], whole[:, 256 * j : 256 * j + 256], preferred_element_type=F32
            )
            gate, up = both[:, :128], both[:, 128:]
            hidden[:, 128 * j : 128 * j + 128] = (gate / (1.0 + jnp.exp(-gate)) * up).astype(BF16)

        def part(block, half):
            at = pl.ds(pl.multiple_of(block * 512 + 256 * half, 256), 256)
            return lax.dot_general(
                hidden[...], whole[at, inner : inner + units], NT, preferred_element_type=F32
            ).astype(BF16)

        f_scatter.first(u, part)

    def feed_sum(u):
        half0, half1 = f_scatter.last(u)
        f_total[u, :, :256] = half0
        f_total[u, :, 256:] = half1
        f_sums.give(u, half0, half1)

    def finish(u):
        scale = lax.rsqrt(f_sums.take(u) / 2048.0 + EPS)
        for k in range(2):
            part = pl.ds(WINDOW * k, WINDOW)
            out_ref[pl.ds(place(2 * u + k), WINDOW), :] = (
                rows[me, 2 * u + k].astype(F32)
                + 0.5 * (f_total[u, part, :] * scale[WINDOW * k : WINDOW * k + WINDOW] * gain_post)
            ).astype(BF16)

    def step(t, carry):
        def when(lag, fn):
            @pl.when((t >= lag) & (t < chunks + lag))
            def _():
                fn(t - lag)

        def when_fed(times, fn):
            now, index = t == times[0], 0
            for n in times[1:]:
                now, index = now | (t == n), index + (t >= n).astype(jnp.int32)

            @pl.when(now)
            def _():
                fn(index)

        when(0, attention)
        when(1, scatter.second)
        when(2, mix)
        when(3, first_rows)
        when(4, relay)

        @pl.when((t >= 5) & (t < chunks + 5))
        def _():
            arrived(t - 5, 2)
            arrived(t - 5, 3)

        for n in range(1, 8):
            @pl.when(t == n)
            def _():
                weights.step(n)

        when_fed(FEED, feed)
        when_fed(SECOND, f_scatter.second)
        when_fed(SUM, feed_sum)
        when_fed(FINISH, finish)
        return carry

    lax.fori_loop(0, FINISH[-1] + 1, step, 0)

    for n in range(4):
        halo(n).wait_send()
    weights.drain()

    def drain(slot, carry):
        scatter.drain(slot)
        sums.drain(slot)
        for m in range(4):
            gather(slot, m).wait_send()
        return carry

    lax.fori_loop(0, chunks, drain, 0)

    def f_drain(slot, carry):
        f_scatter.drain(slot)
        f_sums.drain(slot)
        return carry

    lax.fori_loop(0, half_chunks, f_drain, 0)


def sems(*shapes):
    return [pltpu.SemaphoreType.DMA(s) for s in shapes]


def body(
    residual, rotated_query_rows, rotated_key_rows, value_matrix_rows, head_sink_logit,
    out_proj, gain_mix, gain_pre, gain_post, gate_proj, up_proj, down_proj,
):
    length = residual.shape[0]
    chunks = length // WINDOW
    half = chunks // 2
    units = gate_proj.shape[1]
    sp_count = lax.axis_size("sp")
    full = sp_count * gate_proj.shape[0]
    big = 2 * WINDOW
    vmem = pl.BlockSpec(memory_space=pltpu.VMEM)
    smem = pl.BlockSpec(memory_space=pltpu.SMEM)
    hbm = pl.BlockSpec(memory_space=pl.ANY)
    loaded = (
        residual, rotated_query_rows, rotated_key_rows, value_matrix_rows, out_proj,
        gate_proj, up_proj, down_proj.T,
    )
    return pl.pallas_call(
        functools.partial(layer_kernel, chunks, sp_count),
        out_shape=jax.ShapeDtypeStruct(residual.shape, BF16),
        in_specs=[hbm] * 4 + [smem, hbm] + [vmem] * 3 + [hbm] * 3,
        out_specs=vmem,
        scratch_shapes=[pltpu.VMEM(a.shape, BF16) for a in loaded]
        + [pltpu.VMEM((full, 3 * units), BF16)]
        + [pltpu.VMEM((length + big, 128), BF16)] * 4
        + [
            pltpu.VMEM((WINDOW, 384), BF16),
            pltpu.VMEM((chunks, 6, WINDOW, 256), BF16),
            pltpu.VMEM((chunks, 6, WINDOW, 256), BF16),
            pltpu.VMEM((chunks, WINDOW, 512), BF16),
            pltpu.VMEM((chunks, WINDOW, 512), F32),
            pltpu.VMEM((chunks, 8, 128), F32),
            pltpu.VMEM((chunks, 3, 8, 128), F32),
            pltpu.VMEM((4, chunks, WINDOW, 512), BF16),
            pltpu.VMEM((big, full), BF16),
            pltpu.VMEM((big, units), BF16),
            pltpu.VMEM((half, 6, big, 256), BF16),
            pltpu.VMEM((half, 6, big, 256), BF16),
            pltpu.VMEM((half, big, 512), BF16),
            pltpu.VMEM((half, big, 512), F32),
            pltpu.VMEM((half, 16, 128), F32),
            pltpu.VMEM((half, 3, 16, 128), F32),
        ]
        + sems((8,), (2, 5, 4), (2, 5, 4), (2, 16), (2, 16))
        + sems((4,), (4,), (chunks, 6), (chunks, 6), (chunks, 3), (chunks, 3), (chunks, 4), (chunks, 4))
        + sems((half, 6), (half, 6), (half, 3), (half, 3)),
        compiler_params=pltpu.CompilerParams(
            collective_id=0, has_side_effects=True, vmem_limit_bytes=54 * 2**20
        ),
    )(
        residual, rotated_query_rows, rotated_key_rows, value_matrix_rows, head_sink_logit,
        out_proj, gain_mix[None], gain_pre[None], gain_post[None], *loaded[5:],
    )


def solution(mesh):
    placed = (
        P("sp", "tp"), P("sp", "tp"), P("sp", "tp"), P("sp", "tp"), P("tp"), P("tp", None),
        P(), P(), P(), P("sp", "tp"), P("sp", "tp"), P("tp", "sp"),
    )
    return jax.shard_map(body, mesh=mesh, in_specs=placed, out_specs=P("sp", "tp"), check_vma=False)
```

```python
import functools

import jax
import jax.numpy as jnp
from jax import lax
from jax.experimental import pallas as pl
from jax.experimental.pallas import tpu as pltpu
from jax.sharding import PartitionSpec as P

WINDOW = 128
EPS = 1e-06
FEED, SECOND, SUM, FINISH = (8, 9, 10, 12), (9, 10, 11, 13), (10, 11, 12, 14), (11, 12, 13, 15)
DRAIN = 7
MESH = pl.DeviceIdType.MESH
F32 = jnp.float32
BF16 = jnp.bfloat16
NT = (((1,), (1,)), ((), ()))


def ring():
    me = lax.axis_index("tp")
    right, left, far = (lax.rem(me + k, 4) for k in (1, 3, 2))
    return me, right, left, far


def tp_copy(src, dst, send, recv, to):
    return pltpu.make_async_remote_copy(
        src_ref=src, dst_ref=dst, send_sem=send, recv_sem=recv,
        device_id={"tp": to}, device_id_type=MESH,
    )


class Scatter:
    def __init__(self, sent, got, own, send, recv):
        self.sent, self.got, self.own, self.send, self.recv = sent, got, own, send, recv
        self.me, self.right, self.left, self.far = ring()

    def copy(self, slot, m):
        to = self.right if m % 2 == 0 else self.left
        return tp_copy(
            self.sent.at[slot, m], self.got.at[slot, m],
            self.send.at[slot], self.recv.at[slot, 0 if m < 2 else 1], to,
        )

    def arrived(self, slot, group):
        ref = self.got.at[slot, pl.ds(2 * group, 2 + 2 * group)]
        tp_copy(ref, ref, self.send.at[slot], self.recv.at[slot, group], self.right).wait_recv()

    def first(self, slot, part):
        self.sent[slot, 0] = part(self.far, 0)
        self.sent[slot, 1] = part(self.far, 1)
        self.copy(slot, 0).start()
        self.copy(slot, 1).start()
        self.sent[slot, 2] = part(self.right, 1)
        self.sent[slot, 3] = part(self.left, 0)
        self.copy(slot, 2).start()
        self.copy(slot, 3).start()
        self.sent[slot, 4] = part(self.right, 0)
        self.sent[slot, 5] = part(self.left, 1)
        self.own[slot, :, :256] = part(self.me, 0)
        self.own[slot, :, 256:] = part(self.me, 1)

    def second(self, slot):
        self.arrived(slot, 0)
        for k in (0, 1):
            total = self.sent[slot, 4 + k].astype(F32) + self.got[slot, k].astype(F32)
            self.sent[slot, 4 + k] = total.astype(BF16)
            self.copy(slot, 4 + k).start()

    def last(self, slot):
        self.arrived(slot, 1)
        half0 = (
            self.own[slot, :, :256].astype(F32)
            + self.got[slot, 4].astype(F32)
            + self.got[slot, 3].astype(F32)
        )
        half1 = (
            self.own[slot, :, 256:].astype(F32)
            + self.got[slot, 2].astype(F32)
            + self.got[slot, 5].astype(F32)
        )
        return half0, half1

    def drain(self, slot):
        ref = self.sent.at[slot]
        tp_copy(ref, ref, self.send.at[slot], self.recv.at[slot, 0], self.right).wait_send()


class Squares:
    def __init__(self, mine, got, send, recv):
        self.mine, self.got, self.send, self.recv = mine, got, send, recv
        self.me, self.right, self.left, self.far = ring()

    def copies(self, slot):
        for m, to in enumerate((self.right, self.left, self.far)):
            yield tp_copy(
                self.mine.at[slot], self.got.at[slot, m],
                self.send.at[slot], self.recv.at[slot], to,
            )

    def all(self, slot):
        ref = self.got.at[slot]
        return tp_copy(ref, ref, self.send.at[slot], self.recv.at[slot], self.right)

    def give(self, slot, half0, half1):
        total = jnp.sum(half0 * half0, axis=1, keepdims=True) + jnp.sum(
            half1 * half1, axis=1, keepdims=True
        )
        for g in range(total.shape[0] // 128):
            wide = jnp.broadcast_to(total[128 * g : 128 * g + 128], (128, 128))
            self.mine[slot, 8 * g : 8 * g + 8] = wide.T[:8]
        for copy in self.copies(slot):
            copy.start()

    def take(self, slot):
        self.all(slot).wait_recv()
        total = self.mine[slot] + self.got[slot, 0] + self.got[slot, 1] + self.got[slot, 2]
        columns = [
            jnp.broadcast_to(total[8 * g : 8 * g + 1], (128, 128)).T[:, :1]
            for g in range(total.shape[0] // 8)
        ]
        return columns[0] if len(columns) == 1 else jnp.concatenate(columns, axis=0)

    def drain(self, slot):
        self.all(slot).wait_send()


def attend(row, first_key, q_ref, kv, sink_ref, lowest, highest):
    keys, keys_turned, values, values_turned = (
        a[pl.ds(first_key, 3 * WINDOW), :] for a in kv
    )
    lane = lax.broadcasted_iota(jnp.int32, (WINDOW, 128), 1)
    query = lax.broadcasted_iota(jnp.int32, (WINDOW, 3 * WINDOW), 0)
    key = lax.broadcasted_iota(jnp.int32, (WINDOW, 3 * WINDOW), 1)
    inside = (key >= query) & (key <= query + 2 * WINDOW) & (key >= lowest) & (key < highest)
    tiles = []
    for t in range(3):
        pair = q_ref[pl.ds(row, WINDOW), 128 * t : 128 * t + 128].astype(F32) * 0.125
        outs = []
        for half in range(2):
            h = 2 * t + half
            turned = (h // 3) != half
            q = jnp.where((lane >= 64) == (half == 1), pair, 0.0).astype(BF16)
            scores = lax.dot_general(
                q, keys_turned if turned else keys, NT, preferred_element_type=F32
            )
            scores = jnp.where(inside, scores, -1e30)
            sink = sink_ref[h]
            top = jnp.maximum(jnp.max(scores, axis=1, keepdims=True), sink)
            e = jnp.exp(scores - top)
            below = jnp.sum(e, axis=1, keepdims=True) + jnp.exp(sink - top)
            out = jnp.dot(
                e.astype(BF16), values_turned if turned else values,
                preferred_element_type=F32,
            )
            outs.append(out * (1.0 / below))
        tiles.append(jnp.where(lane < 64, outs[0], outs[1]).astype(BF16))
    return jnp.concatenate(tiles, axis=1)


def turn(x):
    return pltpu.roll(x.astype(F32), 64, 1).astype(BF16)


class Weights:
    across = (0, 1, 3, 2)

    def __init__(self, whole, send, recv, core_send, core_recv):
        self.whole, self.send, self.recv = whole, send, recv
        self.core_send, self.core_recv = core_send, core_recv
        sp = lax.axis_index("sp")
        self.core, self.y, self.z = lax.rem(sp, 2), lax.rem(lax.div(sp, 2), 4), lax.div(sp, 8)

    def device(self, way, a, b, core):
        dy, dz = (a, b) if way == 0 else (b, a)
        return (lax.rem(self.z + dz, 4) * 4 + lax.rem(self.y + dy, 4)) * 2 + core

    def neighbours(self):
        ring = [self.device(0, a, b, self.core) for a, b in ((1, 0), (3, 0), (0, 1), (0, 3))]
        return ring + [self.device(0, 0, 0, 1 - self.core)]

    def rows(self, way, a, b, core, part=None):
        start = self.device(way, a, b, core) * 64 + 32 * way
        if part is None:
            return self.whole.at[pl.ds(pl.multiple_of(start, 32), 32), :]
        return self.whole.at[pl.ds(pl.multiple_of(start + 16 * part, 16), 16), :]

    def at(self, stage, k):
        return (k, 0) if stage == 0 else (self.across[stage - 1], k)

    def copy(self, way, stage, m):
        offset = (0, 0, 3, 1)[m]
        ref = self.rows(way, *self.at(stage, offset), self.core, None if m < 2 else m - 2)
        to = self.device(way, *((1 if m % 2 == 0 else 3, 0) if stage == 0 else (0, 1 if m % 2 == 0 else 3)), self.core)
        return pltpu.make_async_remote_copy(
            src_ref=ref, dst_ref=ref,
            send_sem=self.send.at[way, stage], recv_sem=self.recv.at[way, stage, 0 if m < 2 else 1],
            device_id={"sp": to}, device_id_type=MESH,
        )

    def over(self, way, a, b):
        ref = self.rows(way, a, b, self.core)
        return pltpu.make_async_remote_copy(
            src_ref=ref, dst_ref=ref,
            send_sem=self.core_send.at[way, a], recv_sem=self.core_recv.at[way, a],
            device_id={"sp": self.device(way, 0, 0, 1 - self.core)}, device_id_type=MESH,
        )

    def some(self, count, send, recv):
        ref = self.whole.at[pl.ds(0, count), :]
        return pltpu.make_async_remote_copy(
            src_ref=ref, dst_ref=ref, send_sem=send, recv_sem=recv,
            device_id={"sp": self.device(0, 0, 0, 1 - self.core)}, device_id_type=MESH,
        )

    def open(self, way, stage):
        self.copy(way, stage, 0).start()
        self.copy(way, stage, 1).start()

    def relay(self, way, stage):
        self.some(64, self.send.at[way, stage], self.recv.at[way, stage, 0]).wait_recv()
        self.copy(way, stage, 2).start()
        self.copy(way, stage, 3).start()

    def share(self, way, stage, ks):
        for k in ks:
            self.over(way, *self.at(stage, k)).start()

    def close(self, way, stage):
        self.some(32, self.send.at[way, stage], self.recv.at[way, stage, 1]).wait_recv()
        self.share(way, stage, (2,))

    def step(self, n):
        for way in (0, 1):
            if n == 0:
                self.open(way, 0)
            elif n == 1:
                self.relay(way, 0)
        for way in (0, 1):
            if n == 0:
                self.open(way, 1)
                self.over(way, 0, 0).start()
            elif n == 1:
                self.open(way, 2)
                self.open(way, 3)
                self.share(way, 0, (1, 3))
            elif n == 2:
                self.relay(way, 1)
                self.share(way, 1, (1, 3))
            elif n == 3:
                self.close(way, 0)
                self.open(way, 4)
            elif n == 4:
                for stage in (2, 3):
                    self.relay(way, stage)
                    self.share(way, stage, (1, 3))
            elif n == 5:
                self.close(way, 1)
                self.relay(way, 4)
                self.share(way, 4, (1, 3))
            elif n == 6:
                for stage in (2, 3, 4):
                    self.close(way, stage)
            elif n == 7:
                for a in range(4):
                    self.some(128, self.core_send.at[way, a], self.core_recv.at[way, a]).wait_recv()

    def drain(self):
        for way in (0, 1):
            for stage in range(5):
                self.some(96, self.send.at[way, stage], self.recv.at[way, stage, 0]).wait_send()
            for a in range(4):
                self.some(128, self.core_send.at[way, a], self.core_recv.at[way, a]).wait_send()


def layer_kernel(
    chunks, sp_count,
    res_hbm, q_hbm, k_hbm, v_hbm, sink_ref, proj_hbm, gain_mix_ref, gain_pre_ref, gain_post_ref,
    gate_hbm, up_hbm, down_hbm,
    out_hbm,
    done, res_ref, q_ref, k_ref, v_ref, proj_ref, gate_ref, up_ref, down_ref,
    whole, keys, keys_turned, values, values_turned, att,
    sent, got, own, mixed, mine, squares, rows,
    normed, hidden, f_sent, f_got, f_own, f_total, f_mine, f_squares,
    out_sem, load_sem, w_send, w_recv, core_send, core_recv,
    halo_send, halo_recv, rs_send, rs_recv, sq_send, sq_recv, ag_send, ag_recv,
    f_rs_send, f_rs_recv, f_sq_send, f_sq_recv,
):
    me, right, left, far = ring()
    sp = lax.axis_index("sp")
    after = lax.rem(sp + 1, sp_count)
    before = lax.rem(sp + sp_count - 1, sp_count)
    length = chunks * WINDOW
    half_chunks = chunks // 2
    units = gate_ref.shape[1]
    tiles = units // 128
    inner = 2 * units
    loads = [
        pltpu.make_async_copy(a, b, load_sem.at[n])
        for n, (a, b) in enumerate((
            (gate_hbm, gate_ref), (up_hbm, up_ref), (down_hbm, down_ref), (k_hbm, k_ref),
            (v_hbm, v_ref), (q_hbm, q_ref), (proj_hbm, proj_ref), (res_hbm, res_ref),
        ))
    ]
    for load in loads:
        load.start()
    weights = Weights(whole, w_send, w_recv, core_send, core_recv)
    barrier = pltpu.get_barrier_semaphore()
    others = [{"tp": right}, {"tp": left}, {"tp": far}, {"sp": after}, {"sp": before}]
    others += [{"sp": n} for n in weights.neighbours()]
    for other in others:
        pl.semaphore_signal(barrier, inc=1, device_id=other, device_id_type=MESH)
    for load in loads[:3]:
        load.wait()
    shard = pl.ds(pl.multiple_of(sp * 64, 64), 64)
    for j in range(tiles):
        whole[shard, 256 * j : 256 * j + 128] = gate_ref[:, 128 * j : 128 * j + 128]
        whole[shard, 256 * j + 128 : 256 * j + 256] = up_ref[:, 128 * j : 128 * j + 128]
        whole[shard, inner + 128 * j : inner + 128 * j + 128] = (
            down_ref[:, 128 * j : 128 * j + 128]
        )
    for load in loads[3:5]:
        load.wait()
    pl.semaphore_wait(barrier, len(others))

    def halo(n):
        mine_ref, both = ((k_ref, keys), (v_ref, values))[n // 2]
        if n % 2 == 0:
            src, dst, to = mine_ref.at[pl.ds(length - WINDOW, WINDOW)], both.at[pl.ds(0, WINDOW)], after
        else:
            src, dst, to = mine_ref.at[pl.ds(0, WINDOW)], both.at[pl.ds(length + WINDOW, WINDOW)], before
        return pltpu.make_async_remote_copy(
            src_ref=src, dst_ref=dst, send_sem=halo_send, recv_sem=halo_recv,
            device_id={"sp": to}, device_id_type=MESH,
        )

    halos = keys.at[pl.ds(0, 4 * WINDOW)]
    halos = tp_copy(halos, halos, halo_send, halo_recv, right)
    for n in range(4):
        halo(n).start()
    weights.step(0)
    middle = pl.ds(WINDOW, length)
    keys[middle, :] = k_ref[...]
    values[middle, :] = v_ref[...]
    keys_turned[middle, :] = turn(k_ref[...])
    values_turned[middle, :] = turn(v_ref[...])
    for load in loads[5:]:
        load.wait()

    scatter = Scatter(sent, got, own, rs_send, rs_recv)
    sums = Squares(mine, squares, sq_send, sq_recv)
    f_scatter = Scatter(f_sent, f_got, f_own, f_rs_send, f_rs_recv)
    f_sums = Squares(f_mine, f_squares, f_sq_send, f_sq_recv)
    columns = pl.ds(pl.multiple_of(me * 512, 512), 512)
    gain_mix = gain_mix_ref[:, columns]
    gain_post = gain_post_ref[:, columns]

    def place(slot):
        return pl.multiple_of(lax.rem(slot + 1, chunks) * WINDOW, WINDOW)

    def gather(slot, m):
        owner, to, part = (
            (me, right, pl.ds(0, 512)), (me, left, pl.ds(0, 512)),
            (left, right, pl.ds(0, 256)), (right, left, pl.ds(256, 256)),
        )[m]
        ref = rows.at[owner, slot, :, part]
        return tp_copy(ref, ref, ag_send.at[slot], ag_recv.at[slot, 0 if m < 2 else 1], to)

    def gathers(slot, blocks, group):
        ref = rows.at[pl.ds(0, blocks), slot]
        return tp_copy(ref, ref, ag_send.at[slot], ag_recv.at[slot, group], right)

    def attention(t):
        @pl.when(t == chunks - 2)
        def _():
            halos.wait_recv()
            for at in (0, length + WINDOW):
                keys_turned[pl.ds(at, WINDOW), :] = turn(keys[pl.ds(at, WINDOW), :])
                values_turned[pl.ds(at, WINDOW), :] = turn(values[pl.ds(at, WINDOW), :])

        row = place(t)
        lowest = jnp.where((sp == 0) & (t == chunks - 1), WINDOW, 0)
        highest = jnp.where((sp == sp_count - 1) & (t == chunks - 2), 2 * WINDOW, 3 * WINDOW)
        att[...] = attend(
            row, row, q_ref, (keys, keys_turned, values, values_turned), sink_ref, lowest, highest
        )

        def part(block, half):
            at = pl.ds(pl.multiple_of(block * 512 + 256 * half, 256), 256)
            return jnp.dot(att[...], proj_ref[:, at], preferred_element_type=F32).astype(BF16)

        scatter.first(t, part)

    def mix(s):
        half0, half1 = scatter.last(s)
        mixed[s, :, :256] = half0
        mixed[s, :, 256:] = half1
        sums.give(s, half0, half1)

    def first_rows(s):
        scale = lax.rsqrt(sums.take(s) / 2048.0 + EPS)
        res = res_ref[pl.ds(place(s), WINDOW), :].astype(F32)
        rows[me, s] = (res + mixed[s] * scale * gain_mix).astype(BF16)
        gather(s, 0).start()
        gather(s, 1).start()

    def relay(s):
        gathers(s, 2, 0).wait_recv()
        gather(s, 2).start()
        gather(s, 3).start()

    def feed(u):
        for k in range(2):
            squared = jnp.zeros((WINDOW, 1), F32)
            for b in range(4):
                x = rows[b, 2 * u + k].astype(F32)
                squared += jnp.sum(x * x, axis=1, keepdims=True)
            scale = lax.rsqrt(squared / 2048.0 + EPS)
            for b in range(4):
                x = rows[b, 2 * u + k].astype(F32)
                normed[WINDOW * k : WINDOW * k + WINDOW, 512 * b : 512 * b + 512] = (
                    x * scale * gain_pre_ref[:, 512 * b : 512 * b + 512]
                ).astype(BF16)

        for j in range(tiles):
            both = jnp.dot(
                normed[...], whole[:, 256 * j : 256 * j + 256], preferred_element_type=F32
            )
            gate, up = both[:, :128], both[:, 128:]
            hidden[:, 128 * j : 128 * j + 128] = (gate / (1.0 + jnp.exp(-gate)) * up).astype(BF16)

        def part(block, half):
            at = pl.ds(pl.multiple_of(block * 512 + 256 * half, 256), 256)
            return lax.dot_general(
                hidden[...], whole[at, inner : inner + units], NT, preferred_element_type=F32
            ).astype(BF16)

        f_scatter.first(u, part)

    def feed_sum(u):
        half0, half1 = f_scatter.last(u)
        f_total[u, :, :256] = half0
        f_total[u, :, 256:] = half1
        f_sums.give(u, half0, half1)

    def finish(u):
        scale = lax.rsqrt(f_sums.take(u) / 2048.0 + EPS)
        for k in range(2):
            part = pl.ds(WINDOW * k, WINDOW)
            at = pl.ds(place(2 * u + k), WINDOW)
            done[at, :] = (
                rows[me, 2 * u + k].astype(F32)
                + 0.5 * (f_total[u, part, :] * scale[WINDOW * k : WINDOW * k + WINDOW] * gain_post)
            ).astype(BF16)
            result(2 * u + k).start()

    def result(slot):
        at = pl.ds(place(slot), WINDOW)
        return pltpu.make_async_copy(done.at[at, :], out_hbm.at[at, :], out_sem)

    def drain(slot):
        scatter.drain(slot)
        sums.drain(slot)
        gathers(slot, 3, 0).wait_send()

    def f_drain(u):
        f_scatter.drain(u)
        f_sums.drain(u)

    def step(t, carry):
        def when(lag, fn):
            @pl.when((t >= lag) & (t < chunks + lag))
            def _():
                fn(t - lag)

        def when_fed(times, fn):
            now, index = t == times[0], 0
            for n in times[1:]:
                now, index = now | (t == n), index + (t >= n).astype(jnp.int32)

            @pl.when(now)
            def _():
                fn(index)

        when(0, attention)
        when(1, scatter.second)
        when(2, mix)
        when(3, first_rows)
        when(4, relay)

        @pl.when((t >= 5) & (t < chunks + 5))
        def _():
            gathers(t - 5, 1, 1).wait_recv()

        for n in range(1, 8):
            @pl.when(t == n)
            def _():
                weights.step(n)

        when_fed(FEED, feed)
        when_fed(SECOND, f_scatter.second)
        when_fed(SUM, feed_sum)
        when_fed(FINISH, finish)
        when(DRAIN, drain)

        @pl.when(t == DRAIN)
        def _():
            halos.wait_send()
            weights.drain()

        when_fed(FINISH[1:], f_drain)
        return carry

    lax.fori_loop(0, FINISH[-1] + 1, step, 0)
    f_drain(half_chunks - 1)
    pltpu.make_async_copy(done, out_hbm, out_sem).wait()


def sems(*shapes):
    return [pltpu.SemaphoreType.DMA(s) for s in shapes]


def body(
    residual, rotated_query_rows, rotated_key_rows, value_matrix_rows, head_sink_logit,
    out_proj, gain_mix, gain_pre, gain_post, gate_proj, up_proj, down_proj,
):
    length = residual.shape[0]
    chunks = length // WINDOW
    half = chunks // 2
    units = gate_proj.shape[1]
    sp_count = lax.axis_size("sp")
    full = sp_count * gate_proj.shape[0]
    big = 2 * WINDOW
    vmem = pl.BlockSpec(memory_space=pltpu.VMEM)
    smem = pl.BlockSpec(memory_space=pltpu.SMEM)
    hbm = pl.BlockSpec(memory_space=pl.ANY)
    loaded = (
        residual, rotated_query_rows, rotated_key_rows, value_matrix_rows, out_proj,
        gate_proj, up_proj, down_proj.T,
    )
    return pl.pallas_call(
        functools.partial(layer_kernel, chunks, sp_count),
        out_shape=jax.ShapeDtypeStruct(residual.shape, BF16),
        in_specs=[hbm] * 4 + [smem, hbm] + [vmem] * 3 + [hbm] * 3,
        out_specs=hbm,
        scratch_shapes=[pltpu.VMEM(residual.shape, BF16)]
        + [pltpu.VMEM(a.shape, BF16) for a in loaded]
        + [pltpu.VMEM((full, 3 * units), BF16)]
        + [pltpu.VMEM((length + big, 128), BF16)] * 4
        + [
            pltpu.VMEM((WINDOW, 384), BF16),
            pltpu.VMEM((chunks, 6, WINDOW, 256), BF16),
            pltpu.VMEM((chunks, 6, WINDOW, 256), BF16),
            pltpu.VMEM((chunks, WINDOW, 512), BF16),
            pltpu.VMEM((chunks, WINDOW, 512), F32),
            pltpu.VMEM((chunks, 8, 128), F32),
            pltpu.VMEM((chunks, 3, 8, 128), F32),
            pltpu.VMEM((4, chunks, WINDOW, 512), BF16),
            pltpu.VMEM((big, full), BF16),
            pltpu.VMEM((big, units), BF16),
            pltpu.VMEM((half, 6, big, 256), BF16),
            pltpu.VMEM((half, 6, big, 256), BF16),
            pltpu.VMEM((half, big, 512), BF16),
            pltpu.VMEM((half, big, 512), F32),
            pltpu.VMEM((half, 16, 128), F32),
            pltpu.VMEM((half, 3, 16, 128), F32),
        ]
        + [pltpu.SemaphoreType.DMA]
        + sems((8,), (2, 5), (2, 5, 2), (2, 4), (2, 4))
        + [pltpu.SemaphoreType.DMA] * 2
        + sems((chunks,), (chunks, 2), (chunks,), (chunks,), (chunks,), (chunks, 2))
        + sems((half,), (half, 2), (half,), (half,)),
        compiler_params=pltpu.CompilerParams(
            collective_id=0, has_side_effects=True, vmem_limit_bytes=54 * 2**20
        ),
    )(
        residual, rotated_query_rows, rotated_key_rows, value_matrix_rows, head_sink_logit,
        out_proj, gain_mix[None], gain_pre[None], gain_post[None], *loaded[5:],
    )


def solution(mesh):
    placed = (
        P("sp", "tp"), P("sp", "tp"), P("sp", "tp"), P("sp", "tp"), P("tp"), P("tp", None),
        P(), P(), P(), P("sp", "tp"), P("sp", "tp"), P("tp", "sp"),
    )
    return jax.shard_map(body, mesh=mesh, in_specs=placed, out_specs=P("sp", "tp"), check_vma=False)
```

```python
import functools

import jax
import jax.numpy as jnp
from jax import lax
from jax.experimental import pallas as pl
from jax.experimental.pallas import tpu as pltpu
from jax.sharding import PartitionSpec as P

WINDOW = 128
EPS = 1e-06
MIX = 4
PROJECTION = (0, 1, 2, 3, 4)
WEIGHTS = (5, 5, 4, 6, 6, 8, 9, 10, 12), (2, 5, 6, 4, 6, 8, 10, 12, 12)
FEED, SECOND, SUM, FINISH = (12, 13, 14, 15), (13, 14, 15, 16), (14, 15, 16, 17), (15, 16, 17, 18)
DRAIN = 9
MESH = pl.DeviceIdType.MESH
F32 = jnp.float32
BF16 = jnp.bfloat16
NT = (((1,), (1,)), ((), ()))


def ring():
    me = lax.axis_index("tp")
    right, left, far = (lax.rem(me + k, 4) for k in (1, 3, 2))
    return me, right, left, far


def tp_copy(src, dst, send, recv, to):
    return pltpu.make_async_remote_copy(
        src_ref=src, dst_ref=dst, send_sem=send, recv_sem=recv,
        device_id={"tp": to}, device_id_type=MESH,
    )


class Scatter:
    def __init__(self, sent, got, own, send, recv):
        self.sent, self.got, self.own, self.send, self.recv = sent, got, own, send, recv
        self.me, self.right, self.left, self.far = ring()

    def copy(self, slot, m):
        to = self.right if m % 2 == 0 else self.left
        return tp_copy(
            self.sent.at[slot, m], self.got.at[slot, m],
            self.send.at[slot], self.recv.at[slot, 0 if m < 2 else 1], to,
        )

    def arrived(self, slot, group):
        ref = self.got.at[slot, pl.ds(2 * group, 2 + 2 * group)]
        tp_copy(ref, ref, self.send.at[slot], self.recv.at[slot, group], self.right).wait_recv()

    def first(self, slot, part):
        self.sent[slot, 0] = part(self.far, 0)
        self.sent[slot, 1] = part(self.far, 1)
        self.copy(slot, 0).start()
        self.copy(slot, 1).start()
        self.sent[slot, 2] = part(self.right, 1)
        self.sent[slot, 3] = part(self.left, 0)
        self.copy(slot, 2).start()
        self.copy(slot, 3).start()
        self.sent[slot, 4] = part(self.right, 0)
        self.sent[slot, 5] = part(self.left, 1)
        self.own[slot, :, :256] = part(self.me, 0)
        self.own[slot, :, 256:] = part(self.me, 1)

    def second(self, slot):
        self.arrived(slot, 0)
        for k in (0, 1):
            total = self.sent[slot, 4 + k].astype(F32) + self.got[slot, k].astype(F32)
            self.sent[slot, 4 + k] = total.astype(BF16)
            self.copy(slot, 4 + k).start()

    def last(self, slot):
        self.arrived(slot, 1)
        half0 = (
            self.own[slot, :, :256].astype(F32)
            + self.got[slot, 4].astype(F32)
            + self.got[slot, 3].astype(F32)
        )
        half1 = (
            self.own[slot, :, 256:].astype(F32)
            + self.got[slot, 2].astype(F32)
            + self.got[slot, 5].astype(F32)
        )
        return half0, half1

    def drain(self, slot):
        ref = self.sent.at[slot]
        tp_copy(ref, ref, self.send.at[slot], self.recv.at[slot, 0], self.right).wait_send()


class Squares:
    def __init__(self, mine, got, send, recv):
        self.mine, self.got, self.send, self.recv = mine, got, send, recv
        self.me, self.right, self.left, self.far = ring()

    def copies(self, slot):
        for m, to in enumerate((self.right, self.left, self.far)):
            yield tp_copy(
                self.mine.at[slot], self.got.at[slot, m],
                self.send.at[slot], self.recv.at[slot], to,
            )

    def all(self, slot):
        ref = self.got.at[slot]
        return tp_copy(ref, ref, self.send.at[slot], self.recv.at[slot], self.right)

    def give(self, slot, half0, half1):
        total = jnp.sum(half0 * half0, axis=1, keepdims=True) + jnp.sum(
            half1 * half1, axis=1, keepdims=True
        )
        for g in range(total.shape[0] // 128):
            wide = jnp.broadcast_to(total[128 * g : 128 * g + 128], (128, 128))
            self.mine[slot, 8 * g : 8 * g + 8] = wide.T[:8]
        for copy in self.copies(slot):
            copy.start()

    def take(self, slot):
        self.all(slot).wait_recv()
        total = self.mine[slot] + self.got[slot, 0] + self.got[slot, 1] + self.got[slot, 2]
        columns = [
            jnp.broadcast_to(total[8 * g : 8 * g + 1], (128, 128)).T[:, :1]
            for g in range(total.shape[0] // 8)
        ]
        return columns[0] if len(columns) == 1 else jnp.concatenate(columns, axis=0)

    def drain(self, slot):
        self.all(slot).wait_send()


class Gather:
    def __init__(self, buffer, send, recv):
        self.buffer, self.send, self.recv = buffer, send, recv
        self.me, self.right, self.left, self.far = ring()

    def copy(self, slot, owner, to, group, part):
        ref = self.buffer.at[owner, slot, part]
        return tp_copy(ref, ref, self.send.at[slot], self.recv.at[slot, group], to)

    def some(self, slot, blocks, group):
        ref = self.buffer.at[pl.ds(0, blocks), slot]
        return tp_copy(ref, ref, self.send.at[slot], self.recv.at[slot, group], self.right)

    def open(self, slot):
        whole = pl.ds(0, WINDOW)
        self.copy(slot, self.me, self.right, 0, whole).start()
        self.copy(slot, self.me, self.left, 0, whole).start()

    def relay(self, slot):
        self.some(slot, 2, 0).wait_recv()
        self.copy(slot, self.left, self.right, 1, pl.ds(0, WINDOW // 2)).start()
        self.copy(slot, self.right, self.left, 1, pl.ds(WINDOW // 2, WINDOW // 2)).start()

    def close(self, slot):
        self.some(slot, 1, 1).wait_recv()

    def drain(self, slot):
        self.some(slot, 3, 0).wait_send()


class Projection:
    def __init__(self, taken, source, send, recv):
        self.taken, self.source, self.send, self.recv = taken, source, send, recv
        self.me, self.right, self.left, self.far = ring()
        sp = lax.axis_index("sp")
        self.core, self.y, self.rest = lax.rem(sp, 2), lax.rem(lax.div(sp, 2), 4), lax.div(sp, 8) * 8
        self.depth = source.shape[0] // 8

    def columns(self, owner):
        return pl.ds(pl.multiple_of(owner * 512, 512), 512)

    def eighth(self, dy):
        start = (2 * lax.rem(self.y + dy, 4) + self.core) * self.depth
        return pl.ds(pl.multiple_of(start, self.depth), self.depth)

    def to_sp(self, dy, core):
        return {"sp": self.rest + 2 * lax.rem(self.y + dy, 4) + core}

    def copy(self, src, dst, n, group, to):
        return pltpu.make_async_remote_copy(
            src_ref=src, dst_ref=dst, send_sem=self.send.at[n], recv_sem=self.recv.at[group],
            device_id=to, device_id_type=MESH,
        )

    def piece(self, dy, n, group, to, part=None):
        ref = self.taken.at[pl.ds(1, 3), self.eighth(dy), pl.ds(*(part or (0, 512)))]
        return self.copy(ref, ref, n, group, to)

    def some(self, n, group, pieces):
        ref = self.taken.at[pl.ds(1, 3), pl.ds(0, pieces * self.depth)]
        return self.copy(ref, ref, n, group, {"tp": self.right})

    def across(self, dy):
        self.piece(dy, 2, 3, self.to_sp(0, 1 - self.core)).start()

    def step(self, n):
        if n == 0:
            rows = self.eighth(0)
            for to, k in ((self.right, 3), (self.left, 1), (self.far, 2)):
                self.copy(
                    self.source.at[rows, self.columns(to)], self.taken.at[k, rows], 0, 0, {"tp": to}
                ).start()
        elif n == 1:
            self.some(0, 0, 1).wait_recv()
            self.piece(0, 1, 1, self.to_sp(1, self.core)).start()
            self.piece(0, 1, 1, self.to_sp(3, self.core)).start()
            self.across(0)
        elif n == 2:
            self.some(1, 1, 2).wait_recv()
            self.piece(3, 1, 2, self.to_sp(1, self.core), (0, 256)).start()
            self.piece(1, 1, 2, self.to_sp(3, self.core), (256, 256)).start()
            self.across(1)
            self.across(3)
        elif n == 3:
            self.some(1, 2, 1).wait_recv()
            self.across(2)
        elif n == 4:
            self.some(2, 3, 4).wait_recv()

    def drain(self):
        for n, pieces in enumerate((1, 3, 4)):
            self.some(n, 0, pieces).wait_send()


def attend(row, first_key, q_ref, kv, sink_ref, lowest, highest):
    keys, keys_turned, values, values_turned = (
        a[pl.ds(first_key, 3 * WINDOW), :] for a in kv
    )
    lane = lax.broadcasted_iota(jnp.int32, (WINDOW, 128), 1)
    query = lax.broadcasted_iota(jnp.int32, (WINDOW, 3 * WINDOW), 0)
    key = lax.broadcasted_iota(jnp.int32, (WINDOW, 3 * WINDOW), 1)
    inside = (key >= query) & (key <= query + 2 * WINDOW) & (key >= lowest) & (key < highest)
    tiles = []
    for t in range(3):
        pair = q_ref[pl.ds(row, WINDOW), 128 * t : 128 * t + 128].astype(F32) * 0.125
        outs = []
        for half in range(2):
            h = 2 * t + half
            turned = (h // 3) != half
            q = jnp.where((lane >= 64) == (half == 1), pair, 0.0).astype(BF16)
            scores = lax.dot_general(
                q, keys_turned if turned else keys, NT, preferred_element_type=F32
            )
            scores = jnp.where(inside, scores, -1e30)
            sink = sink_ref[h]
            top = jnp.maximum(jnp.max(scores, axis=1, keepdims=True), sink)
            e = jnp.exp(scores - top)
            below = jnp.sum(e, axis=1, keepdims=True) + jnp.exp(sink - top)
            out = jnp.dot(
                e.astype(BF16), values_turned if turned else values,
                preferred_element_type=F32,
            )
            outs.append(out * (1.0 / below))
        tiles.append(jnp.where(lane < 64, outs[0], outs[1]).astype(BF16))
    return jnp.concatenate(tiles, axis=1)


def turn(x):
    return pltpu.roll(x.astype(F32), 64, 1).astype(BF16)


class Weights:
    across = (0, 1, 3, 2)

    def __init__(self, whole, send, recv, core_send, core_recv):
        self.whole, self.send, self.recv = whole, send, recv
        self.core_send, self.core_recv = core_send, core_recv
        sp = lax.axis_index("sp")
        self.core, self.y, self.z = lax.rem(sp, 2), lax.rem(lax.div(sp, 2), 4), lax.div(sp, 8)

    def device(self, way, a, b, core):
        dy, dz = (a, b) if way == 0 else (b, a)
        return (lax.rem(self.z + dz, 4) * 4 + lax.rem(self.y + dy, 4)) * 2 + core

    def neighbours(self):
        ring = [self.device(0, a, b, self.core) for a, b in ((1, 0), (3, 0), (0, 1), (0, 3))]
        return ring + [self.device(0, 0, 0, 1 - self.core)]

    def rows(self, way, a, b, core, part=None):
        start = self.device(way, a, b, core) * 64 + 32 * way
        if part is None:
            return self.whole.at[pl.ds(pl.multiple_of(start, 32), 32), :]
        return self.whole.at[pl.ds(pl.multiple_of(start + 16 * part, 16), 16), :]

    def at(self, stage, k):
        return (k, 0) if stage == 0 else (self.across[stage - 1], k)

    def copy(self, way, stage, m):
        offset = (0, 0, 3, 1)[m]
        ref = self.rows(way, *self.at(stage, offset), self.core, None if m < 2 else m - 2)
        to = self.device(way, *((1 if m % 2 == 0 else 3, 0) if stage == 0 else (0, 1 if m % 2 == 0 else 3)), self.core)
        return pltpu.make_async_remote_copy(
            src_ref=ref, dst_ref=ref,
            send_sem=self.send.at[way, stage], recv_sem=self.recv.at[way, stage, 0 if m < 2 else 1],
            device_id={"sp": to}, device_id_type=MESH,
        )

    def over(self, way, a, b):
        ref = self.rows(way, a, b, self.core)
        return pltpu.make_async_remote_copy(
            src_ref=ref, dst_ref=ref,
            send_sem=self.core_send.at[way, a], recv_sem=self.core_recv.at[way, a],
            device_id={"sp": self.device(way, 0, 0, 1 - self.core)}, device_id_type=MESH,
        )

    def some(self, count, send, recv):
        ref = self.whole.at[pl.ds(0, count), :]
        return pltpu.make_async_remote_copy(
            src_ref=ref, dst_ref=ref, send_sem=send, recv_sem=recv,
            device_id={"sp": self.device(0, 0, 0, 1 - self.core)}, device_id_type=MESH,
        )

    def open(self, way, stage):
        self.copy(way, stage, 0).start()
        self.copy(way, stage, 1).start()

    def relay(self, way, stage):
        self.some(64, self.send.at[way, stage], self.recv.at[way, stage, 0]).wait_recv()
        self.copy(way, stage, 2).start()
        self.copy(way, stage, 3).start()

    def share(self, way, stage, ks):
        for k in ks:
            self.over(way, *self.at(stage, k)).start()

    def close(self, way, stage):
        self.some(32, self.send.at[way, stage], self.recv.at[way, stage, 1]).wait_recv()
        self.share(way, stage, (2,))

    def step(self, way, n):
        if n == 0:
            self.relay(way, 0)
            self.share(way, 0, (1, 3))
        elif n == 1:
            self.open(way, 2)
            self.open(way, 3)
        elif n == 2:
            self.relay(way, 1)
            self.share(way, 1, (1, 3))
        elif n == 3:
            self.close(way, 0)
        elif n == 4:
            self.open(way, 4)
        elif n == 5:
            for stage in (2, 3):
                self.relay(way, stage)
                self.share(way, stage, (1, 3))
        elif n == 6:
            self.close(way, 1)
            self.relay(way, 4)
            self.share(way, 4, (1, 3))
        elif n == 7:
            for stage in (2, 3, 4):
                self.close(way, stage)
        elif n == 8:
            for a in range(4):
                self.some(128, self.core_send.at[way, a], self.core_recv.at[way, a]).wait_recv()

    def drain(self):
        for way in (0, 1):
            for stage in range(5):
                self.some(96, self.send.at[way, stage], self.recv.at[way, stage, 0]).wait_send()
            for a in range(4):
                self.some(128, self.core_send.at[way, a], self.core_recv.at[way, a]).wait_send()


def layer_kernel(
    chunks, sp_count,
    res_hbm, q_hbm, k_hbm, v_hbm, sink_ref, proj_hbm, gain_mix_ref, gain_pre_ref, gain_post_ref,
    gate_hbm, up_hbm, down_hbm,
    out_hbm,
    done, res_ref, q_ref, k_ref, v_ref, proj_ref, gate_ref, up_ref, down_ref,
    whole, keys, keys_turned, values, values_turned, taken, att,
    mixed, mine, squares, rows,
    normed, hidden, f_sent, f_got, f_own, f_total, f_mine, f_squares,
    out_sem, load_sem, w_send, w_recv, core_send, core_recv,
    halo_send, halo_recv, p_send, p_recv, at_send, at_recv, sq_send, sq_recv, ag_send, ag_recv,
    f_rs_send, f_rs_recv, f_sq_send, f_sq_recv,
):
    me, right, left, far = ring()
    sp = lax.axis_index("sp")
    after = lax.rem(sp + 1, sp_count)
    before = lax.rem(sp + sp_count - 1, sp_count)
    length = chunks * WINDOW
    half_chunks = chunks // 2
    units = gate_ref.shape[1]
    tiles = units // 128
    inner = 2 * units
    loads = [
        pltpu.make_async_copy(a, b, load_sem.at[n])
        for n, (a, b) in enumerate((
            (proj_hbm, proj_ref), (k_hbm, k_ref), (v_hbm, v_ref), (gate_hbm, gate_ref),
            (up_hbm, up_ref), (down_hbm, down_ref), (q_hbm, q_ref), (res_hbm, res_ref),
        ))
    ]
    for load in loads:
        load.start()
    weights = Weights(whole, w_send, w_recv, core_send, core_recv)
    barrier = pltpu.get_barrier_semaphore()
    others = [{"tp": right}, {"tp": left}, {"tp": far}, {"sp": after}, {"sp": before}]
    others += [{"sp": n} for n in weights.neighbours()]
    for other in others:
        pl.semaphore_signal(barrier, inc=1, device_id=other, device_id_type=MESH)
    for load in loads[3:6]:
        load.wait()
    shard = pl.ds(pl.multiple_of(sp * 64, 64), 64)
    for j in range(tiles):
        whole[shard, 256 * j : 256 * j + 128] = gate_ref[:, 128 * j : 128 * j + 128]
        whole[shard, 256 * j + 128 : 256 * j + 256] = up_ref[:, 128 * j : 128 * j + 128]
        whole[shard, inner + 128 * j : inner + 128 * j + 128] = (
            down_ref[:, 128 * j : 128 * j + 128]
        )
    for load in loads[:3]:
        load.wait()
    pl.semaphore_wait(barrier, len(others))

    def halo(n):
        mine_ref, both = ((k_ref, keys), (v_ref, values))[n // 2]
        if n % 2 == 0:
            src, dst, to = mine_ref.at[pl.ds(length - WINDOW, WINDOW)], both.at[pl.ds(0, WINDOW)], after
        else:
            src, dst, to = mine_ref.at[pl.ds(0, WINDOW)], both.at[pl.ds(length + WINDOW, WINDOW)], before
        return pltpu.make_async_remote_copy(
            src_ref=src, dst_ref=dst, send_sem=halo_send, recv_sem=halo_recv,
            device_id={"sp": to}, device_id_type=MESH,
        )

    halos = keys.at[pl.ds(0, 4 * WINDOW)]
    halos = tp_copy(halos, halos, halo_send, halo_recv, right)
    for n in range(4):
        halo(n).start()
    projection = Projection(taken, proj_ref, p_send, p_recv)
    projection.step(0)
    weights.open(1, 0)
    weights.open(0, 1)
    weights.over(0, 0, 0).start()
    weights.over(1, 0, 0).start()
    middle = pl.ds(WINDOW, length)
    keys[middle, :] = k_ref[...]
    values[middle, :] = v_ref[...]
    keys_turned[middle, :] = turn(k_ref[...])
    values_turned[middle, :] = turn(v_ref[...])
    for load in loads[6:]:
        load.wait()
    taken[0] = proj_ref[:, projection.columns(me)]

    mixing = Gather(att, at_send, at_recv)
    feeding = Gather(rows, ag_send, ag_recv)
    sums = Squares(mine, squares, sq_send, sq_recv)
    f_scatter = Scatter(f_sent, f_got, f_own, f_rs_send, f_rs_recv)
    f_sums = Squares(f_mine, f_squares, f_sq_send, f_sq_recv)
    columns = pl.ds(pl.multiple_of(me * 512, 512), 512)
    gain_mix = gain_mix_ref[:, columns]
    gain_post = gain_post_ref[:, columns]

    def place(slot):
        return pl.multiple_of(lax.rem(slot + 1, chunks) * WINDOW, WINDOW)

    def attention(t):
        @pl.when(t == chunks - 2)
        def _():
            halos.wait_recv()
            for at in (0, length + WINDOW):
                keys_turned[pl.ds(at, WINDOW), :] = turn(keys[pl.ds(at, WINDOW), :])
                values_turned[pl.ds(at, WINDOW), :] = turn(values[pl.ds(at, WINDOW), :])

        row = place(t)
        lowest = jnp.where((sp == 0) & (t == chunks - 1), WINDOW, 0)
        highest = jnp.where((sp == sp_count - 1) & (t == chunks - 2), 2 * WINDOW, 3 * WINDOW)
        att[me, t] = attend(
            row, row, q_ref, (keys, keys_turned, values, values_turned), sink_ref, lowest, highest
        )
        mixing.open(t)

    def mix(s):
        mixing.close(s)
        total = jnp.zeros((WINDOW, 512), F32)
        for k, owner in enumerate((me, right, far, left)):
            total += jnp.dot(att[owner, s], taken[k], preferred_element_type=F32)
        mixed[s] = total
        sums.give(s, total[:, :256], total[:, 256:])

    def first_rows(s):
        scale = lax.rsqrt(sums.take(s) / 2048.0 + EPS)
        res = res_ref[pl.ds(place(s), WINDOW), :].astype(F32)
        rows[me, s] = (res + mixed[s] * scale * gain_mix).astype(BF16)
        feeding.open(s)

    def feed(u):
        for k in range(2):
            squared = jnp.zeros((WINDOW, 1), F32)
            for b in range(4):
                x = rows[b, 2 * u + k].astype(F32)
                squared += jnp.sum(x * x, axis=1, keepdims=True)
            scale = lax.rsqrt(squared / 2048.0 + EPS)
            for b in range(4):
                x = rows[b, 2 * u + k].astype(F32)
                normed[WINDOW * k : WINDOW * k + WINDOW, 512 * b : 512 * b + 512] = (
                    x * scale * gain_pre_ref[:, 512 * b : 512 * b + 512]
                ).astype(BF16)

        for j in range(tiles):
            both = jnp.dot(
                normed[...], whole[:, 256 * j : 256 * j + 256], preferred_element_type=F32
            )
            gate, up = both[:, :128], both[:, 128:]
            hidden[:, 128 * j : 128 * j + 128] = (gate / (1.0 + jnp.exp(-gate)) * up).astype(BF16)

        def part(block, half):
            at = pl.ds(pl.multiple_of(block * 512 + 256 * half, 256), 256)
            return lax.dot_general(
                hidden[...], whole[at, inner : inner + units], NT, preferred_element_type=F32
            ).astype(BF16)

        f_scatter.first(u, part)

    def feed_sum(u):
        half0, half1 = f_scatter.last(u)
        f_total[u, :, :256] = half0
        f_total[u, :, 256:] = half1
        f_sums.give(u, half0, half1)

    def finish(u):
        scale = lax.rsqrt(f_sums.take(u) / 2048.0 + EPS)
        for k in range(2):
            part = pl.ds(WINDOW * k, WINDOW)
            at = pl.ds(place(2 * u + k), WINDOW)
            done[at, :] = (
                rows[me, 2 * u + k].astype(F32)
                + 0.5 * (f_total[u, part, :] * scale[WINDOW * k : WINDOW * k + WINDOW] * gain_post)
            ).astype(BF16)
            result(2 * u + k).start()

    def result(slot):
        at = pl.ds(place(slot), WINDOW)
        return pltpu.make_async_copy(done.at[at, :], out_hbm.at[at, :], out_sem)

    def drain(slot):
        mixing.drain(slot)
        sums.drain(slot)
        feeding.drain(slot)

    def f_drain(u):
        f_scatter.drain(u)
        f_sums.drain(u)

    def step(t, carry):
        def when(lag, fn):
            @pl.when((t >= lag) & (t < chunks + lag))
            def _():
                fn(t - lag)

        def when_fed(times, fn):
            now, index = t == times[0], 0
            for n in times[1:]:
                now, index = now | (t == n), index + (t >= n).astype(jnp.int32)

            @pl.when(now)
            def _():
                fn(index)

        when(0, attention)
        when(1, mixing.relay)

        for n in range(1, 5):
            @pl.when(t == PROJECTION[n])
            def _():
                projection.step(n)
                if n == 2:
                    weights.open(0, 0)
                    weights.open(1, 1)

        when(MIX, mix)
        when(MIX + 1, first_rows)
        when(MIX + 2, feeding.relay)
        when(MIX + 3, feeding.close)

        for n in range(9):
            for way in (0, 1):
                @pl.when(t == WEIGHTS[way][n])
                def _():
                    weights.step(way, n)

        when_fed(FEED, feed)
        when_fed(SECOND, f_scatter.second)
        when_fed(SUM, feed_sum)
        when_fed(FINISH, finish)
        when(DRAIN, drain)

        @pl.when(t == SECOND[0])
        def _():
            halos.wait_send()
            weights.drain()
            projection.drain()

        when_fed(FINISH[1:], f_drain)
        return carry

    lax.fori_loop(0, FINISH[-1] + 1, step, 0)
    f_drain(half_chunks - 1)
    pltpu.make_async_copy(done, out_hbm, out_sem).wait()


def sems(*shapes):
    return [pltpu.SemaphoreType.DMA(s) for s in shapes]


def body(
    residual, rotated_query_rows, rotated_key_rows, value_matrix_rows, head_sink_logit,
    out_proj, gain_mix, gain_pre, gain_post, gate_proj, up_proj, down_proj,
):
    length = residual.shape[0]
    chunks = length // WINDOW
    half = chunks // 2
    units = gate_proj.shape[1]
    sp_count = lax.axis_size("sp")
    full = sp_count * gate_proj.shape[0]
    big = 2 * WINDOW
    vmem = pl.BlockSpec(memory_space=pltpu.VMEM)
    smem = pl.BlockSpec(memory_space=pltpu.SMEM)
    hbm = pl.BlockSpec(memory_space=pl.ANY)
    loaded = (
        residual, rotated_query_rows, rotated_key_rows, value_matrix_rows, out_proj,
        gate_proj, up_proj, down_proj.T,
    )
    return pl.pallas_call(
        functools.partial(layer_kernel, chunks, sp_count),
        out_shape=jax.ShapeDtypeStruct(residual.shape, BF16),
        in_specs=[hbm] * 4 + [smem, hbm] + [vmem] * 3 + [hbm] * 3,
        out_specs=hbm,
        scratch_shapes=[pltpu.VMEM(residual.shape, BF16)]
        + [pltpu.VMEM(a.shape, BF16) for a in loaded]
        + [pltpu.VMEM((full, 3 * units), BF16)]
        + [pltpu.VMEM((length + big, 128), BF16)] * 4
        + [
            pltpu.VMEM((4, out_proj.shape[0], 512), BF16),
            pltpu.VMEM((4, chunks, WINDOW, 384), BF16),
            pltpu.VMEM((chunks, WINDOW, 512), F32),
            pltpu.VMEM((chunks, 8, 128), F32),
            pltpu.VMEM((chunks, 3, 8, 128), F32),
            pltpu.VMEM((4, chunks, WINDOW, 512), BF16),
            pltpu.VMEM((big, full), BF16),
            pltpu.VMEM((big, units), BF16),
            pltpu.VMEM((half, 6, big, 256), BF16),
            pltpu.VMEM((half, 6, big, 256), BF16),
            pltpu.VMEM((half, big, 512), BF16),
            pltpu.VMEM((half, big, 512), F32),
            pltpu.VMEM((half, 16, 128), F32),
            pltpu.VMEM((half, 3, 16, 128), F32),
        ]
        + [pltpu.SemaphoreType.DMA]
        + sems((8,), (2, 5), (2, 5, 2), (2, 4), (2, 4))
        + [pltpu.SemaphoreType.DMA] * 2
        + sems((3,), (4,), (chunks,), (chunks, 2), (chunks,), (chunks,), (chunks,), (chunks, 2))
        + sems((half,), (half, 2), (half,), (half,)),
        compiler_params=pltpu.CompilerParams(
            collective_id=0, has_side_effects=True, vmem_limit_bytes=54 * 2**20
        ),
    )(
        residual, rotated_query_rows, rotated_key_rows, value_matrix_rows, head_sink_logit,
        out_proj, gain_mix[None], gain_pre[None], gain_post[None], *loaded[5:],
    )


def solution(mesh):
    placed = (
        P("sp", "tp"), P("sp", "tp"), P("sp", "tp"), P("sp", "tp"), P("tp"), P("tp", None),
        P(), P(), P(), P("sp", "tp"), P("sp", "tp"), P("tp", "sp"),
    )
    return jax.shard_map(body, mesh=mesh, in_specs=placed, out_specs=P("sp", "tp"), check_vma=False)
```

```python
import functools

import jax
import jax.numpy as jnp
from jax import lax
from jax.experimental import pallas as pl
from jax.experimental.pallas import tpu as pltpu
from jax.sharding import PartitionSpec as P

WINDOW = 128
EPS = 1e-06
MIX = 4
PROJECTION = (0, 1, 2, 3, 4)
WEIGHTS = (2, 2, 4, 4, 4, 7, 8, 9, 11), (2, 2, 6, 4, 4, 8, 9, 10, 11)
PREPARE, FEED, SECOND = (11, 12, 13, 14), (12, 13, 14, 15), (13, 14, 15, 16)
SUM, FINISH = (14, 15, 16, 17), (15, 16, 17, 18)
DRAIN = 9
MESH = pl.DeviceIdType.MESH
F32 = jnp.float32
BF16 = jnp.bfloat16
NT = (((1,), (1,)), ((), ()))


def ring():
    me = lax.axis_index("tp")
    right, left, far = (lax.rem(me + k, 4) for k in (1, 3, 2))
    return me, right, left, far


def tp_copy(src, dst, send, recv, to):
    return pltpu.make_async_remote_copy(
        src_ref=src, dst_ref=dst, send_sem=send, recv_sem=recv,
        device_id={"tp": to}, device_id_type=MESH,
    )


class Scatter:
    def __init__(self, sent, got, own, send, recv):
        self.sent, self.got, self.own, self.send, self.recv = sent, got, own, send, recv
        self.me, self.right, self.left, self.far = ring()

    def copy(self, slot, m):
        to = self.right if m % 2 == 0 else self.left
        return tp_copy(
            self.sent.at[slot, m], self.got.at[slot, m],
            self.send.at[slot], self.recv.at[slot, 0 if m < 2 else 1], to,
        )

    def arrived(self, slot, group):
        ref = self.got.at[slot, pl.ds(2 * group, 2 + 2 * group)]
        tp_copy(ref, ref, self.send.at[slot], self.recv.at[slot, group], self.right).wait_recv()

    def first(self, slot, part):
        self.sent[slot, 0] = part(self.far, 0)
        self.sent[slot, 1] = part(self.far, 1)
        self.copy(slot, 0).start()
        self.copy(slot, 1).start()
        self.sent[slot, 2] = part(self.right, 1)
        self.sent[slot, 3] = part(self.left, 0)
        self.copy(slot, 2).start()
        self.copy(slot, 3).start()
        self.sent[slot, 4] = part(self.right, 0)
        self.sent[slot, 5] = part(self.left, 1)
        self.own[slot, :, :256] = part(self.me, 0)
        self.own[slot, :, 256:] = part(self.me, 1)

    def second(self, slot):
        self.arrived(slot, 0)
        for k in (0, 1):
            total = self.sent[slot, 4 + k].astype(F32) + self.got[slot, k].astype(F32)
            self.sent[slot, 4 + k] = total.astype(BF16)
            self.copy(slot, 4 + k).start()

    def last(self, slot):
        self.arrived(slot, 1)
        half0 = (
            self.own[slot, :, :256].astype(F32)
            + self.got[slot, 4].astype(F32)
            + self.got[slot, 3].astype(F32)
        )
        half1 = (
            self.own[slot, :, 256:].astype(F32)
            + self.got[slot, 2].astype(F32)
            + self.got[slot, 5].astype(F32)
        )
        return half0, half1

    def drain(self, slot):
        ref = self.sent.at[slot]
        tp_copy(ref, ref, self.send.at[slot], self.recv.at[slot, 0], self.right).wait_send()


class Squares:
    def __init__(self, mine, got, send, recv):
        self.mine, self.got, self.send, self.recv = mine, got, send, recv
        self.me, self.right, self.left, self.far = ring()

    def copies(self, slot):
        for m, to in enumerate((self.right, self.left, self.far)):
            yield tp_copy(
                self.mine.at[slot], self.got.at[slot, m],
                self.send.at[slot], self.recv.at[slot], to,
            )

    def all(self, slot):
        ref = self.got.at[slot]
        return tp_copy(ref, ref, self.send.at[slot], self.recv.at[slot], self.right)

    def give(self, slot, half0, half1):
        total = jnp.sum(half0 * half0, axis=1, keepdims=True) + jnp.sum(
            half1 * half1, axis=1, keepdims=True
        )
        for g in range(total.shape[0] // 128):
            wide = jnp.broadcast_to(total[128 * g : 128 * g + 128], (128, 128))
            self.mine[slot, 8 * g : 8 * g + 8] = wide.T[:8]
        for copy in self.copies(slot):
            copy.start()

    def take(self, slot):
        self.all(slot).wait_recv()
        total = self.mine[slot] + self.got[slot, 0] + self.got[slot, 1] + self.got[slot, 2]
        columns = [
            jnp.broadcast_to(total[8 * g : 8 * g + 1], (128, 128)).T[:, :1]
            for g in range(total.shape[0] // 8)
        ]
        return columns[0] if len(columns) == 1 else jnp.concatenate(columns, axis=0)

    def drain(self, slot):
        self.all(slot).wait_send()


class Gather:
    def __init__(self, buffer, send, recv):
        self.buffer, self.send, self.recv = buffer, send, recv
        self.me, self.right, self.left, self.far = ring()

    def copy(self, slot, owner, to, group, part):
        ref = self.buffer.at[owner, slot, part]
        return tp_copy(ref, ref, self.send.at[slot], self.recv.at[slot, group], to)

    def some(self, slot, blocks, group):
        ref = self.buffer.at[pl.ds(0, blocks), slot]
        return tp_copy(ref, ref, self.send.at[slot], self.recv.at[slot, group], self.right)

    def open(self, slot):
        whole = pl.ds(0, WINDOW)
        self.copy(slot, self.me, self.right, 0, whole).start()
        self.copy(slot, self.me, self.left, 0, whole).start()

    def relay(self, slot):
        self.some(slot, 2, 0).wait_recv()
        self.copy(slot, self.left, self.right, 1, pl.ds(0, WINDOW // 2)).start()
        self.copy(slot, self.right, self.left, 1, pl.ds(WINDOW // 2, WINDOW // 2)).start()

    def close(self, slot):
        self.some(slot, 1, 1).wait_recv()

    def drain(self, slot):
        self.some(slot, 3, 0).wait_send()


class Projection:
    def __init__(self, taken, source, send, recv):
        self.taken, self.source, self.send, self.recv = taken, source, send, recv
        self.me, self.right, self.left, self.far = ring()
        sp = lax.axis_index("sp")
        self.core, self.y, self.rest = lax.rem(sp, 2), lax.rem(lax.div(sp, 2), 4), lax.div(sp, 8) * 8
        self.depth = source.shape[0] // 8

    def columns(self, owner):
        return pl.ds(pl.multiple_of(owner * 512, 512), 512)

    def eighth(self, dy):
        start = (2 * lax.rem(self.y + dy, 4) + self.core) * self.depth
        return pl.ds(pl.multiple_of(start, self.depth), self.depth)

    def to_sp(self, dy, core):
        return {"sp": self.rest + 2 * lax.rem(self.y + dy, 4) + core}

    def copy(self, src, dst, n, group, to):
        return pltpu.make_async_remote_copy(
            src_ref=src, dst_ref=dst, send_sem=self.send.at[n], recv_sem=self.recv.at[group],
            device_id=to, device_id_type=MESH,
        )

    def piece(self, dy, n, group, to, part=None):
        ref = self.taken.at[pl.ds(1, 3), self.eighth(dy), pl.ds(*(part or (0, 512)))]
        return self.copy(ref, ref, n, group, to)

    def some(self, n, group, pieces):
        ref = self.taken.at[pl.ds(1, 3), pl.ds(0, pieces * self.depth)]
        return self.copy(ref, ref, n, group, {"tp": self.right})

    def across(self, dy):
        self.piece(dy, 2, 3, self.to_sp(0, 1 - self.core)).start()

    def step(self, n):
        if n == 0:
            rows = self.eighth(0)
            for to, k in ((self.right, 3), (self.left, 1), (self.far, 2)):
                self.copy(
                    self.source.at[rows, self.columns(to)], self.taken.at[k, rows], 0, 0, {"tp": to}
                ).start()
        elif n == 1:
            self.some(0, 0, 1).wait_recv()
            self.piece(0, 1, 1, self.to_sp(1, self.core)).start()
            self.piece(0, 1, 1, self.to_sp(3, self.core)).start()
            self.across(0)
        elif n == 2:
            self.some(1, 1, 2).wait_recv()
            self.piece(3, 1, 2, self.to_sp(1, self.core), (0, 256)).start()
            self.piece(1, 1, 2, self.to_sp(3, self.core), (256, 256)).start()
            self.across(1)
            self.across(3)
        elif n == 3:
            self.some(1, 2, 1).wait_recv()
            self.across(2)
        elif n == 4:
            self.some(2, 3, 4).wait_recv()

    def drain(self):
        for n, pieces in enumerate((1, 3, 4)):
            self.some(n, 0, pieces).wait_send()


def attend(row, first_key, q_ref, kv, sink_ref, lowest, highest):
    keys, keys_turned, values, values_turned = (
        a[pl.ds(first_key, 3 * WINDOW), :] for a in kv
    )
    lane = lax.broadcasted_iota(jnp.int32, (WINDOW, 128), 1)
    query = lax.broadcasted_iota(jnp.int32, (WINDOW, 3 * WINDOW), 0)
    key = lax.broadcasted_iota(jnp.int32, (WINDOW, 3 * WINDOW), 1)
    inside = (key >= query) & (key <= query + 2 * WINDOW) & (key >= lowest) & (key < highest)
    tiles = []
    for t in range(3):
        pair = q_ref[pl.ds(row, WINDOW), 128 * t : 128 * t + 128].astype(F32) * 0.125
        outs = []
        for half in range(2):
            h = 2 * t + half
            turned = (h // 3) != half
            q = jnp.where((lane >= 64) == (half == 1), pair, 0.0).astype(BF16)
            scores = lax.dot_general(
                q, keys_turned if turned else keys, NT, preferred_element_type=F32
            )
            scores = jnp.where(inside, scores, -1e30)
            sink = sink_ref[h]
            top = jnp.maximum(jnp.max(scores, axis=1, keepdims=True), sink)
            e = jnp.exp(scores - top)
            below = jnp.sum(e, axis=1, keepdims=True) + jnp.exp(sink - top)
            out = jnp.dot(
                e.astype(BF16), values_turned if turned else values,
                preferred_element_type=F32,
            )
            outs.append(out * (1.0 / below))
        tiles.append(jnp.where(lane < 64, outs[0], outs[1]).astype(BF16))
    return jnp.concatenate(tiles, axis=1)


def turn(x):
    return pltpu.roll(x.astype(F32), 64, 1).astype(BF16)


class Weights:
    across = (0, 1, 3, 2)

    def __init__(self, whole, send, recv, core_send, core_recv):
        self.whole, self.send, self.recv = whole, send, recv
        self.core_send, self.core_recv = core_send, core_recv
        sp = lax.axis_index("sp")
        self.core, self.y, self.z = lax.rem(sp, 2), lax.rem(lax.div(sp, 2), 4), lax.div(sp, 8)

    def device(self, way, a, b, core):
        dy, dz = (a, b) if way == 0 else (b, a)
        return (lax.rem(self.z + dz, 4) * 4 + lax.rem(self.y + dy, 4)) * 2 + core

    def neighbours(self):
        ring = [self.device(0, a, b, self.core) for a, b in ((1, 0), (3, 0), (0, 1), (0, 3))]
        return ring + [self.device(0, 0, 0, 1 - self.core)]

    def rows(self, way, a, b, core, part=None):
        start = self.device(way, a, b, core) * 64 + 32 * way
        if part is None:
            return self.whole.at[pl.ds(pl.multiple_of(start, 32), 32), :]
        return self.whole.at[pl.ds(pl.multiple_of(start + 16 * part, 16), 16), :]

    def at(self, stage, k):
        return (k, 0) if stage == 0 else (self.across[stage - 1], k)

    def copy(self, way, stage, m):
        offset = (0, 0, 3, 1)[m]
        ref = self.rows(way, *self.at(stage, offset), self.core, None if m < 2 else m - 2)
        to = self.device(way, *((1 if m % 2 == 0 else 3, 0) if stage == 0 else (0, 1 if m % 2 == 0 else 3)), self.core)
        return pltpu.make_async_remote_copy(
            src_ref=ref, dst_ref=ref,
            send_sem=self.send.at[way, stage], recv_sem=self.recv.at[way, stage, 0 if m < 2 else 1],
            device_id={"sp": to}, device_id_type=MESH,
        )

    def over(self, way, a, b):
        ref = self.rows(way, a, b, self.core)
        return pltpu.make_async_remote_copy(
            src_ref=ref, dst_ref=ref,
            send_sem=self.core_send.at[way, a], recv_sem=self.core_recv.at[way, a],
            device_id={"sp": self.device(way, 0, 0, 1 - self.core)}, device_id_type=MESH,
        )

    def some(self, count, send, recv):
        ref = self.whole.at[pl.ds(0, count), :]
        return pltpu.make_async_remote_copy(
            src_ref=ref, dst_ref=ref, send_sem=send, recv_sem=recv,
            device_id={"sp": self.device(0, 0, 0, 1 - self.core)}, device_id_type=MESH,
        )

    def open(self, way, stage):
        self.copy(way, stage, 0).start()
        self.copy(way, stage, 1).start()

    def relay(self, way, stage):
        self.some(64, self.send.at[way, stage], self.recv.at[way, stage, 0]).wait_recv()
        self.copy(way, stage, 2).start()
        self.copy(way, stage, 3).start()

    def share(self, way, stage, ks):
        for k in ks:
            self.over(way, *self.at(stage, k)).start()

    def close(self, way, stage):
        self.some(32, self.send.at[way, stage], self.recv.at[way, stage, 1]).wait_recv()
        self.share(way, stage, (2,))

    def step(self, way, n):
        if n == 0:
            self.relay(way, 0)
            self.share(way, 0, (1, 3))
        elif n == 1:
            if way == 1:
                self.open(1, 1)
            self.open(way, 2)
            self.open(way, 3)
        elif n == 2:
            self.relay(way, 1)
            self.share(way, 1, (1, 3))
        elif n == 3:
            self.close(way, 0)
        elif n == 4:
            self.open(way, 4)
        elif n == 5:
            for stage in (2, 3):
                self.relay(way, stage)
                self.share(way, stage, (1, 3))
        elif n == 6:
            self.close(way, 1)
            self.relay(way, 4)
            self.share(way, 4, (1, 3))
        elif n == 7:
            for stage in (2, 3, 4):
                self.close(way, stage)
        elif n == 8:
            for a in range(4):
                self.some(128, self.core_send.at[way, a], self.core_recv.at[way, a]).wait_recv()

    def drain(self):
        for way in (0, 1):
            for stage in range(5):
                self.some(96, self.send.at[way, stage], self.recv.at[way, stage, 0]).wait_send()
            for a in range(4):
                self.some(128, self.core_send.at[way, a], self.core_recv.at[way, a]).wait_send()


def layer_kernel(
    chunks, sp_count,
    res_hbm, q_hbm, k_hbm, v_hbm, sink_ref, proj_hbm, gain_mix_ref, gain_pre_ref, gain_post_ref,
    gate_hbm, up_hbm, down_hbm,
    out_hbm,
    done, res_ref, q_ref, k_ref, v_ref, proj_ref, gate_ref, up_ref, down_ref,
    whole, keys, keys_turned, values, values_turned, taken, att,
    mixed, mine, squares, rows,
    normed, hidden, f_sent, f_got, f_own, f_total, f_mine, f_squares,
    out_sem, load_sem, w_send, w_recv, core_send, core_recv,
    halo_send, halo_recv, p_send, p_recv, at_send, at_recv, sq_send, sq_recv, ag_send, ag_recv,
    f_rs_send, f_rs_recv, f_sq_send, f_sq_recv,
):
    me, right, left, far = ring()
    sp = lax.axis_index("sp")
    after = lax.rem(sp + 1, sp_count)
    before = lax.rem(sp + sp_count - 1, sp_count)
    length = chunks * WINDOW
    half_chunks = chunks // 2
    units = gate_ref.shape[1]
    tiles = units // 128
    inner = 2 * units
    loads = [
        pltpu.make_async_copy(a, b, load_sem.at[n])
        for n, (a, b) in enumerate((
            (proj_hbm, proj_ref), (k_hbm, k_ref), (v_hbm, v_ref), (gate_hbm, gate_ref),
            (up_hbm, up_ref), (down_hbm, down_ref), (q_hbm, q_ref), (res_hbm, res_ref),
        ))
    ]
    for load in loads:
        load.start()
    weights = Weights(whole, w_send, w_recv, core_send, core_recv)
    barrier = pltpu.get_barrier_semaphore()
    others = [{"tp": right}, {"tp": left}, {"tp": far}, {"sp": after}, {"sp": before}]
    others += [{"sp": n} for n in weights.neighbours()]
    for other in others:
        pl.semaphore_signal(barrier, inc=1, device_id=other, device_id_type=MESH)
    for load in loads[:3]:
        load.wait()
    pl.semaphore_wait(barrier, len(others))

    def halo(n):
        mine_ref, both = ((k_ref, keys), (v_ref, values))[n // 2]
        if n % 2 == 0:
            src, dst, to = mine_ref.at[pl.ds(length - WINDOW, WINDOW)], both.at[pl.ds(0, WINDOW)], after
        else:
            src, dst, to = mine_ref.at[pl.ds(0, WINDOW)], both.at[pl.ds(length + WINDOW, WINDOW)], before
        return pltpu.make_async_remote_copy(
            src_ref=src, dst_ref=dst, send_sem=halo_send, recv_sem=halo_recv,
            device_id={"sp": to}, device_id_type=MESH,
        )

    projection = Projection(taken, proj_ref, p_send, p_recv)
    projection.step(0)
    halos = keys.at[pl.ds(0, 4 * WINDOW)]
    halos = tp_copy(halos, halos, halo_send, halo_recv, right)
    for n in range(4):
        halo(n).start()
    for load in loads[3:6]:
        load.wait()
    shard = pl.ds(pl.multiple_of(sp * 64, 64), 64)
    for j in range(tiles):
        whole[shard, 256 * j : 256 * j + 128] = gate_ref[:, 128 * j : 128 * j + 128]
        whole[shard, 256 * j + 128 : 256 * j + 256] = up_ref[:, 128 * j : 128 * j + 128]
        whole[shard, inner + 128 * j : inner + 128 * j + 128] = (
            down_ref[:, 128 * j : 128 * j + 128]
        )
    middle = pl.ds(WINDOW, length)
    keys[middle, :] = k_ref[...]
    values[middle, :] = v_ref[...]
    keys_turned[middle, :] = turn(k_ref[...])
    values_turned[middle, :] = turn(v_ref[...])
    weights.open(0, 0)
    weights.open(1, 0)
    weights.open(0, 1)
    weights.over(0, 0, 0).start()
    weights.over(1, 0, 0).start()
    for load in loads[6:]:
        load.wait()
    taken[0] = proj_ref[:, projection.columns(me)]

    mixing = Gather(att, at_send, at_recv)
    feeding = Gather(rows, ag_send, ag_recv)
    sums = Squares(mine, squares, sq_send, sq_recv)
    f_scatter = Scatter(f_sent, f_got, f_own, f_rs_send, f_rs_recv)
    f_sums = Squares(f_mine, f_squares, f_sq_send, f_sq_recv)
    columns = pl.ds(pl.multiple_of(me * 512, 512), 512)
    gain_mix = gain_mix_ref[:, columns]
    gain_post = gain_post_ref[:, columns]

    def place(slot):
        return pl.multiple_of(lax.rem(slot + 1, chunks) * WINDOW, WINDOW)

    def attention(t):
        @pl.when(t == chunks - 2)
        def _():
            halos.wait_recv()
            for at in (0, length + WINDOW):
                keys_turned[pl.ds(at, WINDOW), :] = turn(keys[pl.ds(at, WINDOW), :])
                values_turned[pl.ds(at, WINDOW), :] = turn(values[pl.ds(at, WINDOW), :])

        row = place(t)
        lowest = jnp.where((sp == 0) & (t == chunks - 1), WINDOW, 0)
        highest = jnp.where((sp == sp_count - 1) & (t == chunks - 2), 2 * WINDOW, 3 * WINDOW)
        att[me, t] = attend(
            row, row, q_ref, (keys, keys_turned, values, values_turned), sink_ref, lowest, highest
        )
        mixing.open(t)

    def mix(s):
        mixing.close(s)
        total = jnp.zeros((WINDOW, 512), F32)
        for k, owner in enumerate((me, right, far, left)):
            total += jnp.dot(att[owner, s], taken[k], preferred_element_type=F32)
        mixed[s] = total
        sums.give(s, total[:, :256], total[:, 256:])

    def first_rows(s):
        scale = lax.rsqrt(sums.take(s) / 2048.0 + EPS)
        res = res_ref[pl.ds(place(s), WINDOW), :].astype(F32)
        rows[me, s] = (res + mixed[s] * scale * gain_mix).astype(BF16)
        feeding.open(s)

    def prepare(u):
        for k in range(2):
            squared = jnp.zeros((WINDOW, 1), F32)
            for b in range(4):
                x = rows[b, 2 * u + k].astype(F32)
                squared += jnp.sum(x * x, axis=1, keepdims=True)
            scale = lax.rsqrt(squared / 2048.0 + EPS)
            for b in range(4):
                x = rows[b, 2 * u + k].astype(F32)
                normed[WINDOW * k : WINDOW * k + WINDOW, 512 * b : 512 * b + 512] = (
                    x * scale * gain_pre_ref[:, 512 * b : 512 * b + 512]
                ).astype(BF16)

        for j in range(tiles):
            both = jnp.dot(
                normed[...], whole[:, 256 * j : 256 * j + 256], preferred_element_type=F32
            )
            gate, up = both[:, :128], both[:, 128:]
            hidden[lax.rem(u, 2), :, 128 * j : 128 * j + 128] = (gate / (1.0 + jnp.exp(-gate)) * up).astype(BF16)

    def feed(u):
        def part(block, half):
            at = pl.ds(pl.multiple_of(block * 512 + 256 * half, 256), 256)
            return lax.dot_general(
                hidden[lax.rem(u, 2)], whole[at, inner : inner + units], NT,
                preferred_element_type=F32,
            ).astype(BF16)

        f_scatter.first(u, part)

    def feed_sum(u):
        half0, half1 = f_scatter.last(u)
        f_total[u, :, :256] = half0
        f_total[u, :, 256:] = half1
        f_sums.give(u, half0, half1)

    def finish(u):
        scale = lax.rsqrt(f_sums.take(u) / 2048.0 + EPS)
        for k in range(2):
            part = pl.ds(WINDOW * k, WINDOW)
            at = pl.ds(place(2 * u + k), WINDOW)
            done[at, :] = (
                rows[me, 2 * u + k].astype(F32)
                + 0.5 * (f_total[u, part, :] * scale[WINDOW * k : WINDOW * k + WINDOW] * gain_post)
            ).astype(BF16)
            result(2 * u + k).start()

    def result(slot):
        at = pl.ds(place(slot), WINDOW)
        return pltpu.make_async_copy(done.at[at, :], out_hbm.at[at, :], out_sem)

    def drain(slot):
        mixing.drain(slot)
        sums.drain(slot)
        feeding.drain(slot)

    def f_drain(u):
        f_scatter.drain(u)
        f_sums.drain(u)

    def step(t, carry):
        def when(lag, fn):
            @pl.when((t >= lag) & (t < chunks + lag))
            def _():
                fn(t - lag)

        def when_fed(times, fn):
            now, index = t == times[0], 0
            for n in times[1:]:
                now, index = now | (t == n), index + (t >= n).astype(jnp.int32)

            @pl.when(now)
            def _():
                fn(index)

        when(0, attention)
        when(1, mixing.relay)

        for n in range(1, 5):
            @pl.when(t == PROJECTION[n])
            def _():
                projection.step(n)

        when(MIX, mix)
        when(MIX + 1, first_rows)

        for n in range(9):
            for way in (0, 1):
                @pl.when(t == WEIGHTS[way][n])
                def _():
                    weights.step(way, n)

        when_fed(PREPARE[:3], prepare)
        when(MIX + 2, feeding.relay)
        when(MIX + 3, feeding.close)

        @pl.when(t == PREPARE[3])
        def _():
            prepare(3)


        when_fed(FEED, feed)
        when_fed(SECOND, f_scatter.second)
        when_fed(SUM, feed_sum)
        when_fed(FINISH, finish)
        when(DRAIN, drain)

        @pl.when(t == SECOND[0])
        def _():
            halos.wait_send()
            weights.drain()
            projection.drain()

        when_fed(FINISH[1:], f_drain)
        return carry

    lax.fori_loop(0, FINISH[-1] + 1, step, 0)
    f_drain(half_chunks - 1)
    pltpu.make_async_copy(done, out_hbm, out_sem).wait()


def sems(*shapes):
    return [pltpu.SemaphoreType.DMA(s) for s in shapes]


def body(
    residual, rotated_query_rows, rotated_key_rows, value_matrix_rows, head_sink_logit,
    out_proj, gain_mix, gain_pre, gain_post, gate_proj, up_proj, down_proj,
):
    length = residual.shape[0]
    chunks = length // WINDOW
    half = chunks // 2
    units = gate_proj.shape[1]
    sp_count = lax.axis_size("sp")
    full = sp_count * gate_proj.shape[0]
    big = 2 * WINDOW
    vmem = pl.BlockSpec(memory_space=pltpu.VMEM)
    smem = pl.BlockSpec(memory_space=pltpu.SMEM)
    hbm = pl.BlockSpec(memory_space=pl.ANY)
    loaded = (
        residual, rotated_query_rows, rotated_key_rows, value_matrix_rows, out_proj,
        gate_proj, up_proj, down_proj.T,
    )
    return pl.pallas_call(
        functools.partial(layer_kernel, chunks, sp_count),
        out_shape=jax.ShapeDtypeStruct(residual.shape, BF16),
        in_specs=[hbm] * 4 + [smem, hbm] + [vmem] * 3 + [hbm] * 3,
        out_specs=hbm,
        scratch_shapes=[pltpu.VMEM(residual.shape, BF16)]
        + [pltpu.VMEM(a.shape, BF16) for a in loaded]
        + [pltpu.VMEM((full, 3 * units), BF16)]
        + [pltpu.VMEM((length + big, 128), BF16)] * 4
        + [
            pltpu.VMEM((4, out_proj.shape[0], 512), BF16),
            pltpu.VMEM((4, chunks, WINDOW, 384), BF16),
            pltpu.VMEM((chunks, WINDOW, 512), F32),
            pltpu.VMEM((chunks, 8, 128), F32),
            pltpu.VMEM((chunks, 3, 8, 128), F32),
            pltpu.VMEM((4, chunks, WINDOW, 512), BF16),
            pltpu.VMEM((big, full), BF16),
            pltpu.VMEM((2, big, units), BF16),
            pltpu.VMEM((half, 6, big, 256), BF16),
            pltpu.VMEM((half, 6, big, 256), BF16),
            pltpu.VMEM((half, big, 512), BF16),
            pltpu.VMEM((half, big, 512), F32),
            pltpu.VMEM((half, 16, 128), F32),
            pltpu.VMEM((half, 3, 16, 128), F32),
        ]
        + [pltpu.SemaphoreType.DMA]
        + sems((8,), (2, 5), (2, 5, 2), (2, 4), (2, 4))
        + [pltpu.SemaphoreType.DMA] * 2
        + sems((3,), (4,), (chunks,), (chunks, 2), (chunks,), (chunks,), (chunks,), (chunks, 2))
        + sems((half,), (half, 2), (half,), (half,)),
        compiler_params=pltpu.CompilerParams(
            collective_id=0, has_side_effects=True, vmem_limit_bytes=54 * 2**20
        ),
    )(
        residual, rotated_query_rows, rotated_key_rows, value_matrix_rows, head_sink_logit,
        out_proj, gain_mix[None], gain_pre[None], gain_post[None], *loaded[5:],
    )


def solution(mesh):
    placed = (
        P("sp", "tp"), P("sp", "tp"), P("sp", "tp"), P("sp", "tp"), P("tp"), P("tp", None),
        P(), P(), P(), P("sp", "tp"), P("sp", "tp"), P("tp", "sp"),
    )
    return jax.shard_map(body, mesh=mesh, in_specs=placed, out_specs=P("sp", "tp"), check_vma=False)
```

```python
import functools

import jax
import jax.numpy as jnp
from jax import lax
from jax.experimental import pallas as pl
from jax.experimental.pallas import tpu as pltpu
from jax.sharding import PartitionSpec as P

WINDOW = 128
EPS = 1e-06
MIX = 4
PIECES = 4
PROJECTION = (0, 1, 2, 3, 4)
WEIGHTS = (2, 2, 4, 4, 4, 7, 8, 9, 11), (2, 2, 6, 4, 4, 8, 9, 10, 11)
PREPARE, FEED, SECOND = (11, 12, 13, 14), (12, 13, 14, 15), (13, 14, 15, 16)
SUM, FINISH = (14, 15, 16, 17), (15, 16, 17, 18)
MESH = pl.DeviceIdType.MESH
F32 = jnp.float32
BF16 = jnp.bfloat16
NT = (((1,), (1,)), ((), ()))


def ring():
    me = lax.axis_index("tp")
    right, left, far = (lax.rem(me + k, 4) for k in (1, 3, 2))
    return me, right, left, far


def tp_copy(src, dst, send, recv, to):
    return pltpu.make_async_remote_copy(
        src_ref=src, dst_ref=dst, send_sem=send, recv_sem=recv,
        device_id={"tp": to}, device_id_type=MESH,
    )


class Scatter:
    def __init__(self, sent, got, own, send, recv):
        self.sent, self.got, self.own, self.send, self.recv = sent, got, own, send, recv
        self.me, self.right, self.left, self.far = ring()

    def copy(self, slot, m):
        to = self.right if m % 2 == 0 else self.left
        return tp_copy(
            self.sent.at[slot, m], self.got.at[slot, m],
            self.send, self.recv.at[slot, 0 if m < 2 else 1], to,
        )

    def arrived(self, slot, group):
        ref = self.got.at[slot, pl.ds(2 * group, 2 + 2 * group)]
        tp_copy(ref, ref, self.send, self.recv.at[slot, group], self.right).wait_recv()

    def first(self, slot, part):
        self.sent[slot, 0] = part(self.far, 0)
        self.sent[slot, 1] = part(self.far, 1)
        self.copy(slot, 0).start()
        self.copy(slot, 1).start()
        self.sent[slot, 2] = part(self.right, 1)
        self.sent[slot, 3] = part(self.left, 0)
        self.copy(slot, 2).start()
        self.copy(slot, 3).start()
        self.sent[slot, 4] = part(self.right, 0)
        self.sent[slot, 5] = part(self.left, 1)
        self.own[slot, :, :256] = part(self.me, 0)
        self.own[slot, :, 256:] = part(self.me, 1)

    def second(self, slot):
        self.arrived(slot, 0)
        for k in (0, 1):
            total = self.sent[slot, 4 + k].astype(F32) + self.got[slot, k].astype(F32)
            self.sent[slot, 4 + k] = total.astype(BF16)
            self.copy(slot, 4 + k).start()

    def last(self, slot):
        self.arrived(slot, 1)
        half0 = (
            self.own[slot, :, :256].astype(F32)
            + self.got[slot, 4].astype(F32)
            + self.got[slot, 3].astype(F32)
        )
        half1 = (
            self.own[slot, :, 256:].astype(F32)
            + self.got[slot, 2].astype(F32)
            + self.got[slot, 5].astype(F32)
        )
        return half0, half1

    def drain(self):
        tp_copy(self.sent, self.sent, self.send, self.recv.at[0, 0], self.right).wait_send()


class Squares:
    def __init__(self, mine, got, send, recv):
        self.mine, self.got, self.send, self.recv = mine, got, send, recv
        self.me, self.right, self.left, self.far = ring()

    def copies(self, slot):
        for m, to in enumerate((self.right, self.left, self.far)):
            yield tp_copy(
                self.mine.at[slot], self.got.at[slot, m],
                self.send, self.recv.at[slot], to,
            )

    def all(self, slot):
        ref = self.got.at[slot]
        return tp_copy(ref, ref, self.send, self.recv.at[slot], self.right)

    def give(self, slot, half0, half1):
        total = jnp.sum(half0 * half0, axis=1, keepdims=True) + jnp.sum(
            half1 * half1, axis=1, keepdims=True
        )
        for g in range(total.shape[0] // 128):
            wide = jnp.broadcast_to(total[128 * g : 128 * g + 128], (128, 128))
            self.mine[slot, 8 * g : 8 * g + 8] = wide.T[:8]
        for copy in self.copies(slot):
            copy.start()

    def take(self, slot):
        self.all(slot).wait_recv()
        total = self.mine[slot] + self.got[slot, 0] + self.got[slot, 1] + self.got[slot, 2]
        columns = [
            jnp.broadcast_to(total[8 * g : 8 * g + 1], (128, 128)).T[:, :1]
            for g in range(total.shape[0] // 8)
        ]
        return columns[0] if len(columns) == 1 else jnp.concatenate(columns, axis=0)

    def drain(self):
        tp_copy(self.got, self.got, self.send, self.recv.at[0], self.right).wait_send()


class Gather:
    def __init__(self, buffer, send, recv):
        self.buffer, self.send, self.recv = buffer, send, recv
        self.me, self.right, self.left, self.far = ring()

    def copy(self, slot, owner, to, group, part):
        ref = self.buffer.at[owner, slot, part]
        return tp_copy(ref, ref, self.send, self.recv.at[slot, group], to)

    def some(self, slot, blocks, group):
        ref = self.buffer.at[pl.ds(0, blocks), slot]
        return tp_copy(ref, ref, self.send, self.recv.at[slot, group], self.right)

    def open(self, slot):
        whole = pl.ds(0, WINDOW)
        self.copy(slot, self.me, self.right, 0, whole).start()
        self.copy(slot, self.me, self.left, 0, whole).start()

    def relay(self, slot):
        self.some(slot, 2, 0).wait_recv()
        self.copy(slot, self.left, self.right, 1, pl.ds(0, WINDOW // 2)).start()
        self.copy(slot, self.right, self.left, 1, pl.ds(WINDOW // 2, WINDOW // 2)).start()

    def close(self, slot):
        self.some(slot, 1, 1).wait_recv()

    def drain(self):
        ref = self.buffer.at[pl.ds(0, 3)]
        tp_copy(ref, ref, self.send, self.recv.at[0, 0], self.right).wait_send()


class Projection:
    def __init__(self, taken, source, send, recv):
        self.taken, self.source, self.send, self.recv = taken, source, send, recv
        self.me, self.right, self.left, self.far = ring()
        sp = lax.axis_index("sp")
        self.core, self.y, self.rest = lax.rem(sp, 2), lax.rem(lax.div(sp, 2), 4), lax.div(sp, 8) * 8
        self.depth = source.shape[0] // 8

    def columns(self, owner):
        return pl.ds(pl.multiple_of(owner * 512, 512), 512)

    def eighth(self, dy):
        start = (2 * lax.rem(self.y + dy, 4) + self.core) * self.depth
        return pl.ds(pl.multiple_of(start, self.depth), self.depth)

    def to_sp(self, dy, core):
        return {"sp": self.rest + 2 * lax.rem(self.y + dy, 4) + core}

    def copy(self, src, dst, n, group, to):
        return pltpu.make_async_remote_copy(
            src_ref=src, dst_ref=dst, send_sem=self.send.at[n], recv_sem=self.recv.at[group],
            device_id=to, device_id_type=MESH,
        )

    def piece(self, dy, n, group, to, part=None):
        ref = self.taken.at[pl.ds(1, 3), self.eighth(dy), pl.ds(*(part or (0, 512)))]
        return self.copy(ref, ref, n, group, to)

    def some(self, n, group, pieces):
        ref = self.taken.at[pl.ds(1, 3), pl.ds(0, pieces * self.depth)]
        return self.copy(ref, ref, n, group, {"tp": self.right})

    def across(self, dy):
        self.piece(dy, 2, 3, self.to_sp(0, 1 - self.core)).start()

    def step(self, n):
        if n == 0:
            rows = self.eighth(0)
            for to, k in ((self.right, 3), (self.left, 1), (self.far, 2)):
                self.copy(
                    self.source.at[rows, self.columns(to)], self.taken.at[k, rows], 0, 0, {"tp": to}
                ).start()
        elif n == 1:
            self.some(0, 0, 1).wait_recv()
            self.piece(0, 1, 1, self.to_sp(1, self.core)).start()
            self.piece(0, 1, 1, self.to_sp(3, self.core)).start()
            self.across(0)
        elif n == 2:
            self.some(1, 1, 2).wait_recv()
            self.piece(3, 1, 2, self.to_sp(1, self.core), (0, 256)).start()
            self.piece(1, 1, 2, self.to_sp(3, self.core), (256, 256)).start()
            self.across(1)
            self.across(3)
        elif n == 3:
            self.some(1, 2, 1).wait_recv()
            self.across(2)
        elif n == 4:
            self.some(2, 3, 4).wait_recv()

    def drain(self):
        for n, pieces in enumerate((1, 3, 4)):
            self.some(n, 0, pieces).wait_send()


def attend(row, first_key, q_ref, kv, sink_ref, lowest, highest):
    keys, keys_turned, values, values_turned = (
        a[pl.ds(first_key, 3 * WINDOW), :] for a in kv
    )
    lane = lax.broadcasted_iota(jnp.int32, (WINDOW, 128), 1)
    query = lax.broadcasted_iota(jnp.int32, (WINDOW, 3 * WINDOW), 0)
    key = lax.broadcasted_iota(jnp.int32, (WINDOW, 3 * WINDOW), 1)
    inside = (key >= query) & (key <= query + 2 * WINDOW) & (key >= lowest) & (key < highest)
    tiles = []
    for t in range(3):
        pair = q_ref[pl.ds(row, WINDOW), 128 * t : 128 * t + 128].astype(F32) * 0.125
        outs = []
        for half in range(2):
            h = 2 * t + half
            turned = (h // 3) != half
            q = jnp.where((lane >= 64) == (half == 1), pair, 0.0).astype(BF16)
            scores = lax.dot_general(
                q, keys_turned if turned else keys, NT, preferred_element_type=F32
            )
            scores = jnp.where(inside, scores, -1e30)
            sink = sink_ref[h]
            top = jnp.maximum(jnp.max(scores, axis=1, keepdims=True), sink)
            e = jnp.exp(scores - top)
            below = jnp.sum(e, axis=1, keepdims=True) + jnp.exp(sink - top)
            out = jnp.dot(
                e.astype(BF16), values_turned if turned else values,
                preferred_element_type=F32,
            )
            outs.append(out * (1.0 / below))
        tiles.append(jnp.where(lane < 64, outs[0], outs[1]).astype(BF16))
    return jnp.concatenate(tiles, axis=1)


def turn(x):
    return pltpu.roll(x.astype(F32), 64, 1).astype(BF16)


class Weights:
    across = (0, 1, 3, 2)

    def __init__(self, whole, send, recv, core_send, core_recv):
        self.whole, self.send, self.recv = whole, send, recv
        self.core_send, self.core_recv = core_send, core_recv
        sp = lax.axis_index("sp")
        self.core, self.y, self.z = lax.rem(sp, 2), lax.rem(lax.div(sp, 2), 4), lax.div(sp, 8)

    def device(self, way, a, b, core):
        dy, dz = (a, b) if way == 0 else (b, a)
        return (lax.rem(self.z + dz, 4) * 4 + lax.rem(self.y + dy, 4)) * 2 + core

    def neighbours(self):
        ring = [self.device(0, a, b, self.core) for a, b in ((1, 0), (3, 0), (0, 1), (0, 3))]
        return ring + [self.device(0, 0, 0, 1 - self.core)]

    def rows(self, way, a, b, core, part=None):
        start = self.device(way, a, b, core) * 64 + 32 * way
        if part is None:
            return self.whole.at[pl.ds(pl.multiple_of(start, 32), 32), :]
        return self.whole.at[pl.ds(pl.multiple_of(start + 16 * part, 16), 16), :]

    def at(self, stage, k):
        return (k, 0) if stage == 0 else (self.across[stage - 1], k)

    def copy(self, way, stage, m):
        offset = (0, 0, 3, 1)[m]
        ref = self.rows(way, *self.at(stage, offset), self.core, None if m < 2 else m - 2)
        to = self.device(way, *((1 if m % 2 == 0 else 3, 0) if stage == 0 else (0, 1 if m % 2 == 0 else 3)), self.core)
        return pltpu.make_async_remote_copy(
            src_ref=ref, dst_ref=ref,
            send_sem=self.send.at[way], recv_sem=self.recv.at[way, stage, 0 if m < 2 else 1],
            device_id={"sp": to}, device_id_type=MESH,
        )

    def over(self, way, a, b):
        ref = self.rows(way, a, b, self.core)
        return pltpu.make_async_remote_copy(
            src_ref=ref, dst_ref=ref,
            send_sem=self.core_send.at[way], recv_sem=self.core_recv.at[way],
            device_id={"sp": self.device(way, 0, 0, 1 - self.core)}, device_id_type=MESH,
        )

    def some(self, count, send, recv):
        ref = self.whole.at[pl.ds(0, count), :]
        return pltpu.make_async_remote_copy(
            src_ref=ref, dst_ref=ref, send_sem=send, recv_sem=recv,
            device_id={"sp": self.device(0, 0, 0, 1 - self.core)}, device_id_type=MESH,
        )

    def open(self, way, stage):
        self.copy(way, stage, 0).start()
        self.copy(way, stage, 1).start()

    def relay(self, way, stage):
        self.some(64, self.send.at[way], self.recv.at[way, stage, 0]).wait_recv()
        self.copy(way, stage, 2).start()
        self.copy(way, stage, 3).start()

    def share(self, way, stage, ks):
        for k in ks:
            self.over(way, *self.at(stage, k)).start()

    def close(self, way, stage):
        self.some(32, self.send.at[way], self.recv.at[way, stage, 1]).wait_recv()
        self.share(way, stage, (2,))

    def step(self, way, n):
        if n == 0:
            self.relay(way, 0)
            self.share(way, 0, (1, 3))
        elif n == 1:
            if way == 1:
                self.open(1, 1)
            self.open(way, 2)
            self.open(way, 3)
        elif n == 2:
            self.relay(way, 1)
            self.share(way, 1, (1, 3))
        elif n == 3:
            self.close(way, 0)
        elif n == 4:
            self.open(way, 4)
        elif n == 5:
            for stage in (2, 3):
                self.relay(way, stage)
                self.share(way, stage, (1, 3))
        elif n == 6:
            self.close(way, 1)
            self.relay(way, 4)
            self.share(way, 4, (1, 3))
        elif n == 7:
            for stage in (2, 3, 4):
                self.close(way, stage)
        elif n == 8:
            self.some(512, self.core_send.at[way], self.core_recv.at[way]).wait_recv()

    def drain(self):
        for way in (0, 1):
            self.some(480, self.send.at[way], self.recv.at[way, 0, 0]).wait_send()
            self.some(512, self.core_send.at[way], self.core_recv.at[way]).wait_send()


def layer_kernel(
    chunks, sp_count,
    res_hbm, q_hbm, k_hbm, v_hbm, sink_ref, proj_hbm, gain_mix_ref, gain_pre_ref, gain_post_ref,
    gate_hbm, up_hbm, down_hbm,
    out_hbm,
    done, res_ref, q_ref, k_ref, v_ref, gate_ref, up_ref, down_ref,
    whole, keys, keys_turned, values, values_turned, taken, att,
    mixed, mine, squares, rows,
    normed, hidden, f_sent, f_got, f_own, f_total, f_mine, f_squares,
    out_sem, load_sem, w_send, w_recv, core_send, core_recv,
    halo_send, halo_recv, p_send, p_recv, at_send, at_recv, sq_send, sq_recv, ag_send, ag_recv,
    f_rs_send, f_rs_recv, f_sq_send, f_sq_recv,
):
    me, right, left, far = ring()
    sp = lax.axis_index("sp")
    after = lax.rem(sp + 1, sp_count)
    before = lax.rem(sp + sp_count - 1, sp_count)
    length = chunks * WINDOW
    half_chunks = chunks // 2
    units = gate_ref.shape[1]
    tiles = units // 128
    inner = 2 * units
    projection = Projection(taken, proj_hbm, p_send, p_recv)
    loads = [
        pltpu.make_async_copy(a, b, load_sem.at[n])
        for n, (a, b) in enumerate((
            (proj_hbm.at[:, projection.columns(me)], taken.at[0]), (k_hbm, k_ref), (v_hbm, v_ref), (gate_hbm, gate_ref),
            (up_hbm, up_ref), (down_hbm, down_ref), (q_hbm, q_ref), (res_hbm, res_ref),
        ))
    ]
    for load in loads:
        load.start()
    weights = Weights(whole, w_send, w_recv, core_send, core_recv)
    barrier = pltpu.get_barrier_semaphore()
    others = [{"tp": right}, {"tp": left}, {"tp": far}, {"sp": after}, {"sp": before}]
    others += [{"sp": n} for n in weights.neighbours()]
    for other in others:
        pl.semaphore_signal(barrier, inc=1, device_id=other, device_id_type=MESH)
    pl.semaphore_wait(barrier, len(others))
    projection.step(0)
    for load in loads[1:3]:
        load.wait()

    def halo(n):
        mine_ref, both = ((k_ref, keys), (v_ref, values))[n // 2]
        if n % 2 == 0:
            src, dst, to = mine_ref.at[pl.ds(length - WINDOW, WINDOW)], both.at[pl.ds(0, WINDOW)], after
        else:
            src, dst, to = mine_ref.at[pl.ds(0, WINDOW)], both.at[pl.ds(length + WINDOW, WINDOW)], before
        return pltpu.make_async_remote_copy(
            src_ref=src, dst_ref=dst, send_sem=halo_send, recv_sem=halo_recv,
            device_id={"sp": to}, device_id_type=MESH,
        )

    halos = keys.at[pl.ds(0, 4 * WINDOW)]
    halos = tp_copy(halos, halos, halo_send, halo_recv, right)
    for n in range(4):
        halo(n).start()
    for load in loads[3:6]:
        load.wait()
    shard = pl.ds(pl.multiple_of(sp * 64, 64), 64)
    for j in range(tiles):
        whole[shard, 256 * j : 256 * j + 128] = gate_ref[:, 128 * j : 128 * j + 128]
        whole[shard, 256 * j + 128 : 256 * j + 256] = up_ref[:, 128 * j : 128 * j + 128]
        whole[shard, inner + 128 * j : inner + 128 * j + 128] = (
            down_ref[:, 128 * j : 128 * j + 128]
        )
    middle = pl.ds(WINDOW, length)
    keys[middle, :] = k_ref[...]
    values[middle, :] = v_ref[...]
    keys_turned[middle, :] = turn(k_ref[...])
    values_turned[middle, :] = turn(v_ref[...])
    weights.open(0, 0)
    weights.open(1, 0)
    weights.open(0, 1)
    weights.over(0, 0, 0).start()
    weights.over(1, 0, 0).start()
    for load in loads[6:] + loads[:1]:
        load.wait()

    mixing = Gather(att, at_send, at_recv)
    feeding = Gather(rows, ag_send, ag_recv)
    sums = Squares(mine, squares, sq_send, sq_recv)
    f_scatter = Scatter(f_sent, f_got, f_own, f_rs_send, f_rs_recv)
    f_sums = Squares(f_mine, f_squares, f_sq_send, f_sq_recv)
    columns = pl.ds(pl.multiple_of(me * 512, 512), 512)
    gain_mix = gain_mix_ref[:, columns]
    gain_post = gain_post_ref[:, columns]

    def place(slot):
        return pl.multiple_of(lax.rem(slot + 1, chunks) * WINDOW, WINDOW)

    def attention(t):
        @pl.when(t == chunks - 2)
        def _():
            halos.wait_recv()
            for at in (0, length + WINDOW):
                keys_turned[pl.ds(at, WINDOW), :] = turn(keys[pl.ds(at, WINDOW), :])
                values_turned[pl.ds(at, WINDOW), :] = turn(values[pl.ds(at, WINDOW), :])

        row = place(t)
        lowest = jnp.where((sp == 0) & (t == chunks - 1), WINDOW, 0)
        highest = jnp.where((sp == sp_count - 1) & (t == chunks - 2), 2 * WINDOW, 3 * WINDOW)
        att[me, t] = attend(
            row, row, q_ref, (keys, keys_turned, values, values_turned), sink_ref, lowest, highest
        )
        mixing.open(t)

    def mix(s):
        mixing.close(s)
        total = jnp.zeros((WINDOW, 512), F32)
        for k, owner in enumerate((me, right, far, left)):
            total += jnp.dot(att[owner, s], taken[k], preferred_element_type=F32)
        mixed[s] = total
        sums.give(s, total[:, :256], total[:, 256:])

    def first_rows(s):
        scale = lax.rsqrt(sums.take(s) / 2048.0 + EPS)
        res = res_ref[pl.ds(place(s), WINDOW), :].astype(F32)
        rows[me, s] = (res + mixed[s] * scale * gain_mix).astype(BF16)
        feeding.open(s)

    def prepare(u):
        for k in range(2):
            squared = jnp.zeros((WINDOW, 1), F32)
            for b in range(4):
                x = rows[b, 2 * u + k].astype(F32)
                squared += jnp.sum(x * x, axis=1, keepdims=True)
            scale = lax.rsqrt(squared / 2048.0 + EPS)
            for b in range(4):
                x = rows[b, 2 * u + k].astype(F32)
                normed[WINDOW * k : WINDOW * k + WINDOW, 512 * b : 512 * b + 512] = (
                    x * scale * gain_pre_ref[:, 512 * b : 512 * b + 512]
                ).astype(BF16)

        for j in range(tiles):
            both = jnp.dot(
                normed[...], whole[:, 256 * j : 256 * j + 256], preferred_element_type=F32
            )
            gate, up = both[:, :128], both[:, 128:]
            hidden[lax.rem(u, 2), :, 128 * j : 128 * j + 128] = (gate / (1.0 + jnp.exp(-gate)) * up).astype(BF16)

    def feed(u):
        def part(block, half):
            at = pl.ds(pl.multiple_of(block * 512 + 256 * half, 256), 256)
            return lax.dot_general(
                hidden[lax.rem(u, 2)], whole[at, inner : inner + units], NT,
                preferred_element_type=F32,
            ).astype(BF16)

        f_scatter.first(u, part)

    def feed_sum(u):
        half0, half1 = f_scatter.last(u)
        f_total[u, :, :256] = half0
        f_total[u, :, 256:] = half1
        f_sums.give(u, half0, half1)

    def finish(u):
        scale = lax.rsqrt(f_sums.take(u) / 2048.0 + EPS)
        for k in range(2):
            part = pl.ds(WINDOW * k, WINDOW)
            at = pl.ds(place(2 * u + k), WINDOW)
            done[at, :] = (
                rows[me, 2 * u + k].astype(F32)
                + 0.5 * (f_total[u, part, :] * scale[WINDOW * k : WINDOW * k + WINDOW] * gain_post)
            ).astype(BF16)
            result(2 * u + k).start()

    def result(slot):
        at = pl.ds(place(slot), WINDOW)
        return pltpu.make_async_copy(done.at[at, :], out_hbm.at[at, :], out_sem)

    def step(t, carry):
        def when(lag, fn):
            @pl.when((t >= lag) & (t < chunks + lag))
            def _():
                fn(t - lag)

        def when_fed(times, fn):
            now, index = t == times[0], 0
            for n in times[1:]:
                now, index = now | (t == n), index + (t >= n).astype(jnp.int32)

            @pl.when(now)
            def _():
                fn(index)

        when(0, attention)
        when(1, mixing.relay)

        for n in range(1, 5):
            @pl.when(t == PROJECTION[n])
            def _():
                projection.step(n)

        when(MIX, mix)
        when(MIX + 1, first_rows)

        for n in range(9):
            for way in (0, 1):
                @pl.when(t == WEIGHTS[way][n])
                def _():
                    weights.step(way, n)

        when_fed(PREPARE[:3], prepare)
        when(MIX + 2, feeding.relay)
        when(MIX + 3, feeding.close)

        @pl.when(t == PREPARE[3])
        def _():
            prepare(3)


        when_fed(FEED, feed)
        when_fed(SECOND, f_scatter.second)
        when_fed(SUM, feed_sum)
        when_fed(FINISH, finish)
        @pl.when(t == FEED[3])
        def _():
            halos.wait_send()
            weights.drain()
            projection.drain()
            mixing.drain()
            feeding.drain()
            sums.drain()

        return carry

    lax.fori_loop(0, FINISH[-1] + 1, step, 0)
    f_scatter.drain()
    f_sums.drain()
    pltpu.make_async_copy(done, out_hbm, out_sem).wait()


def pass_kernel(in_hbm, out_hbm, held, in_sem, out_sem):
    size = held.shape[0] // PIECES
    ins, outs = [], []
    for n in range(PIECES):
        at = pl.ds(n * size, size)
        ins.append(pltpu.make_async_copy(in_hbm.at[at, :], held.at[at, :], in_sem.at[n]))
        outs.append(pltpu.make_async_copy(held.at[at, :], out_hbm.at[at, :], out_sem))
    for copy in ins:
        copy.start()
    for copy, out in zip(ins, outs):
        copy.wait()
        out.start()
    pltpu.make_async_copy(held, out_hbm, out_sem).wait()


def sems(*shapes):
    return [pltpu.SemaphoreType.DMA(s) for s in shapes]


def body(
    residual, rotated_query_rows, rotated_key_rows, value_matrix_rows, head_sink_logit,
    out_proj, gain_mix, gain_pre, gain_post, gate_proj, up_proj, down_proj,
):
    length = residual.shape[0]
    chunks = length // WINDOW
    half = chunks // 2
    units = gate_proj.shape[1]
    sp_count = lax.axis_size("sp")
    full = sp_count * gate_proj.shape[0]
    big = 2 * WINDOW
    vmem = pl.BlockSpec(memory_space=pltpu.VMEM)
    smem = pl.BlockSpec(memory_space=pltpu.SMEM)
    hbm = pl.BlockSpec(memory_space=pl.ANY)
    loaded = (
        residual, rotated_query_rows, rotated_key_rows, value_matrix_rows, out_proj,
        gate_proj, up_proj, down_proj.T,
    )
    result = pl.pallas_call(
        functools.partial(layer_kernel, chunks, sp_count),
        out_shape=jax.ShapeDtypeStruct(residual.shape, BF16),
        in_specs=[hbm] * 4 + [smem, hbm] + [vmem] * 3 + [hbm] * 3,
        out_specs=hbm,
        scratch_shapes=[pltpu.VMEM(residual.shape, BF16)]
        + [pltpu.VMEM(a.shape, BF16) for a in loaded[:4] + loaded[5:]]
        + [pltpu.VMEM((full, 3 * units), BF16)]
        + [pltpu.VMEM((length + big, 128), BF16)] * 4
        + [
            pltpu.VMEM((4, out_proj.shape[0], 512), BF16),
            pltpu.VMEM((4, chunks, WINDOW, 384), BF16),
            pltpu.VMEM((chunks, WINDOW, 512), F32),
            pltpu.VMEM((chunks, 8, 128), F32),
            pltpu.VMEM((chunks, 3, 8, 128), F32),
            pltpu.VMEM((4, chunks, WINDOW, 512), BF16),
            pltpu.VMEM((big, full), BF16),
            pltpu.VMEM((2, big, units), BF16),
            pltpu.VMEM((half, 6, big, 256), BF16),
            pltpu.VMEM((half, 6, big, 256), BF16),
            pltpu.VMEM((half, big, 512), BF16),
            pltpu.VMEM((half, big, 512), F32),
            pltpu.VMEM((half, 16, 128), F32),
            pltpu.VMEM((half, 3, 16, 128), F32),
        ]
        + [pltpu.SemaphoreType.DMA]
        + sems((8,), (2,), (2, 5, 2), (2,), (2,), (), (), (3,), (4,), (), (chunks, 2), (), (chunks,))
        + sems((), (chunks, 2), (), (half, 2), (), (half,)),
        compiler_params=pltpu.CompilerParams(
            collective_id=0, has_side_effects=True, vmem_limit_bytes=54 * 2**20
        ),
    )(
        residual, rotated_query_rows, rotated_key_rows, value_matrix_rows, head_sink_logit,
        out_proj, gain_mix[None], gain_pre[None], gain_post[None], *loaded[5:],
    )
    return pl.pallas_call(
        pass_kernel,
        out_shape=jax.ShapeDtypeStruct(residual.shape, BF16),
        in_specs=[hbm],
        out_specs=hbm,
        scratch_shapes=[pltpu.VMEM(residual.shape, BF16)] + sems((PIECES,), ()),
    )(result)


def solution(mesh):
    placed = (
        P("sp", "tp"), P("sp", "tp"), P("sp", "tp"), P("sp", "tp"), P("tp"), P("tp", None),
        P(), P(), P(), P("sp", "tp"), P("sp", "tp"), P("tp", "sp"),
    )
    return jax.shard_map(body, mesh=mesh, in_specs=placed, out_specs=P("sp", "tp"), check_vma=False)
```

```python
import functools

import jax
import jax.numpy as jnp
from jax import lax
from jax.experimental import pallas as pl
from jax.experimental.pallas import tpu as pltpu
from jax.sharding import PartitionSpec as P

WINDOW = 128
EPS = 1e-06
MIX = 4
PIECES = 4
PROJECTION = (0, 1, 2, 3, 4)
WEIGHTS = (2, 2, 4, 4, 4, 7, 8, 9, 11), (2, 2, 6, 4, 4, 8, 9, 10, 11)
PREPARE, FEED, SECOND = (11, 12, 13, 14), (12, 13, 14, 15), (13, 14, 15, 16)
SUM, FINISH = (14, 15, 16, 17), (15, 16, 17, 18)
MESH = pl.DeviceIdType.MESH
F32 = jnp.float32
BF16 = jnp.bfloat16
NT = (((1,), (1,)), ((), ()))


def ring():
    me = lax.axis_index("tp")
    right, left, far = (lax.rem(me + k, 4) for k in (1, 3, 2))
    return me, right, left, far


def tp_copy(src, dst, send, recv, to):
    return pltpu.make_async_remote_copy(
        src_ref=src, dst_ref=dst, send_sem=send, recv_sem=recv,
        device_id={"tp": to}, device_id_type=MESH,
    )


class Scatter:
    def __init__(self, sent, got, own, send, recv):
        self.sent, self.got, self.own, self.send, self.recv = sent, got, own, send, recv
        self.me, self.right, self.left, self.far = ring()

    def copy(self, slot, m):
        to = self.right if m % 2 == 0 else self.left
        return tp_copy(
            self.sent.at[slot, m], self.got.at[slot, m],
            self.send, self.recv.at[slot, 0 if m < 2 else 1], to,
        )

    def arrived(self, slot, group):
        ref = self.got.at[slot, pl.ds(2 * group, 2 + 2 * group)]
        tp_copy(ref, ref, self.send, self.recv.at[slot, group], self.right).wait_recv()

    def first(self, slot, part):
        self.sent[slot, 0] = part(self.far, 0)
        self.sent[slot, 1] = part(self.far, 1)
        self.copy(slot, 0).start()
        self.copy(slot, 1).start()
        self.sent[slot, 2] = part(self.right, 1)
        self.sent[slot, 3] = part(self.left, 0)
        self.copy(slot, 2).start()
        self.copy(slot, 3).start()
        self.sent[slot, 4] = part(self.right, 0)
        self.sent[slot, 5] = part(self.left, 1)
        self.own[slot, :, :256] = part(self.me, 0)
        self.own[slot, :, 256:] = part(self.me, 1)

    def second(self, slot):
        self.arrived(slot, 0)
        for k in (0, 1):
            total = self.sent[slot, 4 + k].astype(F32) + self.got[slot, k].astype(F32)
            self.sent[slot, 4 + k] = total.astype(BF16)
            self.copy(slot, 4 + k).start()

    def last(self, slot):
        self.arrived(slot, 1)
        half0 = (
            self.own[slot, :, :256].astype(F32)
            + self.got[slot, 4].astype(F32)
            + self.got[slot, 3].astype(F32)
        )
        half1 = (
            self.own[slot, :, 256:].astype(F32)
            + self.got[slot, 2].astype(F32)
            + self.got[slot, 5].astype(F32)
        )
        return half0, half1

    def drain(self):
        tp_copy(self.sent, self.sent, self.send, self.recv.at[0, 0], self.right).wait_send()


class Squares:
    def __init__(self, mine, got, send, recv):
        self.mine, self.got, self.send, self.recv = mine, got, send, recv
        self.me, self.right, self.left, self.far = ring()

    def copies(self, slot):
        for m, to in enumerate((self.right, self.left, self.far)):
            yield tp_copy(
                self.mine.at[slot], self.got.at[slot, m],
                self.send, self.recv.at[slot], to,
            )

    def all(self, slot):
        ref = self.got.at[slot]
        return tp_copy(ref, ref, self.send, self.recv.at[slot], self.right)

    def give(self, slot, half0, half1):
        total = jnp.sum(half0 * half0, axis=1, keepdims=True) + jnp.sum(
            half1 * half1, axis=1, keepdims=True
        )
        for g in range(total.shape[0] // 128):
            wide = jnp.broadcast_to(total[128 * g : 128 * g + 128], (128, 128))
            self.mine[slot, 8 * g : 8 * g + 8] = wide.T[:8]
        for copy in self.copies(slot):
            copy.start()

    def take(self, slot):
        self.all(slot).wait_recv()
        total = self.mine[slot] + self.got[slot, 0] + self.got[slot, 1] + self.got[slot, 2]
        columns = [
            jnp.broadcast_to(total[8 * g : 8 * g + 1], (128, 128)).T[:, :1]
            for g in range(total.shape[0] // 8)
        ]
        return columns[0] if len(columns) == 1 else jnp.concatenate(columns, axis=0)

    def drain(self):
        tp_copy(self.got, self.got, self.send, self.recv.at[0], self.right).wait_send()


class Gather:
    def __init__(self, buffer, send, recv):
        self.buffer, self.send, self.recv = buffer, send, recv
        self.me, self.right, self.left, self.far = ring()

    def copy(self, slot, owner, to, group, part):
        ref = self.buffer.at[owner, slot, part]
        return tp_copy(ref, ref, self.send, self.recv.at[slot, group], to)

    def some(self, slot, blocks, group):
        ref = self.buffer.at[pl.ds(0, blocks), slot]
        return tp_copy(ref, ref, self.send, self.recv.at[slot, group], self.right)

    def open(self, slot):
        whole = pl.ds(0, WINDOW)
        self.copy(slot, self.me, self.right, 0, whole).start()
        self.copy(slot, self.me, self.left, 0, whole).start()

    def relay(self, slot):
        self.some(slot, 2, 0).wait_recv()
        self.copy(slot, self.left, self.right, 1, pl.ds(0, WINDOW // 2)).start()
        self.copy(slot, self.right, self.left, 1, pl.ds(WINDOW // 2, WINDOW // 2)).start()

    def close(self, slot):
        self.some(slot, 1, 1).wait_recv()

    def drain(self):
        ref = self.buffer.at[pl.ds(0, 3)]
        tp_copy(ref, ref, self.send, self.recv.at[0, 0], self.right).wait_send()


class Projection:
    def __init__(self, taken, source, send, recv):
        self.taken, self.source, self.send, self.recv = taken, source, send, recv
        self.me, self.right, self.left, self.far = ring()
        sp = lax.axis_index("sp")
        self.core, self.y, self.rest = lax.rem(sp, 2), lax.rem(lax.div(sp, 2), 4), lax.div(sp, 8) * 8
        self.depth = source.shape[0] // 8

    def columns(self, owner):
        return pl.ds(pl.multiple_of(owner * 512, 512), 512)

    def eighth(self, dy):
        start = (2 * lax.rem(self.y + dy, 4) + self.core) * self.depth
        return pl.ds(pl.multiple_of(start, self.depth), self.depth)

    def to_sp(self, dy, core):
        return {"sp": self.rest + 2 * lax.rem(self.y + dy, 4) + core}

    def copy(self, src, dst, n, group, to):
        return pltpu.make_async_remote_copy(
            src_ref=src, dst_ref=dst, send_sem=self.send.at[n], recv_sem=self.recv.at[group],
            device_id=to, device_id_type=MESH,
        )

    def piece(self, dy, n, group, to, part=None):
        ref = self.taken.at[pl.ds(1, 3), self.eighth(dy), pl.ds(*(part or (0, 512)))]
        return self.copy(ref, ref, n, group, to)

    def some(self, n, group, pieces):
        ref = self.taken.at[pl.ds(1, 3), pl.ds(0, pieces * self.depth)]
        return self.copy(ref, ref, n, group, {"tp": self.right})

    def across(self, dy):
        self.piece(dy, 2, 3, self.to_sp(0, 1 - self.core)).start()

    def step(self, n):
        if n == 0:
            rows = self.eighth(0)
            for to, k in ((self.right, 3), (self.left, 1), (self.far, 2)):
                self.copy(
                    self.source.at[rows, self.columns(to)], self.taken.at[k, rows], 0, 0, {"tp": to}
                ).start()
        elif n == 1:
            self.some(0, 0, 1).wait_recv()
            self.piece(0, 1, 1, self.to_sp(1, self.core)).start()
            self.piece(0, 1, 1, self.to_sp(3, self.core)).start()
            self.across(0)
        elif n == 2:
            self.some(1, 1, 2).wait_recv()
            self.piece(3, 1, 2, self.to_sp(1, self.core), (0, 256)).start()
            self.piece(1, 1, 2, self.to_sp(3, self.core), (256, 256)).start()
            self.across(1)
            self.across(3)
        elif n == 3:
            self.some(1, 2, 1).wait_recv()
            self.across(2)
        elif n == 4:
            self.some(2, 3, 4).wait_recv()

    def drain(self):
        for n, pieces in enumerate((1, 3, 4)):
            self.some(n, 0, pieces).wait_send()


def attend(row, first_key, q_ref, kv, sink_ref, lowest, highest):
    keys, keys_turned, values, values_turned = (
        a[pl.ds(first_key, 3 * WINDOW), :] for a in kv
    )
    lane = lax.broadcasted_iota(jnp.int32, (WINDOW, 128), 1)
    query = lax.broadcasted_iota(jnp.int32, (WINDOW, 3 * WINDOW), 0)
    key = lax.broadcasted_iota(jnp.int32, (WINDOW, 3 * WINDOW), 1)
    inside = (key >= query) & (key <= query + 2 * WINDOW) & (key >= lowest) & (key < highest)
    tiles = []
    for t in range(3):
        pair = q_ref[pl.ds(row, WINDOW), 128 * t : 128 * t + 128].astype(F32) * 0.125
        outs = []
        for half in range(2):
            h = 2 * t + half
            turned = (h // 3) != half
            q = jnp.where((lane >= 64) == (half == 1), pair, 0.0).astype(BF16)
            scores = lax.dot_general(
                q, keys_turned if turned else keys, NT, preferred_element_type=F32
            )
            scores = jnp.where(inside, scores, -1e30)
            sink = sink_ref[h]
            top = jnp.maximum(jnp.max(scores, axis=1, keepdims=True), sink)
            e = jnp.exp(scores - top)
            below = jnp.sum(e, axis=1, keepdims=True) + jnp.exp(sink - top)
            out = jnp.dot(
                e.astype(BF16), values_turned if turned else values,
                preferred_element_type=F32,
            )
            outs.append(out * (1.0 / below))
        tiles.append(jnp.where(lane < 64, outs[0], outs[1]).astype(BF16))
    return jnp.concatenate(tiles, axis=1)


def turn(x):
    return pltpu.roll(x.astype(F32), 64, 1).astype(BF16)


class Weights:
    across = (0, 1, 3, 2)

    def __init__(self, whole, send, recv, core_send, core_recv):
        self.whole, self.send, self.recv = whole, send, recv
        self.core_send, self.core_recv = core_send, core_recv
        sp = lax.axis_index("sp")
        self.core, self.y, self.z = lax.rem(sp, 2), lax.rem(lax.div(sp, 2), 4), lax.div(sp, 8)

    def device(self, way, a, b, core):
        dy, dz = (a, b) if way == 0 else (b, a)
        return (lax.rem(self.z + dz, 4) * 4 + lax.rem(self.y + dy, 4)) * 2 + core

    def neighbours(self):
        ring = [self.device(0, a, b, self.core) for a, b in ((1, 0), (3, 0), (0, 1), (0, 3))]
        return ring + [self.device(0, 0, 0, 1 - self.core)]

    def rows(self, way, a, b, core, part=None):
        start = self.device(way, a, b, core) * 64 + 32 * way
        if part is None:
            return self.whole.at[pl.ds(pl.multiple_of(start, 32), 32), :]
        return self.whole.at[pl.ds(pl.multiple_of(start + 16 * part, 16), 16), :]

    def at(self, stage, k):
        return (k, 0) if stage == 0 else (self.across[stage - 1], k)

    def copy(self, way, stage, m):
        offset = (0, 0, 3, 1)[m]
        ref = self.rows(way, *self.at(stage, offset), self.core, None if m < 2 else m - 2)
        to = self.device(way, *((1 if m % 2 == 0 else 3, 0) if stage == 0 else (0, 1 if m % 2 == 0 else 3)), self.core)
        return pltpu.make_async_remote_copy(
            src_ref=ref, dst_ref=ref,
            send_sem=self.send.at[way], recv_sem=self.recv.at[way, stage, 0 if m < 2 else 1],
            device_id={"sp": to}, device_id_type=MESH,
        )

    def over(self, way, a, b):
        ref = self.rows(way, a, b, self.core)
        return pltpu.make_async_remote_copy(
            src_ref=ref, dst_ref=ref,
            send_sem=self.core_send.at[way], recv_sem=self.core_recv.at[way],
            device_id={"sp": self.device(way, 0, 0, 1 - self.core)}, device_id_type=MESH,
        )

    def some(self, count, send, recv):
        ref = self.whole.at[pl.ds(0, count), :]
        return pltpu.make_async_remote_copy(
            src_ref=ref, dst_ref=ref, send_sem=send, recv_sem=recv,
            device_id={"sp": self.device(0, 0, 0, 1 - self.core)}, device_id_type=MESH,
        )

    def open(self, way, stage):
        self.copy(way, stage, 0).start()
        self.copy(way, stage, 1).start()

    def relay(self, way, stage):
        self.some(64, self.send.at[way], self.recv.at[way, stage, 0]).wait_recv()
        self.copy(way, stage, 2).start()
        self.copy(way, stage, 3).start()

    def share(self, way, stage, ks):
        for k in ks:
            self.over(way, *self.at(stage, k)).start()

    def close(self, way, stage):
        self.some(32, self.send.at[way], self.recv.at[way, stage, 1]).wait_recv()
        self.share(way, stage, (2,))

    def step(self, way, n):
        if n == 0:
            self.relay(way, 0)
            self.share(way, 0, (1, 3))
        elif n == 1:
            if way == 1:
                self.open(1, 1)
            self.open(way, 2)
            self.open(way, 3)
        elif n == 2:
            self.relay(way, 1)
            self.share(way, 1, (1, 3))
        elif n == 3:
            self.close(way, 0)
        elif n == 4:
            self.open(way, 4)
        elif n == 5:
            for stage in (2, 3):
                self.relay(way, stage)
                self.share(way, stage, (1, 3))
        elif n == 6:
            self.close(way, 1)
            self.relay(way, 4)
            self.share(way, 4, (1, 3))
        elif n == 7:
            for stage in (2, 3, 4):
                self.close(way, stage)
        elif n == 8:
            self.some(512, self.core_send.at[way], self.core_recv.at[way]).wait_recv()

    def drain(self):
        for way in (0, 1):
            self.some(480, self.send.at[way], self.recv.at[way, 0, 0]).wait_send()
            self.some(512, self.core_send.at[way], self.core_recv.at[way]).wait_send()


def layer_kernel(
    chunks, sp_count,
    res_hbm, q_hbm, k_hbm, v_hbm, sink_ref, proj_hbm, gain_mix_ref, gain_pre_ref, gain_post_ref,
    gate_hbm, up_hbm, down_hbm,
    out_hbm,
    done, res_ref, q_ref, k_ref, v_ref, gate_ref, up_ref, down_ref,
    whole, keys, keys_turned, values, values_turned, taken, att,
    mixed, mine, squares, rows,
    normed, hidden, f_sent, f_got, f_own, f_total, f_mine, f_squares,
    out_sem, load_sem, w_send, w_recv, core_send, core_recv,
    halo_send, halo_recv, p_send, p_recv, at_send, at_recv, sq_send, sq_recv, ag_send, ag_recv,
    f_rs_send, f_rs_recv, f_sq_send, f_sq_recv,
):
    me, right, left, far = ring()
    sp = lax.axis_index("sp")
    after = lax.rem(sp + 1, sp_count)
    before = lax.rem(sp + sp_count - 1, sp_count)
    length = chunks * WINDOW
    half_chunks = chunks // 2
    units = gate_ref.shape[1]
    tiles = units // 128
    inner = 2 * units
    projection = Projection(taken, proj_hbm, p_send, p_recv)
    loads = [
        pltpu.make_async_copy(a, b, load_sem.at[n])
        for n, (a, b) in enumerate((
            (proj_hbm.at[:, projection.columns(me)], taken.at[0]), (k_hbm, k_ref), (v_hbm, v_ref), (gate_hbm, gate_ref),
            (up_hbm, up_ref), (down_hbm, down_ref), (q_hbm, q_ref), (res_hbm, res_ref),
        ))
    ]
    for load in loads:
        load.start()
    weights = Weights(whole, w_send, w_recv, core_send, core_recv)
    barrier = pltpu.get_barrier_semaphore()
    others = [{"tp": right}, {"tp": left}, {"tp": far}, {"sp": after}, {"sp": before}]
    others += [{"sp": n} for n in weights.neighbours()]
    for other in others:
        pl.semaphore_signal(barrier, inc=1, device_id=other, device_id_type=MESH)
    pl.semaphore_wait(barrier, len(others))
    projection.step(0)
    for load in loads[1:3]:
        load.wait()

    def halo(n):
        mine_ref, both = ((k_ref, keys), (v_ref, values))[n // 2]
        if n % 2 == 0:
            src, dst, to = mine_ref.at[pl.ds(length - WINDOW, WINDOW)], both.at[pl.ds(0, WINDOW)], after
        else:
            src, dst, to = mine_ref.at[pl.ds(0, WINDOW)], both.at[pl.ds(length + WINDOW, WINDOW)], before
        return pltpu.make_async_remote_copy(
            src_ref=src, dst_ref=dst, send_sem=halo_send, recv_sem=halo_recv,
            device_id={"sp": to}, device_id_type=MESH,
        )

    halos = keys.at[pl.ds(0, 4 * WINDOW)]
    halos = tp_copy(halos, halos, halo_send, halo_recv, right)
    for n in range(4):
        halo(n).start()
    for load in loads[3:6]:
        load.wait()
    shard = pl.ds(pl.multiple_of(sp * 64, 64), 64)
    for j in range(tiles):
        whole[shard, 256 * j : 256 * j + 128] = gate_ref[:, 128 * j : 128 * j + 128]
        whole[shard, 256 * j + 128 : 256 * j + 256] = up_ref[:, 128 * j : 128 * j + 128]
        whole[shard, inner + 128 * j : inner + 128 * j + 128] = (
            down_ref[:, 128 * j : 128 * j + 128]
        )
    middle = pl.ds(WINDOW, length)
    keys[middle, :] = k_ref[...]
    values[middle, :] = v_ref[...]
    keys_turned[middle, :] = turn(k_ref[...])
    values_turned[middle, :] = turn(v_ref[...])
    weights.open(0, 0)
    weights.open(1, 0)
    weights.open(0, 1)
    weights.over(0, 0, 0).start()
    weights.over(1, 0, 0).start()
    for load in loads[6:] + loads[:1]:
        load.wait()

    mixing = Gather(att, at_send, at_recv)
    feeding = Gather(rows, ag_send, ag_recv)
    sums = Squares(mine, squares, sq_send, sq_recv)
    f_scatter = Scatter(f_sent, f_got, f_own, f_rs_send, f_rs_recv)
    f_sums = Squares(f_mine, f_squares, f_sq_send, f_sq_recv)
    columns = pl.ds(pl.multiple_of(me * 512, 512), 512)
    gain_mix = gain_mix_ref[:, columns]
    gain_post = gain_post_ref[:, columns]

    def place(slot):
        return pl.multiple_of(lax.rem(slot + 1, chunks) * WINDOW, WINDOW)

    def attention(t):
        @pl.when(t == chunks - 2)
        def _():
            halos.wait_recv()
            for at in (0, length + WINDOW):
                keys_turned[pl.ds(at, WINDOW), :] = turn(keys[pl.ds(at, WINDOW), :])
                values_turned[pl.ds(at, WINDOW), :] = turn(values[pl.ds(at, WINDOW), :])

        row = place(t)
        lowest = jnp.where((sp == 0) & (t == chunks - 1), WINDOW, 0)
        highest = jnp.where((sp == sp_count - 1) & (t == chunks - 2), 2 * WINDOW, 3 * WINDOW)
        att[me, t] = attend(
            row, row, q_ref, (keys, keys_turned, values, values_turned), sink_ref, lowest, highest
        )
        mixing.open(t)

    def mix(s):
        mixing.close(s)
        total = jnp.zeros((WINDOW, 512), F32)
        for k, owner in enumerate((me, right, far, left)):
            total += jnp.dot(att[owner, s], taken[k], preferred_element_type=F32)
        mixed[s] = total
        sums.give(s, total[:, :256], total[:, 256:])

    def first_rows(s):
        scale = lax.rsqrt(sums.take(s) / 2048.0 + EPS)
        res = res_ref[pl.ds(place(s), WINDOW), :].astype(F32)
        rows[me, s] = (res + mixed[s] * scale * gain_mix).astype(BF16)
        feeding.open(s)

    def prepare(u):
        for k in range(2):
            squared = jnp.zeros((WINDOW, 1), F32)
            for b in range(4):
                x = rows[b, 2 * u + k].astype(F32)
                squared += jnp.sum(x * x, axis=1, keepdims=True)
            scale = lax.rsqrt(squared / 2048.0 + EPS)
            for b in range(4):
                x = rows[b, 2 * u + k].astype(F32)
                normed[WINDOW * k : WINDOW * k + WINDOW, 512 * b : 512 * b + 512] = (
                    x * scale * gain_pre_ref[:, 512 * b : 512 * b + 512]
                ).astype(BF16)

        for j in range(tiles):
            both = jnp.dot(
                normed[...], whole[:, 256 * j : 256 * j + 256], preferred_element_type=F32
            )
            gate, up = both[:, :128], both[:, 128:]
            hidden[lax.rem(u, 2), :, 128 * j : 128 * j + 128] = (gate / (1.0 + jnp.exp(-gate)) * up).astype(BF16)

    def feed(u):
        def part(block, half):
            at = pl.ds(pl.multiple_of(block * 512 + 256 * half, 256), 256)
            return lax.dot_general(
                hidden[lax.rem(u, 2)], whole[at, inner : inner + units], NT,
                preferred_element_type=F32,
            ).astype(BF16)

        f_scatter.first(u, part)

    def feed_sum(u):
        half0, half1 = f_scatter.last(u)
        f_total[u, :, :256] = half0
        f_total[u, :, 256:] = half1
        f_sums.give(u, half0, half1)

    def finish(u):
        scale = lax.rsqrt(f_sums.take(u) / 2048.0 + EPS)
        for k in range(2):
            part = pl.ds(WINDOW * k, WINDOW)
            at = pl.ds(place(2 * u + k), WINDOW)
            done[at, :] = (
                rows[me, 2 * u + k].astype(F32)
                + 0.5 * (f_total[u, part, :] * scale[WINDOW * k : WINDOW * k + WINDOW] * gain_post)
            ).astype(BF16)
            result(2 * u + k).start()

    def result(slot):
        at = pl.ds(place(slot), WINDOW)
        return pltpu.make_async_copy(done.at[at, :], out_hbm.at[at, :], out_sem)

    def step(t, carry):
        def when(lag, fn):
            @pl.when((t >= lag) & (t < chunks + lag))
            def _():
                fn(t - lag)

        def when_fed(times, fn):
            now, index = t == times[0], 0
            for n in times[1:]:
                now, index = now | (t == n), index + (t >= n).astype(jnp.int32)

            @pl.when(now)
            def _():
                fn(index)

        when(0, attention)
        when(1, mixing.relay)

        for n in range(1, 5):
            @pl.when(t == PROJECTION[n])
            def _():
                projection.step(n)

        when(MIX, mix)
        when(MIX + 1, first_rows)

        for n in range(9):
            for way in (0, 1):
                @pl.when(t == WEIGHTS[way][n])
                def _():
                    weights.step(way, n)

        when_fed(PREPARE[:3], prepare)
        when(MIX + 2, feeding.relay)
        when(MIX + 3, feeding.close)

        @pl.when(t == PREPARE[3])
        def _():
            prepare(3)


        when_fed(SECOND, f_scatter.second)
        when_fed(FEED, feed)
        when_fed(SUM, feed_sum)
        when_fed(FINISH, finish)
        @pl.when(t == FEED[3])
        def _():
            halos.wait_send()
            weights.drain()
            projection.drain()
            mixing.drain()
            feeding.drain()
            sums.drain()

        return carry

    lax.fori_loop(0, FINISH[-1] + 1, step, 0)
    f_scatter.drain()
    f_sums.drain()
    pltpu.make_async_copy(done, out_hbm, out_sem).wait()


def pass_kernel(in_hbm, out_hbm, held, in_sem, out_sem):
    size = held.shape[0] // PIECES
    ins, outs = [], []
    for n in range(PIECES):
        at = pl.ds(n * size, size)
        ins.append(pltpu.make_async_copy(in_hbm.at[at, :], held.at[at, :], in_sem.at[n]))
        outs.append(pltpu.make_async_copy(held.at[at, :], out_hbm.at[at, :], out_sem))
    for copy in ins:
        copy.start()
    for copy, out in zip(ins, outs):
        copy.wait()
        out.start()
    pltpu.make_async_copy(held, out_hbm, out_sem).wait()


def sems(*shapes):
    return [pltpu.SemaphoreType.DMA(s) for s in shapes]


def body(
    residual, rotated_query_rows, rotated_key_rows, value_matrix_rows, head_sink_logit,
    out_proj, gain_mix, gain_pre, gain_post, gate_proj, up_proj, down_proj,
):
    length = residual.shape[0]
    chunks = length // WINDOW
    half = chunks // 2
    units = gate_proj.shape[1]
    sp_count = lax.axis_size("sp")
    full = sp_count * gate_proj.shape[0]
    big = 2 * WINDOW
    vmem = pl.BlockSpec(memory_space=pltpu.VMEM)
    smem = pl.BlockSpec(memory_space=pltpu.SMEM)
    hbm = pl.BlockSpec(memory_space=pl.ANY)
    loaded = (
        residual, rotated_query_rows, rotated_key_rows, value_matrix_rows, out_proj,
        gate_proj, up_proj, down_proj.T,
    )
    result = pl.pallas_call(
        functools.partial(layer_kernel, chunks, sp_count),
        out_shape=jax.ShapeDtypeStruct(residual.shape, BF16),
        in_specs=[hbm] * 4 + [smem, hbm] + [vmem] * 3 + [hbm] * 3,
        out_specs=hbm,
        scratch_shapes=[pltpu.VMEM(residual.shape, BF16)]
        + [pltpu.VMEM(a.shape, BF16) for a in loaded[:4] + loaded[5:]]
        + [pltpu.VMEM((full, 3 * units), BF16)]
        + [pltpu.VMEM((length + big, 128), BF16)] * 4
        + [
            pltpu.VMEM((4, out_proj.shape[0], 512), BF16),
            pltpu.VMEM((4, chunks, WINDOW, 384), BF16),
            pltpu.VMEM((chunks, WINDOW, 512), F32),
            pltpu.VMEM((chunks, 8, 128), F32),
            pltpu.VMEM((chunks, 3, 8, 128), F32),
            pltpu.VMEM((4, chunks, WINDOW, 512), BF16),
            pltpu.VMEM((big, full), BF16),
            pltpu.VMEM((2, big, units), BF16),
            pltpu.VMEM((half, 6, big, 256), BF16),
            pltpu.VMEM((half, 6, big, 256), BF16),
            pltpu.VMEM((half, big, 512), BF16),
            pltpu.VMEM((half, big, 512), F32),
            pltpu.VMEM((half, 16, 128), F32),
            pltpu.VMEM((half, 3, 16, 128), F32),
        ]
        + [pltpu.SemaphoreType.DMA]
        + sems((8,), (2,), (2, 5, 2), (2,), (2,), (), (), (3,), (4,), (), (chunks, 2), (), (chunks,))
        + sems((), (chunks, 2), (), (half, 2), (), (half,)),
        compiler_params=pltpu.CompilerParams(
            collective_id=0, has_side_effects=True, vmem_limit_bytes=54 * 2**20
        ),
    )(
        residual, rotated_query_rows, rotated_key_rows, value_matrix_rows, head_sink_logit,
        out_proj, gain_mix[None], gain_pre[None], gain_post[None], *loaded[5:],
    )
    return pl.pallas_call(
        pass_kernel,
        out_shape=jax.ShapeDtypeStruct(residual.shape, BF16),
        in_specs=[hbm],
        out_specs=hbm,
        scratch_shapes=[pltpu.VMEM(residual.shape, BF16)] + sems((PIECES,), ()),
    )(result)


def solution(mesh):
    placed = (
        P("sp", "tp"), P("sp", "tp"), P("sp", "tp"), P("sp", "tp"), P("tp"), P("tp", None),
        P(), P(), P(), P("sp", "tp"), P("sp", "tp"), P("tp", "sp"),
    )
    return jax.shard_map(body, mesh=mesh, in_specs=placed, out_specs=P("sp", "tp"), check_vma=False)
```
